32 devices in a mesh: ep: 16 (over z, y, x), tp: 2 (over core).
Axes of the slice: x: 2, y: 2, z: 4, core: 2. Of those that a mesh axis runs over, the one named last changes fastest.
Arguments:
- tokens: bfloat16 [2048, 2048], P('ep'), may hold values from -6 to 6
- cotangent: bfloat16 [2048, 2048], P('ep'), may hold values from -0.625 to 0.625
- routes: int32 [2048, 2], P('ep'), may hold values from 0 to 15, as said below
- router_group: bfloat16 [2048, 4], replicated, may hold values from -0.125 to 0.125
- router_expert: bfloat16 [2048, 16], replicated, may hold values from -0.125 to 0.125
- gate_proj: bfloat16 [16, 2048, 512], P('ep', None, 'tp'), may hold values from -0.125 to 0.125
- up_proj: bfloat16 [16, 2048, 512], P('ep', None, 'tp'), may hold values from -0.125 to 0.125
- down_proj: bfloat16 [16, 512, 2048], P('ep', 'tp'), may hold values from -0.25 to 0.25
Outputs:
- token_grad: bfloat16 [2048, 2048], P('ep', 'tp')
- gate_grad: bfloat16 [16, 2048, 512], P('ep', None, 'tp')
- up_grad: bfloat16 [16, 2048, 512], P('ep', None, 'tp')
- down_grad: bfloat16 [16, 512, 2048], P('ep', 'tp')
- gate_rows: float32 [16, 2048], P('ep')
- up_rows: float32 [16, 2048], P('ep')
- down_rows: float32 [16, 512], P('ep', 'tp')
- router_expert_grad: float32 [2048, 16], P(('ep', 'tp'))
- router_group_grad: float32 [2048, 4], P(('ep', 'tp'))
- router_rows: float32 [2048], P(('ep', 'tp'))
The draws below stay inside these ranges and needn't reach their ends.
Inputs may be any that keep to these rules, and one draw needn't show every extreme that they name: `routes`: the 2 entries of a row are different experts of one group: their quotients by 4 are equal. Among the rows of one device no expert is named more than 32 times, and the experts of one group, the same for all devices, are each named exactly 32 times by the rows of every device.
All inputs are finite; a program needn't handle non-finite values.
Results may differ from the reference program's by a relative error of at most 0.014.
Values may be sent and summed in bfloat16 or wider, within the bound.
A program may use at most 64 MiB of HBM per device.

```python
import jax
import jax.numpy as jnp
from jax import lax

D = 2048
FF = 512
TOK_DEV = 128
GROUPS = 4
TOP = 2
EXPERTS = 16
GROUP_SIZE = 4
TOKENS = 2048
N_TP = 2


def draw_routes(key, part):
    blocks = TOKENS // TOK_DEV
    half_rows = TOK_DEV // 2
    others_rows = TOK_DEV - half_rows
    favored = jax.random.randint(jax.random.fold_in(key, 11), (), 0, GROUPS)
    group_ids = jnp.arange(GROUPS, dtype=jnp.int32)
    is_favored = group_ids[None, :] == favored
    shares = jax.random.randint(jax.random.fold_in(key, 12), (blocks, GROUPS), 2, 5)
    shares = jnp.where(is_favored, 0, shares)
    base_rows = others_rows * shares // jnp.sum(shares, axis=1, keepdims=True)
    leftover = others_rows - jnp.sum(base_rows, axis=1, keepdims=True)
    other_rank = jnp.cumsum(jnp.where(is_favored, 0, 1), axis=1) - 1
    extra_rows = jnp.where(jnp.logical_and(jnp.logical_not(is_favored), other_rank < leftover), 1, 0)
    counts = base_rows + extra_rows + jnp.where(is_favored, half_rows, 0)
    group_end = jnp.cumsum(counts, axis=1)
    group_start = group_end - counts
    position = jnp.arange(TOK_DEV, dtype=jnp.int32)
    labels = jnp.sum((group_end[:, None, :] <= position[None, :, None]).astype(jnp.int32), axis=2)
    within = position[None, :] - jnp.take_along_axis(group_start, labels, axis=1)
    rotate = jax.random.randint(jax.random.fold_in(key, 13), (blocks, GROUPS), 0, GROUP_SIZE)
    offset = jax.random.randint(jax.random.fold_in(key, 14), (blocks, GROUPS), 0, GROUP_SIZE - 1)
    first_pick = (within + jnp.take_along_axis(rotate, labels, axis=1)) % GROUP_SIZE
    turned = (jnp.take_along_axis(offset, labels, axis=1) + within // GROUP_SIZE) % (GROUP_SIZE - 1)
    second_pick = (first_pick + 1 + turned) % GROUP_SIZE
    chosen = jnp.stack([labels * GROUP_SIZE + first_pick, labels * GROUP_SIZE + second_pick], axis=2)
    block_keys = jax.random.split(jax.random.fold_in(key, 15), blocks)
    shuffles = jax.vmap(lambda subkey: jax.random.permutation(subkey, TOK_DEV))(block_keys)
    chosen = jnp.take_along_axis(chosen, shuffles[:, :, None], axis=1)
    return chosen.reshape(TOKENS, TOP).astype(jnp.int32)


def spiked(values, rng, source, target, blocks, factor):
    def block_of(axis_at):
        return (jnp.arange(values.shape[axis_at]) // (values.shape[axis_at] // blocks)).reshape((-1,) + (1,) * (values.ndim - 1 - axis_at))

    first = jax.random.permutation(rng, blocks)[block_of(target)]
    other_side = (block_of(target) + blocks // 2) % blocks
    return jnp.where((block_of(source) == first) | (block_of(source) == other_side), factor * values, values)


def level_of(key, shape, cuts, low, high):
    def one(dim, shards_of):
        heights = jax.random.uniform(jax.random.fold_in(jax.random.fold_in(key, 6), dim), (shards_of,), jnp.float32, low / len(cuts), high / len(cuts))
        return jnp.repeat(jnp.exp(heights), shape[dim] // shards_of).reshape((-1,) + (1,) * (len(shape) - dim - 1))

    factor_of = one(*cuts[0])
    for cut in cuts[1:]:
        factor_of = factor_of * one(*cut)
    return factor_of


def noise(key, shape, width, most, pieces=(), kind=jnp.bfloat16):
    loudness = level_of(key, shape, pieces, -0.22, 0.18) if pieces else 1.0
    result = jax.random.normal(key, shape, jnp.float32) * width * loudness
    return jnp.minimum(jnp.maximum(result, -most), most).astype(kind)


def heavy_noise(rng, extent, width, reach, pieces, heavy, kind=jnp.bfloat16):
    array = width * jax.random.normal(rng, extent, jnp.float32)
    if pieces:
        array = array * level_of(rng, extent, pieces, -0.22, 0.18)
    return jnp.clip(spiked(array, jax.random.fold_in(rng, 3), *heavy), -reach, reach).astype(kind)


def setup_inputs(seed: int = 0) -> dict:
    keys = jax.random.split(jax.random.key(seed), 9)
    tokens = heavy_noise(keys[0], (TOKENS, D), 1.0, 6.0, ((0, 16),), (0, 1, 16, 2.0))
    cotangent = noise(keys[1], (TOKENS, D), 0.1, 0.625, ((0, 16),))
    routes = draw_routes(jax.random.fold_in(keys[8], 71), 0)
    router_group = noise(keys[3], (D, GROUPS), D ** -0.5, 0.125)
    router_expert = noise(keys[4], (D, EXPERTS), D ** -0.5, 0.125)
    gate_proj = noise(keys[5], (EXPERTS, D, FF), D ** -0.5, 0.125, ((0, 16), (2, 2)))
    up_proj = noise(keys[6], (EXPERTS, D, FF), D ** -0.5, 0.125, ((0, 16), (2, 2)))
    down_proj = noise(keys[7], (EXPERTS, FF, D), FF ** -0.5, 0.25, ((0, 16), (1, 2)))
    return dict(tokens=tokens, cotangent=cotangent, routes=routes, router_group=router_group, router_expert=router_expert, gate_proj=gate_proj, up_proj=up_proj, down_proj=down_proj)


tile_rows = 128


def contract_rows(left_side, right_side):
    return lax.dot_general(left_side, right_side, (((0,), (0,)), ((), ())), preferred_element_type=jnp.float32)


def contract_cols(left_side, right_side):
    return lax.dot_general(left_side, right_side, (((1,), (1,)), ((), ())), preferred_element_type=jnp.float32)


def router_forward(tokens, routes, router_group, router_expert):
    groups = router_group.shape[1]
    experts = router_expert.shape[1]
    group_logits = jnp.dot(tokens, router_group, preferred_element_type=jnp.float32)
    expert_logits = jnp.dot(tokens, router_expert, preferred_element_type=jnp.float32)
    group_exp = jnp.exp(group_logits)
    group_prob = group_exp / jnp.sum(group_exp, axis=1, keepdims=True)
    chosen_group = routes[:, 0] // (experts // groups)
    group_onehot = (chosen_group[:, None] == jnp.arange(groups, dtype=jnp.int32)[None, :]).astype(jnp.float32)
    picked = jnp.sum(group_prob * group_onehot, axis=1)
    chosen_logits = jnp.take_along_axis(expert_logits, routes, axis=1)
    paired_exp = jnp.exp(chosen_logits)
    paired = paired_exp / jnp.sum(paired_exp, axis=1, keepdims=True)
    return group_prob, group_onehot, picked, paired


def router_backward(dweight, routes, group_prob, group_onehot, picked, paired, experts):
    dpicked = jnp.sum(dweight * paired, axis=1)
    dpaired = dweight * picked[:, None]
    dchosen = paired * (dpaired - jnp.sum(paired * dpaired, axis=1, keepdims=True))
    dgroup = ((dpicked * picked)[:, None] * (group_onehot - group_prob)).astype(jnp.bfloat16)
    expert_onehot = (routes[:, :, None] == jnp.arange(experts, dtype=jnp.int32)[None, None, :]).astype(jnp.float32)
    dexpert = jnp.sum(dchosen[:, :, None] * expert_onehot, axis=1).astype(jnp.bfloat16)
    return dgroup, dexpert


def reference(tokens, cotangent, routes, router_group, router_expert, gate_proj, up_proj, down_proj):
    group_prob, group_onehot, picked, paired = router_forward(tokens, routes, router_group, router_expert)
    weights = (picked[:, None] * paired).astype(jnp.bfloat16)
    assigned = TOKENS * TOP
    flat_ids = routes.reshape(assigned).astype(jnp.int32)
    counts = jnp.zeros((EXPERTS,), jnp.int32).at[flat_ids].add(1)
    tile_count = ((counts + (tile_rows - 1)) // tile_rows).astype(jnp.int32)
    tile_end = jnp.cumsum(tile_count).astype(jnp.int32)
    tile_begin = (tile_end - tile_count).astype(jnp.int32)
    count_begin = (jnp.cumsum(counts).astype(jnp.int32) - counts).astype(jnp.int32)
    ordering = jnp.argsort(flat_ids, stable=True).astype(jnp.int32)
    sorted_ids = flat_ids[ordering]
    ranking = jnp.arange(assigned, dtype=jnp.int32) - count_begin[sorted_ids]
    padded_pos = (tile_begin[sorted_ids] * tile_rows + ranking).astype(jnp.int32)
    tile_total = (assigned + tile_rows - 1) // tile_rows + EXPERTS
    owners = jnp.full((tile_total * tile_rows,), assigned, jnp.int32).at[padded_pos].set(ordering)
    tile_marks = jnp.arange(tile_total, dtype=jnp.int32)[:, None]
    tile_expert = jnp.minimum(jnp.sum((tile_end[None, :] <= tile_marks).astype(jnp.int32), axis=1), EXPERTS - 1).astype(jnp.int32)
    flat_weights = weights.reshape(assigned)
    piece_width = FF // N_TP

    def tile_step(totals, tile_index):
        grad_gate, grad_up, grad_down = totals
        expert = tile_expert[tile_index]
        members = lax.dynamic_slice_in_dim(owners, tile_index * tile_rows, tile_rows)
        source_rows = members // TOP
        inputs = jnp.take(tokens, source_rows, axis=0, mode="fill", fill_value=0)
        upstream = jnp.take(cotangent, source_rows, axis=0, mode="fill", fill_value=0)
        slot_scale = jnp.take(flat_weights, members, axis=0, mode="fill", fill_value=0).astype(jnp.float32)
        gate_mat = gate_proj[expert]
        up_mat = up_proj[expert]
        down_mat = down_proj[expert]
        gate_pre = jnp.dot(inputs, gate_mat, preferred_element_type=jnp.float32)
        up_pre = jnp.dot(inputs, up_mat, preferred_element_type=jnp.float32)
        sigmoid_gate = jax.nn.sigmoid(gate_pre)
        hidden = (gate_pre * sigmoid_gate * up_pre).astype(jnp.bfloat16)
        pulled = contract_cols(upstream, down_mat)
        weight_part = jnp.sum(pulled * hidden.astype(jnp.float32), axis=1)
        dhidden = slot_scale[:, None] * pulled
        gate_delta = (dhidden * up_pre * sigmoid_gate * (1.0 + gate_pre * (1.0 - sigmoid_gate))).astype(jnp.bfloat16)
        up_delta = (dhidden * gate_pre * sigmoid_gate).astype(jnp.bfloat16)
        scaled_cot = (slot_scale[:, None] * upstream.astype(jnp.float32)).astype(jnp.bfloat16)
        grad_gate = grad_gate.at[expert].add(contract_rows(inputs, gate_delta))
        grad_up = grad_up.at[expert].add(contract_rows(inputs, up_delta))
        grad_down = grad_down.at[expert].add(contract_rows(hidden, scaled_cot))
        token_total = jnp.zeros((tile_rows, D), jnp.float32)
        for piece_index in range(N_TP):
            first_col = piece_index * piece_width
            last_col = first_col + piece_width
            piece_term = contract_cols(gate_delta[:, first_col:last_col], gate_mat[:, first_col:last_col])
            piece_term = piece_term + contract_cols(up_delta[:, first_col:last_col], up_mat[:, first_col:last_col])
            token_total = token_total + piece_term.astype(jnp.bfloat16).astype(jnp.float32)
        return (grad_gate, grad_up, grad_down), (token_total.astype(jnp.bfloat16), weight_part)

    start_totals = (jnp.zeros((EXPERTS, D, FF), jnp.float32), jnp.zeros((EXPERTS, D, FF), jnp.float32),
                    jnp.zeros((EXPERTS, FF, D), jnp.float32))
    totals, tile_outputs = lax.scan(tile_step, start_totals, jnp.arange(tile_total, dtype=jnp.int32))
    grad_gate, grad_up, grad_down = totals
    token_tiles, weight_tiles = tile_outputs
    position = jnp.zeros((assigned,), jnp.int32).at[ordering].set(padded_pos)
    token_rows = token_tiles.reshape(tile_total * tile_rows, D)[position]
    expert_part = jnp.sum(token_rows.reshape(TOKENS, TOP, D).astype(jnp.float32), axis=1)
    dweight = weight_tiles.reshape(tile_total * tile_rows)[position].astype(jnp.bfloat16).astype(jnp.float32)
    dweight = dweight.reshape(TOKENS, TOP)
    dgroup, dexpert = router_backward(dweight, routes, group_prob, group_onehot, picked, paired, EXPERTS)
    router_part = contract_cols(dgroup, router_group) + contract_cols(dexpert, router_expert)
    token_grad = (expert_part + router_part).astype(jnp.bfloat16)
    router_expert_grad = contract_rows(tokens, dexpert)
    router_group_grad = contract_rows(tokens, dgroup)
    router_rows = jnp.sum(router_expert_grad * router_expert_grad, axis=1) + jnp.sum(router_group_grad * router_group_grad, axis=1)
    gate_rows = jnp.sum(grad_gate * grad_gate, axis=2)
    up_rows = jnp.sum(grad_up * grad_up, axis=2)
    down_rows = jnp.sum(grad_down * grad_down, axis=2)
    return (token_grad, grad_gate.astype(jnp.bfloat16), grad_up.astype(jnp.bfloat16), grad_down.astype(jnp.bfloat16),
            gate_rows, up_rows, down_rows, router_expert_grad, router_group_grad, router_rows)
```

```python
import functools

import jax
import jax.numpy as jnp
from jax import lax
from jax.experimental import pallas as pl
from jax.experimental.pallas import tpu as pltpu
from jax.sharding import PartitionSpec as P

MESH = pl.DeviceIdType.MESH
BF = jnp.bfloat16
F32 = jnp.float32


def mm(a, b, da=1, db=0):
    return lax.dot_general(a, b, (((da,), (db,)), ((), ())), preferred_element_type=F32)


def lanes_of(shape, dim=1):
    return lax.broadcasted_iota(jnp.int32, shape, dim)


class Sizes:
    pass


def sizes_of(mesh, tokens, routes, router_group, router_expert, gate_proj):
    z = Sizes()
    z.n_ep, z.n_tp = mesh["ep"], mesh["tp"]
    z.rows, z.width = tokens.shape
    z.top = routes.shape[1]
    z.groups, z.experts = router_group.shape[1], router_expert.shape[1]
    z.gs = z.experts // z.groups
    z.cap = z.rows // z.gs
    z.gr = z.gs * z.cap // z.top
    z.r1 = z.groups * z.gr
    z.sl = z.groups * z.cap
    z.pairs = z.gs * z.sl
    z.ff = gate_proj.shape[2]
    z.cw = z.width // z.n_tp
    z.half_chunks = 4
    z.nc = 2 * z.half_chunks
    z.cc = z.cw // z.half_chunks
    z.rl = -(-(z.experts + z.groups) // 128) * 128
    z.rw = -(-(z.experts + z.groups) // 8) * 8
    z.ch = z.width // z.n_ep
    z.reduce_here = z.ch % 128 == 0 and z.n_ep % 2 == 0
    assert z.experts == z.n_ep and z.n_tp == 2 and z.top == 2
    assert z.sl & (z.sl - 1) == 0 and z.gr & (z.gr - 1) == 0
    return z


def kernel(
    z, tok_ref, cot_ref, routes_ref, rexp_ref, rgrp_ref, gate_ref, up_ref, down_ref,
    tg_out, gate_out, up_out, down_out, gsq_out, usq_out, dsq_out, rout_out,
    rc_ref, s1w, r1w,
    s_mat, t_mat, s1m, r1m, s1, r1, s2m, x2m, s2, x2, y2m, y2,
    gacc, uacc, pacc, dcat, hid, wcol, wp, wpr, pts, ptr, pto,
    s3m, r3m, s3, r3, s4m, r4m, s4, r4, sq, sqr, term, trec, tsum, tsumr,
    z1s, z1r, p2s, p2r, fs, fr, ptsm, ptrm, r3s, r3r, r4s, r4r, ms, mr, ts, tr,
):
    e, t = lax.axis_index("ep"), lax.axis_index("tp")
    g, p = e // z.gs, e % z.gs
    other = 1 - t

    def rcopy(src, dst, ss, rs, ep, tp):
        return pltpu.make_async_remote_copy(
            src_ref=src, dst_ref=dst, send_sem=ss, recv_sem=rs,
            device_id=(ep, tp), device_id_type=MESH,
        )

    barrier = pltpu.get_barrier_semaphore()
    for d in range(1, z.n_ep):
        pl.semaphore_signal(
            barrier, inc=1, device_id=((e + d) % z.n_ep, t), device_id_type=MESH
        )
    pl.semaphore_signal(barrier, inc=1, device_id=(e, other), device_id_type=MESH)

    sends = []

    def grows(h):
        return pl.ds(pl.multiple_of(h * z.gr, z.gr), z.gr)

    def prows(q):
        return pl.ds(pl.multiple_of(q * z.sl, z.sl), z.sl)

    def group_send(src, dst, ss, rs, c):
        for d in range(1, z.groups):
            h = (g + d) % z.groups
            cp = rcopy(src.at[grows(h)], dst.at[grows(g)], ss.at[c, d], rs.at[c, d], h * z.gs + p, t)
            cp.start()
            sends.append(cp)
        dst[grows(g), :] = src[grows(g), :]

    def group_wait(src, dst, ss, rs, c):
        for d in range(1, z.groups):
            h = (g + z.groups - d) % z.groups
            rcopy(src.at[grows(h)], dst.at[grows(h)], ss.at[c, d], rs.at[c, d], h * z.gs + p, t).wait_recv()

    def plane_send(src, dst, ss, rs, c):
        for d in range(1, z.gs):
            q = (p + d) % z.gs
            cp = rcopy(src.at[prows(q)], dst.at[prows(p)], ss.at[c, d], rs.at[c, d], g * z.gs + q, t)
            cp.start()
            sends.append(cp)
        dst[prows(p), :] = src[prows(p), :]

    def plane_wait_one(src, dst, ss, rs, c, d):
        q = (p + z.gs - d) % z.gs
        rcopy(src.at[prows(q)], dst.at[prows(q)], ss.at[c, d], rs.at[c, d], g * z.gs + q, t).wait_recv()

    def plane_wait(src, dst, ss, rs, c):
        for d in range(1, z.gs):
            plane_wait_one(src, dst, ss, rs, c, d)

    def pair_send(src, dst, ss, rs):
        cp = rcopy(src, dst, ss, rs, e, other)
        cp.start()
        sends.append(cp)
        return cp

    lane = lanes_of((z.rows, z.rl))
    eye = lanes_of((z.rows, z.rows), 0) == lanes_of((z.rows, z.rows), 1)

    def column(row):
        return jnp.sum(jnp.where(eye, row.astype(F32), 0.0), axis=1, keepdims=True).astype(jnp.int32)

    r0, r1_ = column(routes_ref[0:1, :]), column(routes_ref[1:2, :])
    chosen = (lane == r0) | (lane == r1_)
    low = (lane - z.experts) * z.gs
    is_group = (lane >= z.experts) & (lane < z.experts + z.groups)
    in_group = is_group & (r0 >= low) & (r0 < low + z.gs)

    def before(n):
        return (lanes_of((n, n), 1) < lanes_of((n, n), 0)).astype(F32).astype(BF)

    ghot = in_group.astype(F32)
    grank = mm(before(z.rows), ghot.astype(BF))
    grank = jnp.where(in_group, grank, -1.0).astype(BF)
    er, el = lanes_of((z.rl, z.r1), 0) - z.experts, lanes_of((z.rl, z.r1), 1)
    expand = ((el >= er * z.gr) & (el < (er + 1) * z.gr)).astype(F32).astype(BF)
    place = (lanes_of((z.rows, z.r1)) & (z.gr - 1)).astype(F32)
    s_mat[...] = (mm(grank, expand) == place).astype(F32).astype(BF)

    s1m[...] = mm(s_mat[...], chosen.astype(F32).astype(BF), 0, 0).astype(BF)
    pl.semaphore_wait(barrier, z.n_ep)
    group_send(s1m, r1m, z1s, z1r, z.nc)

    def cols_at(half, k):
        return pl.ds(pl.multiple_of(half * z.cw + k * z.cc, z.cc), z.cc)

    for c in range(z.nc):
        src = tok_ref if c < z.half_chunks else cot_ref
        s1[c] = mm(s_mat[...], src[:, cols_at(t, c % z.half_chunks)], 0, 0).astype(BF)
        group_send(s1.at[c], r1.at[c], z1s, z1r, c)

    rc_ref[...] = jnp.zeros_like(rc_ref)
    rc_ref[0 : z.experts, :] = rexp_ref[...]
    rc_ref[z.experts : z.experts + z.groups, :] = rgrp_ref[...]
    expd = jnp.exp(mm(tok_ref[...], rc_ref[...], 1, 1))
    gexp = jnp.where(is_group, expd, 0.0)
    gprob = gexp / jnp.sum(gexp, axis=1, keepdims=True)
    picked = jnp.sum(jnp.where(in_group, gprob, 0.0), axis=1, keepdims=True)
    pexp = jnp.where(chosen, expd, 0.0)
    paired = pexp / jnp.sum(pexp, axis=1, keepdims=True)
    s1w[...] = mm(s_mat[...], (picked * paired).astype(BF), 0, 0).astype(BF)
    group_send(s1w, r1w, z1s, z1r, z.nc + 1)

    group_wait(s1m, r1m, z1s, z1r, z.nc)
    vals = r1m[...]
    lane1 = lanes_of((z.r1, z.rl))
    member = (vals.astype(F32) > 0.0) & (lane1 < z.experts)
    rank = mm(before(z.r1), member.astype(F32).astype(BF))
    rank = jnp.where(member, rank, -1.0).astype(BF)
    er, el = lanes_of((z.rl, z.pairs), 0) - g * z.gs, lanes_of((z.rl, z.pairs), 1)
    expand = ((el >= er * z.sl) & (el < (er + 1) * z.sl)).astype(F32).astype(BF)
    place = (lanes_of((z.r1, z.pairs)) & (z.sl - 1)).astype(F32)
    t_mat[...] = (mm(rank, expand) == place).astype(F32).astype(BF)

    def pack_two(c):
        group_wait(s1.at[c], r1.at[c], z1s, z1r, c)
        s2[c] = mm(t_mat[...], r1[c], 0, 0).astype(BF)
        plane_send(s2.at[c], x2.at[c], p2s, p2r, c)
        pair_send(x2.at[c, prows(p)], y2.at[c, prows(p)], fs.at[c, 0], fr.at[c, 0])

    def accumulate(x, half, c):
        if c < z.half_chunks:
            at = cols_at(half, c)
            gate_add, up_add = mm(x, gate_ref[at, :]), mm(x, up_ref[at, :])
            gacc[...] += gate_add
            uacc[...] += up_add
        else:
            pacc[...] += mm(x, down_ref[:, cols_at(half, c - z.half_chunks)], 1, 1)

    def land(c):
        for d in range(1, z.gs):
            plane_wait_one(s2.at[c], x2.at[c], p2s, p2r, c, d)
            q = (p + z.gs - d) % z.gs
            pair_send(x2.at[c, prows(q)], y2.at[c, prows(q)], fs.at[c, d], fr.at[c, d])
        accumulate(x2[c], t, c)

    def land_other(c):
        for d in range(z.gs):
            q = (p + z.gs - d) % z.gs
            rcopy(x2.at[c, prows(q)], y2.at[c, prows(q)], fs.at[c, d], fr.at[c, d], e, other).wait_recv()
        accumulate(y2[c], other, c)

    gacc[...] = jnp.zeros_like(gacc)
    uacc[...] = jnp.zeros_like(uacc)
    pacc[...] = jnp.zeros_like(pacc)
    for c in range(z.nc + 3):
        if c < z.nc:
            pack_two(c)
        if c == z.nc - 1:
            group_wait(s1w, r1w, z1s, z1r, z.nc + 1)
            s2m[...] = mm(t_mat[...], r1w[...], 0, 0).astype(BF)
            plane_send(s2m, x2m, p2s, p2r, z.nc)
        if 2 <= c < z.nc + 2:
            land(c - 2)
        if c >= 3:
            land_other(c - 3)
    plane_wait(s2m, x2m, p2s, p2r, z.nc)

    lane2 = lanes_of((z.pairs, z.rl))
    scale = jnp.sum(jnp.where(lane2 == e, x2m[...].astype(F32), 0.0), axis=1, keepdims=True)
    wcol[...] = jnp.broadcast_to(scale, wcol.shape)
    gate_pre, up_pre, pulled = gacc[...], uacc[...], pacc[...]
    sig = 1.0 / (1.0 + jnp.exp(-gate_pre))
    silu = gate_pre * sig
    hidden = (silu * up_pre).astype(BF)
    hid[...] = hidden
    wp[...] = jnp.broadcast_to(
        jnp.sum(pulled * hidden.astype(F32), axis=1, keepdims=True), wp.shape
    )
    w_copy = pair_send(wp, wpr, ms.at[0], mr.at[0])
    dh = scale * pulled
    dcat[:, : z.ff] = (dh * up_pre * sig * (1.0 + gate_pre * (1.0 - sig))).astype(BF)
    dcat[:, z.ff :] = (dh * silu).astype(BF)

    def token_term(half, k):
        at = cols_at(half, k)
        return (
            mm(dcat[:, : z.ff], gate_ref[at, :], 1, 1) + mm(dcat[:, z.ff :], up_ref[at, :], 1, 1)
        ).astype(BF)

    pt = []
    for k in range(z.half_chunks):
        pts[k] = token_term(other, k)
        pt.append(pair_send(pts.at[k], ptr.at[k], ptsm.at[k], ptrm.at[k]))
    w_copy.wait_recv()
    wsum = wp[:, 0:1] + wpr[:, 0:1]
    s3m[...] = jnp.where(lane2 == e, wsum, 0.0).astype(BF)
    plane_send(s3m, r3m, r3s, r3r, z.half_chunks)
    for k in range(z.half_chunks):
        pto[k] = token_term(t, k)
        pt[k].wait_recv()
        s3[k] = (pto[k].astype(F32) + ptr[k].astype(F32)).astype(BF)
        plane_send(s3.at[k], r3.at[k], r3s, r3r, k)

    ones_ff = jnp.ones((16, z.ff), BF)

    def gate_up_grads(xs, half, k):
        at = cols_at(half, k)
        total = mm(xs[k], dcat[...], 0, 0)
        gate_out[at, :] = total[:, : z.ff].astype(BF)
        up_out[at, :] = total[:, z.ff :].astype(BF)
        square = (total * total).astype(BF)
        sq[0:1, at] = mm(ones_ff, square[:, : z.ff], 1, 1)[0:1]
        sq[1:2, at] = mm(ones_ff, square[:, z.ff :], 1, 1)[0:1]

    def down_grads(xs, half, k):
        scaled = (wcol[:, 0:1] * xs[z.half_chunks + k].astype(F32)).astype(BF)
        total = mm(hid[...], scaled, 0, 0)
        down_out[:, cols_at(half, k)] = total.astype(BF)
        return mm(jnp.ones((16, z.cc), BF), (total * total).astype(BF), 1, 1)[0:1]

    def back_two(k):
        plane_wait(s3.at[k], r3.at[k], r3s, r3r, k)
        s4[k] = mm(t_mat[...], r3[k]).astype(BF)
        group_send(s4.at[k], r4.at[k], r4s, r4r, k)

    gate_up_grads(x2, t, 0)
    plane_wait(s3m, r3m, r3s, r3r, z.half_chunks)
    s4m[...] = mm(t_mat[...], r3m[...]).astype(BF)
    group_send(s4m, r4m, r4s, r4r, z.half_chunks)
    gate_up_grads(x2, t, 1)
    for k in range(z.half_chunks - 1):
        back_two(k)
        if k + 2 < z.half_chunks:
            gate_up_grads(x2, t, k + 2)
        else:
            gate_up_grads(y2, other, 0)

    group_wait(s4m, r4m, r4s, r4r, z.half_chunks)
    dw = mm(s_mat[...], r4m[...])
    dpicked = jnp.sum(dw * paired, axis=1, keepdims=True)
    q = picked * dw
    dchosen = paired * (q - jnp.sum(paired * q, axis=1, keepdims=True))
    dgroup = jnp.where(is_group, (dpicked * picked) * (ghot - gprob), 0.0)
    dall = (dchosen + dgroup).astype(BF)
    dterm = dall[:, : z.rw] if z.rw < z.rl else dall
    tcopies = []
    if z.reduce_here:
        full = mm(dterm, tok_ref[...], 0, 0)
        for i in range(z.n_ep):
            term[i] = full[:, i * z.ch : (i + 1) * z.ch]

        def term_copy(m):
            to = (e + 2 * m + t) % z.n_ep
            return rcopy(term.at[to], trec.at[m], ts.at[m], tr.at[m], to, t)

        @pl.when(t == 0)
        def _():
            trec[0] = term[e]

        @pl.when(t == 1)
        def _():
            term_copy(0).start()

        for m in range(1, z.n_ep // 2):
            term_copy(m).start()
    else:
        row = lanes_of((z.rows, z.rl), 0)[:, : dterm.shape[1]]
        mine = (row >= t * (z.rows // 2)) & (row < (t + 1) * (z.rows // 2))
        dterm = jnp.where(mine, dterm.astype(F32), 0.0).astype(BF)
        rout_out[...] = mm(dterm, tok_ref[...], 0, 0)

    back_two(z.half_chunks - 1)
    for k in range(1, z.half_chunks):
        gate_up_grads(y2, other, k)
    sq_copy = pair_send(sq, sqr, ms.at[1], mr.at[1])
    dsq = jnp.zeros((1, z.ff), F32)
    for k in range(z.half_chunks):
        dsq += down_grads(x2, t, k)

    if z.reduce_here:

        @pl.when(t == 1)
        def _():
            term_copy(0).wait_recv()

        for m in range(1, z.n_ep // 2):
            term_copy(m).wait_recv()
        acc = trec[0]
        for m in range(1, z.n_ep // 2):
            acc = acc + trec[m]
        tsum[...] = acc
        t_pair = pair_send(tsum, tsumr, ms.at[2], mr.at[2])
    for k in range(z.half_chunks):
        dsq += down_grads(y2, other, k)
    dsq_out[...] = dsq

    for k in range(z.half_chunks):
        group_wait(s4.at[k], r4.at[k], r4s, r4r, k)
        tg_out[:, k * z.cc : (k + 1) * z.cc] = (
            mm(s_mat[...], r4[k]) + mm(dall, rc_ref[:, cols_at(t, k)])
        ).astype(BF)
    sq_copy.wait_recv()
    gsq_out[...] = sq[0:1, :] + sqr[0:1, :]
    usq_out[...] = sq[1:2, :] + sqr[1:2, :]
    if z.reduce_here:
        t_pair.wait_recv()
        rout_out[...] = tsum[...] + tsumr[...]

        @pl.when(t == 1)
        def _():
            term_copy(0).wait_send()

        for m in range(1, z.n_ep // 2):
            term_copy(m).wait_send()
    for cp in sends:
        cp.wait_send()


def sourced(
    z, tok_h, cot_h, routes_h, rexp_h, rgrp_h, gate_h, up_h, down_h,
    tg_out, gate_out, up_out, down_out, gsq_out, usq_out, dsq_out, rout_out,
    tok_ref, cot_ref, routes_ref, rexp_ref, rgrp_ref, gate_ref, up_ref, down_ref,
    rc_ref, s_mat, s_tr, t_mat, t_tr, s1m, r1m, s1w, r1w, s1, r1, s2m, x2m, s2, x2, y2,
    gacc, uacc, dcat, hid, wcol, wp, wpr, pts, ptr, s3m, r3m, s3, r3, s4, r4, dall_ref,
    sq, sqr, term, tra, tsa, trb, tsum, tsumr,
    ins, z1s, z1r, p2s, p2r, fs, fr, ws, wr, ptsm, ptrm, r3s, r3r, r4s, r4r, ms, mr, tas, tar, tbs, tbr,
):
    e, t = lax.axis_index("ep"), lax.axis_index("tp")
    g, p = e // z.gs, e % z.gs
    other = 1 - t
    hk = [g, g + 1 - 2 * (g % 2), 3 - g, (g + 2) % 4]
    qd = [p, p + 1 - 2 * (p % 2), (p + 2) % 4, 3 - p]
    nj, cc, gr, cap, blk, per = z.nj, z.cc, z.gr, z.cap, z.blk, z.per
    ng = 2 * nj
    far = (1, 2, 3)

    def rcopy(src, dst, ss, rs, ep, tp):
        return pltpu.make_async_remote_copy(
            src_ref=src, dst_ref=dst, send_sem=ss, recv_sem=rs,
            device_id=(ep, tp), device_id_type=MESH,
        )

    barrier = pltpu.get_barrier_semaphore()
    for k in far:
        pl.semaphore_signal(barrier, inc=1, device_id=(hk[k] * z.gs + p, t), device_id_type=MESH)
        pl.semaphore_signal(barrier, inc=1, device_id=(g * z.gs + qd[k], t), device_id_type=MESH)
    pl.semaphore_signal(barrier, inc=1, device_id=(e, other), device_id_type=MESH)

    loads = [
        pltpu.make_async_copy(a, b, ins.at[i])
        for i, (a, b) in enumerate((
            (routes_h, routes_ref), (tok_h, tok_ref), (rexp_h, rexp_ref), (rgrp_h, rgrp_ref),
            (cot_h, cot_ref), (gate_h, gate_ref), (up_h, up_ref), (down_h, down_ref),
        ))
    ]
    for cp in loads:
        cp.start()

    sends = []

    def go(cp):
        cp.start()
        sends.append(cp)
        return cp

    def kr(k):
        return pl.ds(k * gr, gr)

    def kb(k):
        return pl.ds(k * blk, blk)

    def slot(q):
        return pl.ds(pl.multiple_of(q * cap, cap), cap)

    def in_block(k, q):
        return pl.ds(pl.multiple_of(k * blk + q * cap, cap), cap)

    def cols(half, j):
        return pl.ds(pl.multiple_of(half * z.cw + j * cc, cc), cc)

    def z_send(src, dst, c, k):
        go(rcopy(src.at[kr(k)], dst.at[kr(k)], z1s.at[c, k], z1r.at[c, k], hk[k] * z.gs + p, t))

    def z_wait(src, dst, c, k):
        rcopy(src.at[kr(k)], dst.at[kr(k)], z1s.at[c, k], z1r.at[c, k], hk[k] * z.gs + p, t).wait_recv()

    def plane_send(src, dst, c, k):
        for d in (3, 1, 2):
            go(rcopy(src.at[in_block(k, qd[d])], dst.at[in_block(k, p)], p2s.at[c, k, d], p2r.at[c, k, d],
                     g * z.gs + qd[d], t))
        dst[in_block(k, p), :] = src[in_block(k, p), :]

    def plane_wait(src, dst, c, k):
        for d in (1, 2, 3):
            rcopy(src.at[in_block(k, qd[d])], dst.at[in_block(k, qd[d])], p2s.at[c, k, d], p2r.at[c, k, d],
                  g * z.gs + qd[d], t).wait_recv()

    def back_send(src, dst, c, k):
        for d in (3, 1, 2):
            go(rcopy(src.at[in_block(k, qd[d])], dst.at[in_block(k, p)], r3s.at[c, k, d], r3r.at[c, k, d],
                     g * z.gs + qd[d], t))
        dst[in_block(k, p), :] = src[in_block(k, p), :]

    def back_wait(src, dst, c, k):
        for d in (1, 2, 3):
            rcopy(src.at[in_block(k, qd[d])], dst.at[in_block(k, qd[d])], r3s.at[c, k, d], r3r.at[c, k, d],
                  g * z.gs + qd[d], t).wait_recv()

    def pair(src, dst, ss, rs):
        return rcopy(src, dst, ss, rs, e, other)

    lane = lanes_of((z.rows, z.rl))
    ll, lb = lane % per, lane // per
    eye = lanes_of((z.rows, z.rows), 0) == lanes_of((z.rows, z.rows), 1)

    def column(row):
        return jnp.sum(jnp.where(eye, row.astype(F32), 0.0), axis=1, keepdims=True).astype(jnp.int32)

    def before(n):
        return (lanes_of((n, n), 1) < lanes_of((n, n), 0)).astype(F32).astype(BF)

    loads[0].wait()
    r0, r1_ = column(routes_ref[0:1, :]), column(routes_ref[1:2, :])
    chosen = (ll == r0) | (ll == r1_)
    low = (ll - z.experts) * z.gs
    is_group = (ll >= z.experts) & (ll < z.experts + z.groups)
    in_group = is_group & (r0 >= low) & (r0 < low + z.gs)
    grank = mm(before(z.rows), in_group.astype(F32).astype(BF))
    grank = jnp.where(in_group, grank, -1.0).astype(BF)
    er, el = lanes_of((z.rl, z.r1), 0) - z.experts, lanes_of((z.rl, z.r1), 1)
    kk = el // gr
    want = jnp.where(kk == 0, hk[0], jnp.where(kk == 1, hk[1], jnp.where(kk == 2, hk[2], hk[3])))
    expand = (er == want).astype(F32).astype(BF)
    place = (lanes_of((z.rows, z.r1)) % gr).astype(F32)
    s_f = (mm(grank, expand) == place).astype(F32)
    s_mat[...] = s_f.astype(BF)
    s_tr[...] = s_f.T.astype(BF)
    s1m[...] = mm(s_tr[...], jnp.where(chosen & (lb == 0), 1.0, 0.0).astype(BF)).astype(BF)
    r1m[kr(0), :] = s1m[kr(0), :]

    def fill(c):
        j = c % nj
        src = tok_ref if c < nj else cot_ref
        s1[c] = mm(s_tr[...], src[:, cols(t, j)]).astype(BF)
        r1[c, kr(0), :] = s1[c, kr(0), :]

    loads[1].wait()
    fill(0)
    pl.semaphore_wait(barrier, 7)
    for k in far:
        z_send(s1m, r1m, ng, k)
    for k in (1, 2):
        z_send(s1.at[0], r1.at[0], 0, k)
    for c in range(1, nj):
        fill(c)
        for k in (1, 2):
            z_send(s1.at[c], r1.at[c], c, k)

    def make_t(k):
        if k:
            z_wait(s1m, r1m, ng, k)
        vals = r1m[kr(k), :]
        ln = lanes_of((gr, z.rl))
        member = (vals.astype(F32) > 0.0) & (ln < z.experts)
        rank = mm(before(gr), member.astype(F32).astype(BF))
        rank = jnp.where(member, rank, -1.0).astype(BF)
        sr, sc = lanes_of((z.rl, blk), 0) - g * z.gs, lanes_of((z.rl, blk), 1)
        spread = (sr == sc // cap).astype(F32).astype(BF)
        spot = (lanes_of((gr, blk)) % cap).astype(F32)
        tf = (mm(rank, spread) == spot).astype(F32)
        t_mat[k] = tf.astype(BF)
        t_tr[k] = tf.T.astype(BF)

    def op_a(k, c):
        if k:
            z_wait(s1.at[c], r1.at[c], c, k)
        s2[c, kb(k), :] = mm(t_tr[k], r1[c, kr(k), :]).astype(BF)
        plane_send(s2.at[c], x2.at[c], c, k)

    def op_am(k):
        if k:
            z_wait(s1w, r1w, ng + 1, k)
        s2m[kb(k), :] = mm(t_tr[k], r1w[kr(k), :]).astype(BF)
        plane_send(s2m, x2m, ng, k)

    make_t(0)
    for c in range(nj):
        op_a(0, c)

    rc_ref[...] = jnp.zeros_like(rc_ref)
    loads[2].wait()
    loads[3].wait()
    for b in range(z.rl // per):
        rc_ref[b * per : b * per + z.experts, :] = rexp_ref[...]
        rc_ref[b * per + z.experts : b * per + z.experts + z.groups, :] = rgrp_ref[...]
    expd = jnp.exp(mm(tok_ref[...], rc_ref[...], 1, 1))
    gexp = jnp.where(is_group, expd, 0.0)
    gprob = gexp / jnp.sum(jnp.where(lb == 0, gexp, 0.0), axis=1, keepdims=True)
    picked = jnp.sum(jnp.where(in_group & (lb == 0), gprob, 0.0), axis=1, keepdims=True)
    pexp = jnp.where(chosen, expd, 0.0)
    paired = pexp / jnp.sum(jnp.where(lb == 0, pexp, 0.0), axis=1, keepdims=True)
    both = paired + gprob
    upper = both.astype(BF).astype(F32)
    meta = jnp.where(lb == 1, picked * paired, jnp.where(lb == 2, upper, jnp.where(lb == 3, both - upper, 0.0)))
    s1w[...] = mm(s_tr[...], meta.astype(BF)).astype(BF)
    r1w[kr(0), :] = s1w[kr(0), :]
    for k in far:
        z_send(s1w, r1w, ng + 1, k)
    loads[4].wait()
    for c in range(nj, ng):
        fill(c)
        for k in (1, 2):
            z_send(s1.at[c], r1.at[c], c, k)
        op_a(0, c)
    for c in range(ng):
        z_send(s1.at[c], r1.at[c], c, 3)
    op_am(0)

    def op_b(k, c):
        plane_wait(s2.at[c], x2.at[c], c, k)
        go(pair(x2.at[c, kb(k)], y2.at[c, kb(k)], fs.at[c, k], fr.at[c, k]))

    def y_wait(k, c):
        pair(x2.at[c, kb(k)], y2.at[c, kb(k)], fs.at[c, k], fr.at[c, k]).wait_recv()

    def op_c1(k):
        ga = ua = None
        for half, xs in ((t, x2), (other, y2)):
            for j in range(nj):
                if xs is y2:
                    y_wait(k, j)
                x, at = xs[j, kb(k), :], cols(half, j)
                a, b = mm(x, gate_ref[at, :]), mm(x, up_ref[at, :])
                ga, ua = (a, b) if ga is None else (ga + a, ua + b)
        gacc[...] = ga
        uacc[...] = ua

    lane2 = lanes_of((blk, z.rl))

    def token_term(k, half, j):
        at = cols(half, j)
        return (
            mm(dcat[kb(k), : z.ff], gate_ref[at, :], 1, 1) + mm(dcat[kb(k), z.ff :], up_ref[at, :], 1, 1)
        ).astype(BF)

    def op_c2(k):
        pulled = None
        for half, xs in ((t, x2), (other, y2)):
            for j in range(nj):
                if xs is y2:
                    y_wait(k, nj + j)
                a = mm(xs[nj + j, kb(k), :], down_ref[:, cols(half, j)], 1, 1)
                pulled = a if pulled is None else pulled + a
        plane_wait(s2m, x2m, ng, k)
        scale = jnp.sum(jnp.where(lane2 == per + e, x2m[kb(k), :].astype(F32), 0.0), axis=1, keepdims=True)
        wcol[kb(k), :] = jnp.broadcast_to(scale, (blk, z.rl))
        gate_pre, up_pre = gacc[...], uacc[...]
        sig = 1.0 / (1.0 + jnp.exp(-gate_pre))
        silu = gate_pre * sig
        hidden = (silu * up_pre).astype(BF)
        hid[kb(k), :] = hidden
        wp[kb(k), :] = jnp.broadcast_to(
            jnp.sum(pulled * hidden.astype(F32), axis=1, keepdims=True), (blk, z.rl)
        )
        go(pair(wp.at[kb(k)], wpr.at[kb(k)], ws.at[k], wr.at[k]))
        dh = scale * pulled
        dcat[kb(k), : z.ff] = (dh * up_pre * sig * (1.0 + gate_pre * (1.0 - sig))).astype(BF)
        dcat[kb(k), z.ff :] = (dh * silu).astype(BF)
        for j in range(nj):
            pts[j, kb(k), :] = token_term(k, other, j)
            go(pair(pts.at[j, kb(k)], ptr.at[j, kb(k)], ptsm.at[j, k], ptrm.at[j, k]))

    def op_d(k):
        pair(wp.at[kb(k)], wpr.at[kb(k)], ws.at[k], wr.at[k]).wait_recv()
        wsum = wp[kb(k), :] + wpr[kb(k), :]
        s3m[kb(k), :] = jnp.where(lane2 == e, wsum, 0.0).astype(BF)
        back_send(s3m, r3m, nj, k)
        for j in range(nj):
            mine = token_term(k, t, j)
            pair(pts.at[j, kb(k)], ptr.at[j, kb(k)], ptsm.at[j, k], ptrm.at[j, k]).wait_recv()
            s3[j, kb(k), :] = (mine.astype(F32) + ptr[j, kb(k), :].astype(F32)).astype(BF)
            back_send(s3.at[j], r3.at[j], j, k)

    def home_copy(j, k):
        return rcopy(s4.at[j, kr(k)], r4.at[j, kr(k)], r4s.at[j, k], r4r.at[j, k], hk[k] * z.gs + p, t)

    lane3 = lanes_of((gr, z.rl))
    i1, i2 = lanes_of((z.rl, z.rl), 0), lanes_of((z.rl, z.rl), 1)
    fold = ((i2 < per) & ((i1 == 2 * per + i2) | (i1 == 3 * per + i2))).astype(F32).astype(BF)

    def op_f(k):
        vals = mm(r1w[kr(k), :], fold)
        pr = jnp.where(lane3 < z.experts, vals, 0.0)
        gp = jnp.where((lane3 >= z.experts) & (lane3 < z.experts + z.groups), vals, 0.0)
        here = lane3 == z.experts + g
        pk = jnp.sum(jnp.where(here, vals, 0.0), axis=1, keepdims=True)
        back_wait(s3m, r3m, nj, k)
        dw = mm(t_mat[k], r3m[kb(k), :])
        dpicked = jnp.sum(dw * pr, axis=1, keepdims=True)
        q = pk * dw
        dchosen = pr * (q - jnp.sum(pr * q, axis=1, keepdims=True))
        dgroup = (dpicked * pk) * (here.astype(F32) - gp)
        dgroup = jnp.where((lane3 >= z.experts) & (lane3 < z.experts + z.groups), dgroup, 0.0)
        dall = (dchosen + dgroup).astype(BF)
        dall_ref[kr(k), :] = dall
        for j in range(nj):
            back_wait(s3.at[j], r3.at[j], j, k)
            row = (mm(t_mat[k], r3[j, kb(k), :]) + mm(dall, rc_ref[:, cols(t, j)])).astype(BF)
            if k:
                s4[j, kr(k), :] = row
                go(home_copy(j, k))
            else:
                r4[j, kr(k), :] = row

    sub = min(cc, 256)
    ns = cc // sub
    ones_ff = jnp.ones((16, z.ff), BF)
    ones_sub = jnp.ones((16, sub), BF)

    def gate_up_grads(xs, half, i):
        j, o = i // ns, (i % ns) * sub
        at = pl.ds(pl.multiple_of(half * z.cw + i * sub, sub), sub)
        total = mm(xs[j, :, o : o + sub], dcat[...], 0, 0)
        gate_out[at, :] = total[:, : z.ff].astype(BF)
        up_out[at, :] = total[:, z.ff :].astype(BF)
        square = (total * total).astype(BF)
        sq[0:1, at] = mm(ones_ff, square[:, : z.ff], 1, 1)[0:1]
        sq[1:2, at] = mm(ones_ff, square[:, z.ff :], 1, 1)[0:1]

    def down_grads(xs, half, i):
        j, o = i // ns, (i % ns) * sub
        at = pl.ds(pl.multiple_of(half * z.cw + i * sub, sub), sub)
        scaled = (wcol[:, 0:1] * xs[nj + j, :, o : o + sub].astype(F32)).astype(BF)
        total = mm(hid[...], scaled, 0, 0)
        down_out[:, at] = total.astype(BF)
        return mm(ones_sub, (total * total).astype(BF), 1, 1)[0:1]

    for i in (5, 6, 7):
        loads[i].wait()

    def all_a(k, cs):
        for c in cs:
            op_a(k, c)

    def all_b(k, cs):
        for c in cs:
            op_b(k, c)

    tk, ct = range(nj), range(nj, ng)
    make_t(1)
    for c in range(ng):
        op_a(1, c)
        op_b(0, c)
    op_am(1)
    op_c1(0)
    op_c2(0)
    all_b(1, tk)
    op_d(0)
    all_b(1, ct)
    make_t(2)
    all_a(2, tk)
    op_c1(1)
    op_c2(1)
    op_f(0)
    all_a(2, ct)
    op_am(2)
    op_d(1)
    all_b(2, tk)
    make_t(3)
    op_c1(2)
    op_f(1)
    all_b(2, ct)
    op_c2(2)
    op_d(2)
    all_a(3, tk)
    op_f(2)
    all_a(3, ct)
    op_am(3)
    all_b(3, tk)
    op_c1(3)
    all_b(3, ct)
    op_c2(3)
    op_d(3)
    n_piece = z.cw // sub
    for i in range(n_piece):
        gate_up_grads(x2, t, i)
    op_f(3)

    dterm = dall_ref[:, : z.rw]
    half_chunks = z.cw // z.ch
    for j in range(nj):
        full = mm(dterm, r1[j], 0, 0)
        for i in range(cc // z.ch):
            n = j * (cc // z.ch) + i
            term[n % z.gs, n // z.gs] = full[:, i * z.ch : (i + 1) * z.ch]

    def term_a(d):
        return rcopy(term.at[qd[d]], tra.at[d], tas.at[d], tar.at[d], g * z.gs + qd[d], t)

    for d in far:
        go(term_a(d))
    per_core = half_chunks // z.gs

    for i in range(n_piece):
        gate_up_grads(y2, other, i)
    sq_copy = go(pair(sq, sqr, ms.at[1], mr.at[1]))
    for d in far:
        term_a(d).wait_recv()
    tsa[...] = term[p] + tra[1] + tra[2] + tra[3]
    home_core = g // per_core

    def term_b(k):
        return rcopy(tsa.at[hk[k] % per_core], trb.at[k], tbs.at[k], tbr.at[k], hk[k] * z.gs + p, t)

    for k in far:

        @pl.when(hk[k] // per_core == t)
        def _():
            term_b(k).start()

    dsq = jnp.zeros((1, z.ff), F32)
    for i in range(n_piece):
        dsq += down_grads(x2, t, i)
    for i in range(n_piece):
        dsq += down_grads(y2, other, i)
    dsq_out[...] = dsq

    t_pair = pair(tsum, tsumr, ms.at[2], mr.at[2])

    @pl.when(home_core == t)
    def _():
        for k in far:
            term_b(k).wait_recv()
        tsum[...] = tsa[g % per_core] + trb[1] + trb[2] + trb[3]
        t_pair.start()
        rout_out[...] = tsum[...]

    for j in range(nj):
        for k in far:
            home_copy(j, k).wait_recv()
        tg_out[:, j * cc : (j + 1) * cc] = mm(s_mat[...], r4[j]).astype(BF)
    sq_copy.wait_recv()
    gsq_out[...] = sq[0:1, :] + sqr[0:1, :]
    usq_out[...] = sq[1:2, :] + sqr[1:2, :]

    @pl.when(home_core != t)
    def _():
        t_pair.wait_recv()
        rout_out[...] = tsumr[...]

    @pl.when(home_core == t)
    def _():
        t_pair.wait_send()

    for k in far:

        @pl.when(hk[k] // per_core == t)
        def _():
            term_b(k).wait_send()

    for cp in sends:
        cp.wait_send()


def finish(
    z, gate_in, up_in, down_in, tg_in, gsq_in, usq_in, dsq_in, rout_in,
    gate_out, up_out, down_out, tg_out, gsq_out, usq_out, dsq_out, reg_out, rgg_out, rows_out, sem,
):
    copies = []
    pairs = (
        (gate_in, gate_out), (up_in, up_out), (down_in, down_out), (tg_in, tg_out),
        (gsq_in, gsq_out), (usq_in, usq_out), (dsq_in, dsq_out),
    )
    for i, (src, dst) in enumerate(pairs):
        cp = pltpu.make_async_copy(src, dst, sem.at[i])
        cp.start()
        copies.append(cp)
    half = z.ch // 2
    both = rout_in[...]
    mine = jnp.where(lax.axis_index("tp") == 0, both[:, :half], both[:, half:])
    reg = mine[: z.experts]
    rgg = mine[z.experts : z.experts + z.groups]
    reg_out[...] = reg
    rgg_out[...] = rgg
    rows_out[...] = jnp.sum(reg * reg, axis=0, keepdims=True) + jnp.sum(rgg * rgg, axis=0, keepdims=True)
    for cp in copies:
        cp.wait()


def by_source(z):
    return (
        z.reduce_here and z.groups == 4 and z.gs == 4 and z.cap % 16 == 0 and z.gr % 16 == 0
        and z.experts + z.groups <= z.rl // 4 and z.cw % 512 == 0 and (z.cw // z.ch) % z.gs == 0
    )


def run_sourced(z, outs, tokens, cotangent, routes, router_group, router_expert, gate_proj, up_proj, down_proj):
    z.nj = 2
    z.cc = z.cw // z.nj
    z.blk = z.gs * z.cap
    z.per = z.rl // 4
    nj, ng, cc = z.nj, 2 * z.nj, z.cc
    V = pltpu.VMEM
    args = (tokens, cotangent, routes.T, router_expert.T, router_group.T, gate_proj[0], up_proj[0], down_proj[0])
    hb = z.cw // z.ch // z.gs
    scratch = [V(a.shape, a.dtype) for a in args] + [
        V((z.rl, z.width), BF), V((z.rows, z.r1), BF), V((z.r1, z.rows), BF),
        V((z.groups, z.gr, z.blk), BF), V((z.groups, z.blk, z.gr), BF),
        V((z.r1, z.rl), BF), V((z.r1, z.rl), BF), V((z.r1, z.rl), BF), V((z.r1, z.rl), BF),
        V((ng, z.r1, cc), BF), V((ng, z.r1, cc), BF),
        V((z.pairs, z.rl), BF), V((z.pairs, z.rl), BF),
        V((ng, z.pairs, cc), BF), V((ng, z.pairs, cc), BF), V((ng, z.pairs, cc), BF),
        V((z.blk, z.ff), F32), V((z.blk, z.ff), F32),
        V((z.pairs, 2 * z.ff), BF), V((z.pairs, z.ff), BF), V((z.pairs, z.rl), F32),
        V((z.pairs, z.rl), F32), V((z.pairs, z.rl), F32),
        V((nj, z.pairs, cc), BF), V((nj, z.pairs, cc), BF),
        V((z.pairs, z.rl), BF), V((z.pairs, z.rl), BF),
        V((nj, z.pairs, cc), BF), V((nj, z.pairs, cc), BF),
        V((nj, z.r1, cc), BF), V((nj, z.r1, cc), BF), V((z.r1, z.rl), BF),
        V((2, z.width), F32), V((2, z.width), F32),
        V((z.gs, hb, z.rw, z.ch), F32), V((z.gs, hb, z.rw, z.ch), F32), V((hb, z.rw, z.ch), F32),
        V((z.groups, z.rw, z.ch), F32), V((z.rw, z.ch), F32), V((z.rw, z.ch), F32),
    ]
    D = pltpu.SemaphoreType.DMA
    both = [
        (ng + 2, 4), (ng + 1, 4, 4), (ng, 4), (4,), (nj, 4), (nj + 1, 4, 4), (nj, 4), (3,), (4,), (4,),
    ]
    sems = [D((len(args),))]
    for s in both:
        sems += [D(s), D(s)]
    spec = pl.BlockSpec(memory_space=pltpu.VMEM)
    return pl.pallas_call(
        functools.partial(sourced, z),
        out_shape=[jax.ShapeDtypeStruct(s, d) for s, d in outs],
        in_specs=[pl.BlockSpec(memory_space=pltpu.HBM)] * len(args),
        out_specs=[spec] * len(outs),
        scratch_shapes=scratch + sems,
        compiler_params=pltpu.CompilerParams(
            collective_id=0, has_side_effects=True, vmem_limit_bytes=50 * 2**20
        ),
    )(*args)


def run_wide(z, outs, tokens, cotangent, routes, router_group, router_expert, gate_proj, up_proj, down_proj):
    h, nc, cc = z.half_chunks, z.nc, z.cc
    V = pltpu.VMEM
    chd = z.ch if z.reduce_here else 128
    scratch = [
        V((z.rl, z.width), BF), V((z.r1, z.rl), BF), V((z.r1, z.rl), BF),
        V((z.rows, z.r1), BF), V((z.r1, z.pairs), BF),
        V((z.r1, z.rl), BF), V((z.r1, z.rl), BF),
        V((nc, z.r1, cc), BF), V((nc, z.r1, cc), BF),
        V((z.pairs, z.rl), BF), V((z.pairs, z.rl), BF),
        V((nc, z.pairs, cc), BF), V((nc, z.pairs, cc), BF),
        V((8, 128), BF), V((nc, z.pairs, cc), BF),
        V((z.pairs, z.ff), F32), V((z.pairs, z.ff), F32), V((z.pairs, z.ff), F32),
        V((z.pairs, 2 * z.ff), BF), V((z.pairs, z.ff), BF), V((z.pairs, 128), F32),
        V((z.pairs, 128), F32), V((z.pairs, 128), F32),
        V((h, z.pairs, cc), BF), V((h, z.pairs, cc), BF), V((h, z.pairs, cc), BF),
        V((z.pairs, z.rl), BF), V((z.pairs, z.rl), BF),
        V((h, z.pairs, cc), BF), V((h, z.pairs, cc), BF),
        V((z.r1, z.rl), BF), V((z.r1, z.rl), BF),
        V((h, z.r1, cc), BF), V((h, z.r1, cc), BF),
        V((2, z.width), F32), V((2, z.width), F32),
        V((z.n_ep, z.rw, chd), F32), V((z.n_ep // 2, z.rw, chd), F32),
        V((z.rw, chd), F32), V((z.rw, chd), F32),
    ]
    D = pltpu.SemaphoreType.DMA
    sems = [
        D((nc + 2, z.groups)), D((nc + 2, z.groups)), D((nc + 1, z.gs)), D((nc + 1, z.gs)),
        D((nc, z.gs)), D((nc, z.gs)), D((h,)), D((h,)),
        D((h + 1, z.gs)), D((h + 1, z.gs)), D((h + 1, z.groups)), D((h + 1, z.groups)),
        D((3,)), D((3,)), D((z.n_ep // 2,)), D((z.n_ep // 2,)),
    ]
    spec = pl.BlockSpec(memory_space=pltpu.VMEM)
    return pl.pallas_call(
        functools.partial(kernel, z),
        out_shape=[jax.ShapeDtypeStruct(s, d) for s, d in outs],
        in_specs=[spec] * 8,
        out_specs=[spec] * len(outs),
        scratch_shapes=scratch + sems,
        compiler_params=pltpu.CompilerParams(
            collective_id=0, has_side_effects=True, vmem_limit_bytes=44 * 2**20
        ),
    )(tokens, cotangent, routes.T, router_expert.T, router_group.T, gate_proj[0], up_proj[0], down_proj[0])


def body(axes, tokens, cotangent, routes, router_group, router_expert, gate_proj, up_proj, down_proj):
    z = sizes_of(axes, tokens, routes, router_group, router_expert, gate_proj)
    rout_shape = (z.rw, z.ch) if z.reduce_here else (min(z.rw, z.rl), z.width)
    outs = [
        ((z.rows, z.cw), BF), ((z.width, z.ff), BF), ((z.width, z.ff), BF), ((z.ff, z.width), BF),
        ((1, z.width), F32), ((1, z.width), F32), ((1, z.ff), F32), (rout_shape, F32),
    ]
    spec = pl.BlockSpec(memory_space=pltpu.VMEM)
    D = pltpu.SemaphoreType.DMA
    run = run_sourced if by_source(z) else run_wide
    tg, gate, up, down, gsq, usq, dsq, rout = run(
        z, outs, tokens, cotangent, routes, router_group, router_expert, gate_proj, up_proj, down_proj
    )
    if z.reduce_here:
        half = z.ch // 2
        shapes = [gate, up, down, tg, gsq, usq, dsq]
        anywhere = pl.BlockSpec(memory_space=pl.ANY)
        gate, up, down, tg, gsq, usq, dsq, reg, rgg, rrows = pl.pallas_call(
            functools.partial(finish, z),
            out_shape=[jax.ShapeDtypeStruct(a.shape, a.dtype) for a in shapes]
            + [jax.ShapeDtypeStruct((n, half), F32) for n in (z.experts, z.groups, 1)],
            in_specs=[spec] * 8,
            out_specs=[anywhere] * 7 + [spec] * 3,
            scratch_shapes=[D((7,))],
            compiler_params=pltpu.CompilerParams(vmem_limit_bytes=16 * 2**20),
        )(*shapes, rout)
        reg, rgg, rrows = reg.T, rgg.T, rrows[0]
    else:
        mine = lax.psum_scatter(rout.T, ("ep", "tp"), scatter_dimension=0, tiled=True)
        reg = mine[:, : z.experts]
        rgg = mine[:, z.experts : z.experts + z.groups]
        rrows = jnp.sum(reg * reg, axis=1) + jnp.sum(rgg * rgg, axis=1)
    return (tg, gate[None], up[None], down[None], gsq, usq, dsq, reg, rgg, rrows)


def solution(mesh):
    return jax.shard_map(
        functools.partial(body, dict(mesh.shape)),
        mesh=mesh,
        in_specs=(
            P("ep", None), P("ep", None), P("ep", None), P(), P(),
            P("ep", None, "tp"), P("ep", None, "tp"), P("ep", "tp", None),
        ),
        out_specs=(
            P("ep", "tp"), P("ep", None, "tp"), P("ep", None, "tp"), P("ep", "tp", None),
            P("ep", None), P("ep", None), P("ep", "tp"),
            P(("ep", "tp"), None), P(("ep", "tp"), None), P(("ep", "tp")),
        ),
        check_vma=False,
    )
```

```python
import functools

import jax
import jax.numpy as jnp
from jax import lax
from jax.experimental import pallas as pl
from jax.experimental.pallas import tpu as pltpu
from jax.sharding import PartitionSpec as P

MESH = pl.DeviceIdType.MESH
BF = jnp.bfloat16
F32 = jnp.float32


def mm(a, b, da=1, db=0):
    return lax.dot_general(a, b, (((da,), (db,)), ((), ())), preferred_element_type=F32)


def lanes_of(shape, dim=1):
    return lax.broadcasted_iota(jnp.int32, shape, dim)


class Sizes:
    pass


def sizes_of(mesh, tokens, routes, router_group, router_expert, gate_proj):
    z = Sizes()
    z.n_ep, z.n_tp = mesh["ep"], mesh["tp"]
    z.rows, z.width = tokens.shape
    z.top = routes.shape[1]
    z.groups, z.experts = router_group.shape[1], router_expert.shape[1]
    z.gs = z.experts // z.groups
    z.cap = z.rows // z.gs
    z.gr = z.gs * z.cap // z.top
    z.r1 = z.groups * z.gr
    z.sl = z.groups * z.cap
    z.pairs = z.gs * z.sl
    z.ff = gate_proj.shape[2]
    z.cw = z.width // z.n_tp
    z.half_chunks = 4
    z.nc = 2 * z.half_chunks
    z.cc = z.cw // z.half_chunks
    z.rl = -(-(z.experts + z.groups) // 128) * 128
    z.rw = -(-(z.experts + z.groups) // 8) * 8
    z.ch = z.width // z.n_ep
    z.reduce_here = z.ch % 128 == 0 and z.n_ep % 2 == 0
    assert z.experts == z.n_ep and z.n_tp == 2 and z.top == 2
    assert z.sl & (z.sl - 1) == 0 and z.gr & (z.gr - 1) == 0
    return z


def kernel(
    z, tok_ref, cot_ref, routes_ref, rexp_ref, rgrp_ref, gate_ref, up_ref, down_ref,
    tg_out, gate_out, up_out, down_out, gsq_out, usq_out, dsq_out, rout_out,
    rc_ref, s1w, r1w,
    s_mat, t_mat, s1m, r1m, s1, r1, s2m, x2m, s2, x2, y2m, y2,
    gacc, uacc, pacc, dcat, hid, wcol, wp, wpr, pts, ptr, pto,
    s3m, r3m, s3, r3, s4m, r4m, s4, r4, sq, sqr, term, trec, tsum, tsumr,
    z1s, z1r, p2s, p2r, fs, fr, ptsm, ptrm, r3s, r3r, r4s, r4r, ms, mr, ts, tr,
):
    e, t = lax.axis_index("ep"), lax.axis_index("tp")
    g, p = e // z.gs, e % z.gs
    other = 1 - t

    def rcopy(src, dst, ss, rs, ep, tp):
        return pltpu.make_async_remote_copy(
            src_ref=src, dst_ref=dst, send_sem=ss, recv_sem=rs,
            device_id=(ep, tp), device_id_type=MESH,
        )

    barrier = pltpu.get_barrier_semaphore()
    for d in range(1, z.n_ep):
        pl.semaphore_signal(
            barrier, inc=1, device_id=((e + d) % z.n_ep, t), device_id_type=MESH
        )
    pl.semaphore_signal(barrier, inc=1, device_id=(e, other), device_id_type=MESH)

    sends = []

    def grows(h):
        return pl.ds(pl.multiple_of(h * z.gr, z.gr), z.gr)

    def prows(q):
        return pl.ds(pl.multiple_of(q * z.sl, z.sl), z.sl)

    def group_send(src, dst, ss, rs, c):
        for d in range(1, z.groups):
            h = (g + d) % z.groups
            cp = rcopy(src.at[grows(h)], dst.at[grows(g)], ss.at[c, d], rs.at[c, d], h * z.gs + p, t)
            cp.start()
            sends.append(cp)
        dst[grows(g), :] = src[grows(g), :]

    def group_wait(src, dst, ss, rs, c):
        for d in range(1, z.groups):
            h = (g + z.groups - d) % z.groups
            rcopy(src.at[grows(h)], dst.at[grows(h)], ss.at[c, d], rs.at[c, d], h * z.gs + p, t).wait_recv()

    def plane_send(src, dst, ss, rs, c):
        for d in range(1, z.gs):
            q = (p + d) % z.gs
            cp = rcopy(src.at[prows(q)], dst.at[prows(p)], ss.at[c, d], rs.at[c, d], g * z.gs + q, t)
            cp.start()
            sends.append(cp)
        dst[prows(p), :] = src[prows(p), :]

    def plane_wait_one(src, dst, ss, rs, c, d):
        q = (p + z.gs - d) % z.gs
        rcopy(src.at[prows(q)], dst.at[prows(q)], ss.at[c, d], rs.at[c, d], g * z.gs + q, t).wait_recv()

    def plane_wait(src, dst, ss, rs, c):
        for d in range(1, z.gs):
            plane_wait_one(src, dst, ss, rs, c, d)

    def pair_send(src, dst, ss, rs):
        cp = rcopy(src, dst, ss, rs, e, other)
        cp.start()
        sends.append(cp)
        return cp

    lane = lanes_of((z.rows, z.rl))
    eye = lanes_of((z.rows, z.rows), 0) == lanes_of((z.rows, z.rows), 1)

    def column(row):
        return jnp.sum(jnp.where(eye, row.astype(F32), 0.0), axis=1, keepdims=True).astype(jnp.int32)

    r0, r1_ = column(routes_ref[0:1, :]), column(routes_ref[1:2, :])
    chosen = (lane == r0) | (lane == r1_)
    low = (lane - z.experts) * z.gs
    is_group = (lane >= z.experts) & (lane < z.experts + z.groups)
    in_group = is_group & (r0 >= low) & (r0 < low + z.gs)

    def before(n):
        return (lanes_of((n, n), 1) < lanes_of((n, n), 0)).astype(F32).astype(BF)

    ghot = in_group.astype(F32)
    grank = mm(before(z.rows), ghot.astype(BF))
    grank = jnp.where(in_group, grank, -1.0).astype(BF)
    er, el = lanes_of((z.rl, z.r1), 0) - z.experts, lanes_of((z.rl, z.r1), 1)
    expand = ((el >= er * z.gr) & (el < (er + 1) * z.gr)).astype(F32).astype(BF)
    place = (lanes_of((z.rows, z.r1)) & (z.gr - 1)).astype(F32)
    s_mat[...] = (mm(grank, expand) == place).astype(F32).astype(BF)

    s1m[...] = mm(s_mat[...], chosen.astype(F32).astype(BF), 0, 0).astype(BF)
    pl.semaphore_wait(barrier, z.n_ep)
    group_send(s1m, r1m, z1s, z1r, z.nc)

    def cols_at(half, k):
        return pl.ds(pl.multiple_of(half * z.cw + k * z.cc, z.cc), z.cc)

    for c in range(z.nc):
        src = tok_ref if c < z.half_chunks else cot_ref
        s1[c] = mm(s_mat[...], src[:, cols_at(t, c % z.half_chunks)], 0, 0).astype(BF)
        group_send(s1.at[c], r1.at[c], z1s, z1r, c)

    rc_ref[...] = jnp.zeros_like(rc_ref)
    rc_ref[0 : z.experts, :] = rexp_ref[...]
    rc_ref[z.experts : z.experts + z.groups, :] = rgrp_ref[...]
    expd = jnp.exp(mm(tok_ref[...], rc_ref[...], 1, 1))
    gexp = jnp.where(is_group, expd, 0.0)
    gprob = gexp / jnp.sum(gexp, axis=1, keepdims=True)
    picked = jnp.sum(jnp.where(in_group, gprob, 0.0), axis=1, keepdims=True)
    pexp = jnp.where(chosen, expd, 0.0)
    paired = pexp / jnp.sum(pexp, axis=1, keepdims=True)
    s1w[...] = mm(s_mat[...], (picked * paired).astype(BF), 0, 0).astype(BF)
    group_send(s1w, r1w, z1s, z1r, z.nc + 1)

    group_wait(s1m, r1m, z1s, z1r, z.nc)
    vals = r1m[...]
    lane1 = lanes_of((z.r1, z.rl))
    member = (vals.astype(F32) > 0.0) & (lane1 < z.experts)
    rank = mm(before(z.r1), member.astype(F32).astype(BF))
    rank = jnp.where(member, rank, -1.0).astype(BF)
    er, el = lanes_of((z.rl, z.pairs), 0) - g * z.gs, lanes_of((z.rl, z.pairs), 1)
    expand = ((el >= er * z.sl) & (el < (er + 1) * z.sl)).astype(F32).astype(BF)
    place = (lanes_of((z.r1, z.pairs)) & (z.sl - 1)).astype(F32)
    t_mat[...] = (mm(rank, expand) == place).astype(F32).astype(BF)

    def pack_two(c):
        group_wait(s1.at[c], r1.at[c], z1s, z1r, c)
        s2[c] = mm(t_mat[...], r1[c], 0, 0).astype(BF)
        plane_send(s2.at[c], x2.at[c], p2s, p2r, c)
        pair_send(x2.at[c, prows(p)], y2.at[c, prows(p)], fs.at[c, 0], fr.at[c, 0])

    def accumulate(x, half, c):
        if c < z.half_chunks:
            at = cols_at(half, c)
            gate_add, up_add = mm(x, gate_ref[at, :]), mm(x, up_ref[at, :])
            gacc[...] += gate_add
            uacc[...] += up_add
        else:
            pacc[...] += mm(x, down_ref[:, cols_at(half, c - z.half_chunks)], 1, 1)

    def land(c):
        for d in range(1, z.gs):
            plane_wait_one(s2.at[c], x2.at[c], p2s, p2r, c, d)
            q = (p + z.gs - d) % z.gs
            pair_send(x2.at[c, prows(q)], y2.at[c, prows(q)], fs.at[c, d], fr.at[c, d])
        accumulate(x2[c], t, c)

    def land_other(c):
        for d in range(z.gs):
            q = (p + z.gs - d) % z.gs
            rcopy(x2.at[c, prows(q)], y2.at[c, prows(q)], fs.at[c, d], fr.at[c, d], e, other).wait_recv()
        accumulate(y2[c], other, c)

    gacc[...] = jnp.zeros_like(gacc)
    uacc[...] = jnp.zeros_like(uacc)
    pacc[...] = jnp.zeros_like(pacc)
    for c in range(z.nc + 3):
        if c < z.nc:
            pack_two(c)
        if c == z.nc - 1:
            group_wait(s1w, r1w, z1s, z1r, z.nc + 1)
            s2m[...] = mm(t_mat[...], r1w[...], 0, 0).astype(BF)
            plane_send(s2m, x2m, p2s, p2r, z.nc)
        if 2 <= c < z.nc + 2:
            land(c - 2)
        if c >= 3:
            land_other(c - 3)
    plane_wait(s2m, x2m, p2s, p2r, z.nc)

    lane2 = lanes_of((z.pairs, z.rl))
    scale = jnp.sum(jnp.where(lane2 == e, x2m[...].astype(F32), 0.0), axis=1, keepdims=True)
    wcol[...] = jnp.broadcast_to(scale, wcol.shape)
    gate_pre, up_pre, pulled = gacc[...], uacc[...], pacc[...]
    sig = 1.0 / (1.0 + jnp.exp(-gate_pre))
    silu = gate_pre * sig
    hidden = (silu * up_pre).astype(BF)
    hid[...] = hidden
    wp[...] = jnp.broadcast_to(
        jnp.sum(pulled * hidden.astype(F32), axis=1, keepdims=True), wp.shape
    )
    w_copy = pair_send(wp, wpr, ms.at[0], mr.at[0])
    dh = scale * pulled
    dcat[:, : z.ff] = (dh * up_pre * sig * (1.0 + gate_pre * (1.0 - sig))).astype(BF)
    dcat[:, z.ff :] = (dh * silu).astype(BF)

    def token_term(half, k):
        at = cols_at(half, k)
        return (
            mm(dcat[:, : z.ff], gate_ref[at, :], 1, 1) + mm(dcat[:, z.ff :], up_ref[at, :], 1, 1)
        ).astype(BF)

    pt = []
    for k in range(z.half_chunks):
        pts[k] = token_term(other, k)
        pt.append(pair_send(pts.at[k], ptr.at[k], ptsm.at[k], ptrm.at[k]))
    w_copy.wait_recv()
    wsum = wp[:, 0:1] + wpr[:, 0:1]
    s3m[...] = jnp.where(lane2 == e, wsum, 0.0).astype(BF)
    plane_send(s3m, r3m, r3s, r3r, z.half_chunks)
    for k in range(z.half_chunks):
        pto[k] = token_term(t, k)
        pt[k].wait_recv()
        s3[k] = (pto[k].astype(F32) + ptr[k].astype(F32)).astype(BF)
        plane_send(s3.at[k], r3.at[k], r3s, r3r, k)

    ones_ff = jnp.ones((16, z.ff), BF)

    def gate_up_grads(xs, half, k):
        at = cols_at(half, k)
        total = mm(xs[k], dcat[...], 0, 0)
        gate_out[at, :] = total[:, : z.ff].astype(BF)
        up_out[at, :] = total[:, z.ff :].astype(BF)
        square = (total * total).astype(BF)
        sq[0:1, at] = mm(ones_ff, square[:, : z.ff], 1, 1)[0:1]
        sq[1:2, at] = mm(ones_ff, square[:, z.ff :], 1, 1)[0:1]

    def down_grads(xs, half, k):
        scaled = (wcol[:, 0:1] * xs[z.half_chunks + k].astype(F32)).astype(BF)
        total = mm(hid[...], scaled, 0, 0)
        down_out[:, cols_at(half, k)] = total.astype(BF)
        return mm(jnp.ones((16, z.cc), BF), (total * total).astype(BF), 1, 1)[0:1]

    def back_two(k):
        plane_wait(s3.at[k], r3.at[k], r3s, r3r, k)
        s4[k] = mm(t_mat[...], r3[k]).astype(BF)
        group_send(s4.at[k], r4.at[k], r4s, r4r, k)

    gate_up_grads(x2, t, 0)
    plane_wait(s3m, r3m, r3s, r3r, z.half_chunks)
    s4m[...] = mm(t_mat[...], r3m[...]).astype(BF)
    group_send(s4m, r4m, r4s, r4r, z.half_chunks)
    gate_up_grads(x2, t, 1)
    for k in range(z.half_chunks - 1):
        back_two(k)
        if k + 2 < z.half_chunks:
            gate_up_grads(x2, t, k + 2)
        else:
            gate_up_grads(y2, other, 0)

    group_wait(s4m, r4m, r4s, r4r, z.half_chunks)
    dw = mm(s_mat[...], r4m[...])
    dpicked = jnp.sum(dw * paired, axis=1, keepdims=True)
    q = picked * dw
    dchosen = paired * (q - jnp.sum(paired * q, axis=1, keepdims=True))
    dgroup = jnp.where(is_group, (dpicked * picked) * (ghot - gprob), 0.0)
    dall = (dchosen + dgroup).astype(BF)
    dterm = dall[:, : z.rw] if z.rw < z.rl else dall
    tcopies = []
    if z.reduce_here:
        full = mm(dterm, tok_ref[...], 0, 0)
        for i in range(z.n_ep):
            term[i] = full[:, i * z.ch : (i + 1) * z.ch]

        def term_copy(m):
            to = (e + 2 * m + t) % z.n_ep
            return rcopy(term.at[to], trec.at[m], ts.at[m], tr.at[m], to, t)

        @pl.when(t == 0)
        def _():
            trec[0] = term[e]

        @pl.when(t == 1)
        def _():
            term_copy(0).start()

        for m in range(1, z.n_ep // 2):
            term_copy(m).start()
    else:
        row = lanes_of((z.rows, z.rl), 0)[:, : dterm.shape[1]]
        mine = (row >= t * (z.rows // 2)) & (row < (t + 1) * (z.rows // 2))
        dterm = jnp.where(mine, dterm.astype(F32), 0.0).astype(BF)
        rout_out[...] = mm(dterm, tok_ref[...], 0, 0)

    back_two(z.half_chunks - 1)
    for k in range(1, z.half_chunks):
        gate_up_grads(y2, other, k)
    sq_copy = pair_send(sq, sqr, ms.at[1], mr.at[1])
    dsq = jnp.zeros((1, z.ff), F32)
    for k in range(z.half_chunks):
        dsq += down_grads(x2, t, k)

    if z.reduce_here:

        @pl.when(t == 1)
        def _():
            term_copy(0).wait_recv()

        for m in range(1, z.n_ep // 2):
            term_copy(m).wait_recv()
        acc = trec[0]
        for m in range(1, z.n_ep // 2):
            acc = acc + trec[m]
        tsum[...] = acc
        t_pair = pair_send(tsum, tsumr, ms.at[2], mr.at[2])
    for k in range(z.half_chunks):
        dsq += down_grads(y2, other, k)
    dsq_out[...] = dsq

    for k in range(z.half_chunks):
        group_wait(s4.at[k], r4.at[k], r4s, r4r, k)
        tg_out[:, k * z.cc : (k + 1) * z.cc] = (
            mm(s_mat[...], r4[k]) + mm(dall, rc_ref[:, cols_at(t, k)])
        ).astype(BF)
    sq_copy.wait_recv()
    gsq_out[...] = sq[0:1, :] + sqr[0:1, :]
    usq_out[...] = sq[1:2, :] + sqr[1:2, :]
    if z.reduce_here:
        t_pair.wait_recv()
        rout_out[...] = tsum[...] + tsumr[...]

        @pl.when(t == 1)
        def _():
            term_copy(0).wait_send()

        for m in range(1, z.n_ep // 2):
            term_copy(m).wait_send()
    for cp in sends:
        cp.wait_send()


def sourced(
    z, tok_h, cot_h, routes_h, rexp_h, rgrp_h, gate_h, up_h, down_h,
    tg_out, gate_out, up_out, down_out, gsq_out, usq_out, dsq_out, rout_out,
    tok_ref, cot_ref, routes_ref, rexp_ref, rgrp_ref, gate_ref, up_ref, down_ref,
    rc_ref, s_mat, s_tr, t_mat, t_tr, s1w, r1w, s1, r1, s2m, x2m, s2, x2, y2,
    gacc, uacc, pacc, gate_tr, up_tr, down_tr,
    dcat, hid, hid_tr, wp, wpr, pts, ptr, s3m, r3m, s3, r3, s4, r4, dall_ref,
    sq, sqr, term, tra, tsa, trb,
    ins, z1s, z1r, p2s, p2r, fs, fr, ws, wr, ptsm, ptrm, r3s, r3r, r4s, r4r, ms, mr, tas, tar, tbs, tbr,
):
    e, t = lax.axis_index("ep"), lax.axis_index("tp")
    g, p = e // z.gs, e % z.gs
    other = 1 - t
    hk = [g, g + 1 - 2 * (g % 2), 3 - g, (g + 2) % 4]
    qd = [p, p + 1 - 2 * (p % 2), (p + 2) % 4, 3 - p]
    inner = (g + 1) // 2 == 1
    nj, cc, gr, cap, blk, per = z.nj, z.cc, z.gr, z.cap, z.blk, z.per
    ng = 2 * nj
    far = (1, 2, 3)

    def rcopy(src, dst, ss, rs, ep, tp):
        return pltpu.make_async_remote_copy(
            src_ref=src, dst_ref=dst, send_sem=ss, recv_sem=rs,
            device_id=(ep, tp), device_id_type=MESH,
        )

    barrier = pltpu.get_barrier_semaphore()
    for k in far:
        pl.semaphore_signal(barrier, inc=1, device_id=(hk[k] * z.gs + p, t), device_id_type=MESH)
        pl.semaphore_signal(barrier, inc=1, device_id=(hk[k] * z.gs + p, other), device_id_type=MESH)
        pl.semaphore_signal(barrier, inc=1, device_id=(g * z.gs + qd[k], t), device_id_type=MESH)
    pl.semaphore_signal(barrier, inc=1, device_id=(e, other), device_id_type=MESH)

    loads = [
        pltpu.make_async_copy(a, b, ins.at[i])
        for i, (a, b) in enumerate((
            (routes_h, routes_ref), (tok_h, tok_ref), (rexp_h, rexp_ref), (rgrp_h, rgrp_ref),
            (cot_h, cot_ref), (gate_h, gate_ref), (up_h, up_ref), (down_h, down_ref),
        ))
    ]
    for cp in loads:
        cp.start()

    def kr(k, n=1):
        return pl.ds(k * gr, n * gr)

    def kb(k, n=1):
        return pl.ds(k * blk, n * blk)

    def in_block(k, q):
        return pl.ds(pl.multiple_of(k * blk + q * cap, cap), cap)

    def three(k):
        return pl.ds(k * blk, 3 * cap)

    def cols(half, j):
        return pl.ds(pl.multiple_of(half * z.cw + j * cc, cc), cc)

    def z_copy(src, dst, c, k):
        return rcopy(src.at[kr(k)], dst.at[kr(k)], z1s.at[c // ng], z1r.at[c, k - 1], hk[k] * z.gs + p, t)

    def spread(src, dst, ss, rs, k):
        for d in (3, 1, 2):
            rcopy(src.at[in_block(k, qd[d])], dst.at[in_block(k, p)], ss, rs, g * z.gs + qd[d], t).start()
        dst[in_block(k, p), :] = src[in_block(k, p), :]

    def gathered(src, dst, ss, rs, k):
        rcopy(src.at[three(k)], dst.at[three(k)], ss, rs, g * z.gs + qd[3], t).wait_recv()

    def line_out(src, dst, ss, rs, k, line):
        mine = pl.ds(pl.multiple_of((k * z.gs + p) * 16, 16), 16)
        src[k * 16 : (k + 1) * 16, :] = line.astype(BF)
        for d in (3, 1, 2):
            rcopy(src.at[pl.ds(k * 16, 16)], dst.at[mine], ss, rs, g * z.gs + qd[d], t).start()
        dst[mine, :] = src[k * 16 : (k + 1) * 16, :]

    def line_wait(dst, ss, rs, k):
        part = dst.at[pl.ds(k * z.gs * 16, 48)]
        rcopy(part, part, ss, rs, g * z.gs + qd[3], t).wait_recv()

    def line_column(dst, k):
        tiles = []
        for q in range(z.gs):
            at = (k * z.gs + q) * 16
            tiles += [dst[at : at + 16, :]] * (cap // 16)
        rows = jnp.concatenate(tiles, axis=0).astype(F32)
        r, c = lanes_of((blk, blk), 0), lanes_of((blk, blk), 1)
        return jnp.sum(jnp.where(c == p * cap + r % cap, rows, 0.0), axis=1, keepdims=True)

    def pair(src, dst, ss, rs):
        return rcopy(src, dst, ss, rs, e, other)

    lane = lanes_of((z.rows, z.rl))
    ll, lb = lane % per, lane // per
    eye = lanes_of((z.rows, z.rows), 0) == lanes_of((z.rows, z.rows), 1)

    def column(row):
        return jnp.sum(jnp.where(eye, row.astype(F32), 0.0), axis=1, keepdims=True).astype(jnp.int32)

    def before(n):
        r, c = lanes_of((n, n), 0), lanes_of((n, n), 1)
        return ((c < r) & (r // gr == c // gr)).astype(F32).astype(BF)

    def make_t(k, n):
        m = n * gr
        vals = r1w[kr(k, n), :]
        member = (vals.astype(F32) > 0.0) & (lanes_of((m, z.rl)) < z.experts)
        rank = mm(before(m), member.astype(F32).astype(BF))
        rank = jnp.where(member, rank, -1.0).astype(BF)
        sr, sc = lanes_of((z.rl, blk), 0) - g * z.gs, lanes_of((z.rl, blk), 1)
        expand = (sr == sc // cap).astype(F32).astype(BF)
        spot = (lanes_of((m, blk)) % cap).astype(F32)
        tf = (mm(rank, expand) == spot).astype(F32)
        t_mat[kr(k, n), :] = tf.astype(BF)
        t_tr[:, kr(k, n)] = tf.T.astype(BF)

    def t_rows(k):
        return t_mat[k * gr : (k + 1) * gr, :]

    def t_cols(k):
        return t_tr[:, k * gr : (k + 1) * gr]

    loads[0].wait()
    r0, r1_ = column(routes_ref[0:1, :]), column(routes_ref[1:2, :])
    chosen = (ll == r0) | (ll == r1_)
    low = (ll - z.experts) * z.gs
    is_group = (ll >= z.experts) & (ll < z.experts + z.groups)
    in_group = is_group & (r0 >= low) & (r0 < low + z.gs)
    tri = lanes_of((z.rows, z.rows), 1) < lanes_of((z.rows, z.rows), 0)
    grank = mm(tri.astype(F32).astype(BF), in_group.astype(F32).astype(BF))
    grank = jnp.where(in_group, grank, -1.0).astype(BF)
    er, el = lanes_of((z.rl, z.r1), 0) - z.experts, lanes_of((z.rl, z.r1), 1)
    kk = el // gr
    want = jnp.where(kk == 0, hk[0], jnp.where(kk == 1, hk[1], jnp.where(kk == 2, hk[2], hk[3])))
    expand = (er == want).astype(F32).astype(BF)
    place = (lanes_of((z.rows, z.r1)) % gr).astype(F32)
    s_f = (mm(grank, expand) == place).astype(F32)
    s_mat[...] = s_f.astype(BF)
    s_tr[...] = s_f.T.astype(BF)
    pick_mask = jnp.where(chosen & (lb == 0), 1.0, 0.0)
    r1w[kr(0), :] = mm(s_tr[kr(0), :], pick_mask.astype(BF)).astype(BF)

    def fill(c):
        j = c % nj
        src = tok_ref if c < nj else cot_ref
        s1[c] = mm(s_tr[...], src[:, cols(t, j)]).astype(BF)
        r1[c, kr(0), :] = s1[c, kr(0), :]

    def near_out(c):
        z_copy(s1.at[c], r1.at[c], c, 1).start()

        @pl.when(inner)
        def _():
            z_copy(s1.at[c], r1.at[c], c, 2).start()

    def op_a(k, c):
        if k:
            z_copy(s1.at[c], r1.at[c], c, k).wait_recv()
        s2[c, kb(k), :] = mm(t_cols(k), r1[c, kr(k), :]).astype(BF)
        spread(s2.at[c], x2.at[c], p2s.at[0], p2r.at[c, k], k)

    def op_am(k):
        er, ec = lanes_of((z.rl, blk), 0), lanes_of((z.rl, blk), 1)
        pick = (er == per + g * z.gs + ec // cap).astype(F32).astype(BF)
        weight = mm(r1w[kr(k), :], pick) * t_rows(k).astype(F32)
        line_out(s2m, x2m, p2s.at[1], p2r.at[ng, k], k, mm(jnp.ones((16, gr), BF), weight.astype(BF)))

    make_t(0, 1)
    loads[1].wait()
    fill(0)
    pl.semaphore_wait(barrier, 10)
    near_out(0)
    op_a(0, 0)
    for c in range(1, nj):
        fill(c)
        near_out(c)
        op_a(0, c)

    rc_ref[...] = jnp.zeros_like(rc_ref)
    loads[2].wait()
    loads[3].wait()
    for b in range(z.rl // per):
        rc_ref[b * per : b * per + z.experts, :] = rexp_ref[...]
        rc_ref[b * per + z.experts : b * per + z.experts + z.groups, :] = rgrp_ref[...]
    expd = jnp.exp(mm(tok_ref[...], rc_ref[...], 1, 1))
    gexp = jnp.where(is_group, expd, 0.0)
    gprob = gexp / jnp.sum(jnp.where(lb == 0, gexp, 0.0), axis=1, keepdims=True)
    picked = jnp.sum(jnp.where(in_group & (lb == 0), gprob, 0.0), axis=1, keepdims=True)
    pexp = jnp.where(chosen, expd, 0.0)
    paired = pexp / jnp.sum(jnp.where(lb == 0, pexp, 0.0), axis=1, keepdims=True)
    both = paired + gprob
    upper = both.astype(BF).astype(F32)
    meta = jnp.where(lb == 1, picked * paired, jnp.where(lb == 2, upper, jnp.where(lb == 3, both - upper, pick_mask)))
    s1w[...] = mm(s_tr[...], meta.astype(BF)).astype(BF)
    r1w[kr(0), :] = s1w[kr(0), :]
    for k in far:
        z_copy(s1w, r1w, ng, k).start()
    loads[4].wait()
    for c in range(nj, ng):
        fill(c)
        near_out(c)
        op_a(0, c)

    def op_s(k):
        for c in range(ng):
            z_copy(s1.at[c], r1.at[c], c, k).start()

    @pl.when(inner)
    def _():
        op_s(3)

    op_am(0)

    def op_t(k):
        z_copy(s1w, r1w, ng, k).wait_recv()
        make_t(k, 1)

    def relay(k, c):
        return pair(x2.at[c, kb(k)], y2.at[c, kb(k)], fs.at[0], fr.at[c, k])

    def op_b(k, c):
        gathered(s2.at[c], x2.at[c], p2s.at[0], p2r.at[c, k], k)
        relay(k, c).start()

    def op_c1(k, n):
        ga = ua = None
        for half, xs in ((t, x2), (other, y2)):
            for j in range(nj):
                if xs is y2:
                    for i in range(n):
                        relay(k + i, j).wait_recv()
                x, at = xs[j, kb(k, n), :], cols(half, j)
                a, b = mm(x, gate_ref[at, :]), mm(x, up_ref[at, :])
                ga, ua = (a, b) if ga is None else (ga + a, ua + b)
        gacc[kb(k, n), :] = ga
        uacc[kb(k, n), :] = ua

    def token_term(k, n, half, j):
        at = cols(half, j)
        return (
            mm(dcat[kb(k, n), : z.ff], gate_tr[:, at]) + mm(dcat[kb(k, n), z.ff :], up_tr[:, at])
        ).astype(BF)

    def w_pair(k, n):
        return pair(wp.at[kb(k, n)], wpr.at[kb(k, n)], ws.at[0], wr.at[k])

    def pt_pair(j, k, n):
        return pair(pts.at[j, kb(k, n)], ptr.at[j, kb(k, n)], ptsm.at[0], ptrm.at[j, k])

    def pull(k, n, js, pulled):
        for half, xs in ((t, x2), (other, y2)):
            for j in js:
                if xs is y2:
                    for i in range(n):
                        relay(k + i, nj + j).wait_recv()
                a = mm(xs[nj + j, kb(k, n), :], down_tr[cols(half, j), :])
                pulled = a if pulled is None else pulled + a
        return pulled

    def op_p(k, n):
        pacc[kb(k, n), :] = pull(k, n, range(nj - 1), None)

    def op_c2(k, n):
        pulled = pull(k, n, (nj - 1,), pacc[kb(k, n), :])
        for i in range(n):
            line_wait(x2m, p2s.at[1], p2r.at[ng, k + i], k + i)
        m = n * blk
        scale = jnp.concatenate([line_column(x2m, k + i) for i in range(n)], axis=0)
        gate_pre, up_pre = gacc[kb(k, n), :], uacc[kb(k, n), :]
        sig = 1.0 / (1.0 + jnp.exp(-gate_pre))
        silu = gate_pre * sig
        product = silu * up_pre
        hidden = product.astype(BF)
        hid[kb(k, n), :] = (scale * product).astype(BF)
        wp[kb(k, n), :] = jnp.broadcast_to(
            jnp.sum(pulled * hidden.astype(F32), axis=1, keepdims=True), (m, z.rl)
        )
        w_pair(k, n).start()
        dh = scale * pulled
        dcat[kb(k, n), : z.ff] = (dh * up_pre * sig * (1.0 + gate_pre * (1.0 - sig))).astype(BF)
        dcat[kb(k, n), z.ff :] = (dh * silu).astype(BF)
        for j in range(nj):
            pts[j, kb(k, n), :] = token_term(k, n, other, j)
            pt_pair(j, k, n).start()

    def op_d(k, n, out=False):
        mine = token_term(k, n, t, 0)
        w_pair(k, n).wait_recv()
        wsum = wp[kb(k, n), :] + wpr[kb(k, n), :]
        same = lanes_of((blk, blk), 0) == lanes_of((blk, blk), 1)
        for i in range(n):
            diag = jnp.where(same, wsum[i * blk : (i + 1) * blk, :blk], 0.0).astype(BF)
            line_out(s3m, r3m, r3s.at[1], r3r.at[nj, k + i], k + i, mm(jnp.ones((16, blk), BF), diag))
        for j in range(nj):
            if j:
                mine = token_term(k, n, t, j)
            pt_pair(j, k, n).wait_recv()
            s3[j, kb(k, n), :] = (mine.astype(F32) + ptr[j, kb(k, n), :].astype(F32)).astype(BF)
            if out:
                spread(s3.at[j], r3.at[j], r3s.at[0], r3r.at[j, k], k)

    def op_dr(k, n):
        op_d(k, n, True)

    def op_r(k):
        for j in range(nj):
            spread(s3.at[j], r3.at[j], r3s.at[0], r3r.at[j, k], k)

    def home_copy(j, k):
        return rcopy(s4.at[j, kr(k)], r4.at[j, kr(k)], r4s.at[0], r4r.at[j, k - 1], hk[k] * z.gs + p, t)

    lane3 = lanes_of((gr, z.rl))
    i1, i2 = lanes_of((z.rl, z.rl), 0), lanes_of((z.rl, z.rl), 1)
    fold = ((i2 < per) & ((i1 == 2 * per + i2) | (i1 == 3 * per + i2))).astype(F32).astype(BF)

    def op_e(k):
        vals = mm(r1w[kr(k), :], fold)
        g_lane = (lane3 >= z.experts) & (lane3 < z.experts + z.groups)
        pr = jnp.where(lane3 < z.experts, vals, 0.0)
        here = lane3 == z.experts + g
        pk = jnp.sum(jnp.where(here, vals, 0.0), axis=1, keepdims=True)
        line_wait(r3m, r3s.at[1], r3r.at[nj, k], k)
        lr, lc = lanes_of((blk, z.rl), 0), lanes_of((blk, z.rl), 1)
        dw = mm(t_rows(k), jnp.where(lc == g * z.gs + lr // cap, line_column(r3m, k), 0.0).astype(BF))
        dpicked = jnp.sum(dw * pr, axis=1, keepdims=True)
        q = pk * dw
        dchosen = pr * (q - jnp.sum(pr * q, axis=1, keepdims=True))
        dgroup = jnp.where(g_lane, (dpicked * pk) * (here.astype(F32) - vals), 0.0)
        dall_ref[kr(k), :] = (dchosen + dgroup).astype(BF)

    def op_f(k):
        dall = dall_ref[kr(k), :]
        for j in range(nj):
            gathered(s3.at[j], r3.at[j], r3s.at[0], r3r.at[j, k], k)
            row = (mm(t_rows(k), r3[j, kb(k), :]) + mm(dall, rc_ref[:, cols(t, j)])).astype(BF)
            if k:
                s4[j, kr(k), :] = row
                home_copy(j, k).start()
            else:
                r4[j, kr(k), :] = row

    sub = min(cc, 256)
    ns = cc // sub
    ones_ff = jnp.ones((16, z.ff), BF)
    ones_sub = jnp.ones((16, sub), BF)
    n_piece = z.cw // sub

    def gate_up_grads(i):
        half, xs = (t, x2) if i < n_piece else (other, y2)
        i = i % n_piece
        j, o = i // ns, (i % ns) * sub
        at = pl.ds(pl.multiple_of(half * z.cw + i * sub, sub), sub)
        total = mm(xs[j, :, o : o + sub], dcat[...], 0, 0)
        gate_out[at, :] = total[:, : z.ff].astype(BF)
        up_out[at, :] = total[:, z.ff :].astype(BF)
        square = (total * total).astype(BF)
        sq[0:1, at] = mm(ones_ff, square[:, : z.ff], 1, 1)[0:1]
        sq[1:2, at] = mm(ones_ff, square[:, z.ff :], 1, 1)[0:1]

    def down_grads(i):
        half, xs = (t, x2) if i < n_piece else (other, y2)
        i = i % n_piece
        j, o = i // ns, (i % ns) * sub
        at = pl.ds(pl.multiple_of(half * z.cw + i * sub, sub), sub)
        total = mm(hid_tr[...], xs[nj + j, :, o : o + sub])
        down_out[:, at] = total.astype(BF)
        return mm(ones_sub, (total * total).astype(BF), 1, 1)[0:1]

    loads[5].wait()
    gate_tr[...] = gate_ref[...].T
    loads[6].wait()
    up_tr[...] = up_ref[...].T
    loads[7].wait()
    down_tr[...] = down_ref[...].T

    per_core = z.cw // z.ch // z.gs
    home_core = g // per_core
    all_a = rcopy(term.at[pl.ds(0, 3)], tra, tas.at[0], tar.at[0], g * z.gs + qd[3], t)

    def term_b(k, core):
        return rcopy(tsa.at[hk[k] % per_core], trb.at[k], tbs.at[k, core], tbr.at[0], hk[k] * z.gs + p, core)

    t_pair = pair(tsa.at[g % per_core], trb.at[0], ms.at[1], mr.at[1])

    def op_x():
        dterm = dall_ref[:, : z.rw]
        for j in range(nj):
            full = mm(dterm, r1[j], 0, 0)
            for i in range(cc // z.ch):
                n = j * (cc // z.ch) + i
                term[n % z.gs, n // z.gs] = full[:, i * z.ch : (i + 1) * z.ch]
        for d in far:
            rcopy(term.at[qd[d]], tra.at[d - 1], tas.at[0], tar.at[0], g * z.gs + qd[d], t).start()

    def op_y():
        all_a.wait_recv()
        tsa[...] = term[p] + tra[0] + tra[1] + tra[2]
        for k in far:

            @pl.when(hk[k] // per_core == t)
            def _():
                for core in range(z.n_tp):
                    term_b(k, core).start()

        @pl.when(home_core == t)
        def _():
            t_pair.start()

    sq_copy = pair(sq, sqr, ms.at[0], mr.at[0])

    def op_h():
        hid_tr[...] = hid[...].T

    def op_q():
        sq_copy.start()

    def op_w(i):
        part = down_grads(i)
        dsq_out[...] = dsq_out[...] + part if i else part

    ops = {
        "t": op_t, "a": op_a, "m": op_am, "b": op_b, "c": op_c1, "p": op_p, "C": op_c2, "d": op_d, "D": op_dr, "r": op_r,
        "e": op_e, "f": op_f, "x": op_x, "y": op_y, "g": gate_up_grads, "h": op_h, "q": op_q, "w": op_w, "s": op_s,
    }

    def play(text):
        for word in " ".join(text).split():
            ops[word[0]](*(int(x) for x in word[1:]))

    @pl.when((g + 1) // 2 != 1)
    def _():
        play(z.order_end)

    @pl.when(inner)
    def _():
        play(z.order_mid)

    def home(j):
        for k in far:
            home_copy(j, k).wait_recv()
        tg_out[:, j * cc : (j + 1) * cc] = mm(s_mat[...], r4[j]).astype(BF)

    for j in range(nj):
        home(j)
    sq_copy.wait_recv()
    gsq_out[...] = sq[0:1, :] + sqr[0:1, :]
    usq_out[...] = sq[1:2, :] + sqr[1:2, :]
    got = trb.at[pl.ds(1, 3)]
    rcopy(got, got, tbs.at[1, 0], tbr.at[0], e, other).wait_recv()

    @pl.when(home_core == t)
    def _():
        rout_out[...] = tsa[g % per_core] + trb[1] + trb[2] + trb[3]

    @pl.when(home_core != t)
    def _():
        t_pair.wait_recv()
        rout_out[...] = trb[0] + trb[1] + trb[2] + trb[3]

    @pl.when(home_core == t)
    def _():
        t_pair.wait_send()

    for k in far:

        @pl.when(hk[k] // per_core == t)
        def _():
            for core in range(z.n_tp):
                term_b(k, core).wait_send()

    most, some = pl.ds(0, 3 * blk), pl.ds(0, 16 * 12)

    def left(src, dst, ss, rs):
        rcopy(src, dst, ss, rs, e, other).wait_send()

    left(s1.at[:, kr(1, 3)], r1.at[:, kr(1, 3)], z1s.at[0], z1r.at[0, 0])
    left(s1w.at[kr(1, 3)], r1w.at[kr(1, 3)], z1s.at[1], z1r.at[ng, 0])
    left(s2.at[:, most], x2.at[:, most], p2s.at[0], p2r.at[0, 0])
    left(x2m.at[some], x2m.at[some], p2s.at[1], p2r.at[ng, 0])
    left(x2, y2, fs.at[0], fr.at[0, 0])
    left(wp, wpr, ws.at[0], wr.at[0])
    left(pts, ptr, ptsm.at[0], ptrm.at[0, 0])
    left(s3.at[:, most], r3.at[:, most], r3s.at[0], r3r.at[0, 0])
    left(r3m.at[some], r3m.at[some], r3s.at[1], r3r.at[nj, 0])
    left(s4.at[:, kr(1, 3)], r4.at[:, kr(1, 3)], r4s.at[0], r4r.at[0, 0])
    all_a.wait_send()
    sq_copy.wait_send()


def finish(
    z, gate_in, up_in, down_in, tg_in, gsq_in, usq_in, dsq_in, rout_in,
    gate_out, up_out, down_out, tg_out, gsq_out, usq_out, dsq_out, reg_out, rgg_out, rows_out,
    reg_ref, rgg_ref, rows_ref, sem,
):
    pairs = [
        (gate_in, gate_out), (up_in, up_out), (down_in, down_out), (tg_in, tg_out),
        (gsq_in, gsq_out), (usq_in, usq_out), (dsq_in, dsq_out),
        (reg_ref, reg_out), (rgg_ref, rgg_out), (rows_ref, rows_out),
    ]
    copies = [pltpu.make_async_copy(src, dst, sem.at[i]) for i, (src, dst) in enumerate(pairs)]
    for cp in copies[:7]:
        cp.start()
    half = z.ch // 2
    both = rout_in[...]
    mine = jnp.where(lax.axis_index("tp") == 0, both[:, :half], both[:, half:])
    reg = mine[: z.experts]
    rgg = mine[z.experts : z.experts + z.groups]
    reg_ref[...] = reg
    rgg_ref[...] = rgg
    rows_ref[...] = jnp.sum(reg * reg, axis=0, keepdims=True) + jnp.sum(rgg * rgg, axis=0, keepdims=True)
    for cp in copies[7:]:
        cp.start()
    for cp in copies:
        cp.wait()


def by_source(z):
    return (
        z.reduce_here and z.groups == 4 and z.gs == 4 and z.cap % 16 == 0 and z.gr % 16 == 0
        and z.experts + z.groups <= z.rl // 4 and z.cw % 512 == 0 and (z.cw // z.ch) % z.gs == 0
    )


def run_sourced(z, outs, tokens, cotangent, routes, router_group, router_expert, gate_proj, up_proj, down_proj):
    z.nj = 2
    z.cc = z.cw // z.nj
    z.blk = z.gs * z.cap
    z.per = z.rl // 4
    z.order_end = (
        "t1 a10 b00 a11", "b01 a12 b02 a13", "b03 m1 b10 t3", "a30 b11 a31 b12", "a32 s2 s3 b13",
        "a33 m3 c02 p02", "C02 d02 t2 a20", "b30 b31 a21 c31", "a22 b32 p31 b33", "a23 m2 C31 b20",
        "b21 D31 r1 c21", "b22 p21 b23 C21", "D21 e3 f3 e1", "e0 g0 e2 x", "r0 f2 f1 g1", "g2 y g3 g4",
        "g5 g6 g7 q", "h w0 w1 f0", "w2 w3 w4 w5", "w6 w7",
    )
    z.order_mid = (
        "t1 a10 b00 a11", "b01 a12 b02 a13", "b03 m1 t2 a20", "a21 a22 a23 m2", "b10 b11 c02 b12",
        "p02 b13 C02 d02", "r1 b20 b21 c21", "b22 p21 b23 t3", "a30 a31 C21 a32", "a33 m3 D21 e0",
        "e1 f1 b30 b31", "c31 b32 p31 b33", "C31 e2 f2 D31", "g0 g1 g2 g3", "e3 x r0 f3", "g4 g5 g6 g7",
        "q h y w0", "w1 w2 f0 w3", "w4 w5 w6 w7",
    )
    nj, ng, cc = z.nj, 2 * z.nj, z.cc
    V = pltpu.VMEM
    args = (tokens, cotangent, routes.T, router_expert.T, router_group.T, gate_proj[0], up_proj[0], down_proj[0])
    hb = z.cw // z.ch // z.gs
    scratch = [V(a.shape, a.dtype) for a in args] + [
        V((z.rl, z.width), BF), V((z.rows, z.r1), BF), V((z.r1, z.rows), BF),
        V((z.r1, z.blk), BF), V((z.blk, z.r1), BF),
        V((z.r1, z.rl), BF), V((z.r1, z.rl), BF),
        V((ng, z.r1, cc), BF), V((ng, z.r1, cc), BF),
        V((16 * 4, z.blk), BF), V((16 * 4 * z.gs, z.blk), BF),
        V((ng, z.pairs, cc), BF), V((ng, z.pairs, cc), BF), V((ng, z.pairs, cc), BF),
        V((z.pairs, z.ff), F32), V((z.pairs, z.ff), F32), V((z.pairs, z.ff), F32),
        V((z.ff, z.width), BF), V((z.ff, z.width), BF), V((z.width, z.ff), BF),
        V((z.pairs, 2 * z.ff), BF), V((z.pairs, z.ff), BF), V((z.ff, z.pairs), BF),
        V((z.pairs, z.rl), F32), V((z.pairs, z.rl), F32),
        V((nj, z.pairs, cc), BF), V((nj, z.pairs, cc), BF),
        V((16 * 4, z.blk), BF), V((16 * 4 * z.gs, z.blk), BF),
        V((nj, z.pairs, cc), BF), V((nj, z.pairs, cc), BF),
        V((nj, z.r1, cc), BF), V((nj, z.r1, cc), BF), V((z.r1, z.rl), BF),
        V((2, z.width), F32), V((2, z.width), F32),
        V((z.gs, hb, z.rw, z.ch), F32), V((z.gs - 1, hb, z.rw, z.ch), F32), V((hb, z.rw, z.ch), F32),
        V((z.groups, z.rw, z.ch), F32),
    ]
    D = pltpu.SemaphoreType.DMA
    sems = [D((len(args),))] + [
        D(s) for s in (
            (2,), (ng + 1, 3), (2,), (ng + 1, 4), (1,), (ng, 4), (1,), (4,), (1,), (nj, 4),
            (2,), (nj + 1, 4), (1,), (nj, 3), (2,), (2,), (1,), (1,), (4, 2), (1,),
        )
    ]
    spec = pl.BlockSpec(memory_space=pltpu.VMEM)
    return pl.pallas_call(
        functools.partial(sourced, z),
        out_shape=[pltpu.VMEM(s, d) for s, d in outs],
        in_specs=[pl.BlockSpec(memory_space=pltpu.HBM)] * len(args),
        out_specs=[spec] * len(outs),
        scratch_shapes=scratch + sems,
        compiler_params=pltpu.CompilerParams(
            collective_id=0, has_side_effects=True, vmem_limit_bytes=44 * 2**20
        ),
    )(*[pltpu.with_memory_space_constraint(a, pltpu.HBM) for a in args])


def run_wide(z, outs, tokens, cotangent, routes, router_group, router_expert, gate_proj, up_proj, down_proj):
    h, nc, cc = z.half_chunks, z.nc, z.cc
    V = pltpu.VMEM
    chd = z.ch if z.reduce_here else 128
    scratch = [
        V((z.rl, z.width), BF), V((z.r1, z.rl), BF), V((z.r1, z.rl), BF),
        V((z.rows, z.r1), BF), V((z.r1, z.pairs), BF),
        V((z.r1, z.rl), BF), V((z.r1, z.rl), BF),
        V((nc, z.r1, cc), BF), V((nc, z.r1, cc), BF),
        V((z.pairs, z.rl), BF), V((z.pairs, z.rl), BF),
        V((nc, z.pairs, cc), BF), V((nc, z.pairs, cc), BF),
        V((8, 128), BF), V((nc, z.pairs, cc), BF),
        V((z.pairs, z.ff), F32), V((z.pairs, z.ff), F32), V((z.pairs, z.ff), F32),
        V((z.pairs, 2 * z.ff), BF), V((z.pairs, z.ff), BF), V((z.pairs, 128), F32),
        V((z.pairs, 128), F32), V((z.pairs, 128), F32),
        V((h, z.pairs, cc), BF), V((h, z.pairs, cc), BF), V((h, z.pairs, cc), BF),
        V((z.pairs, z.rl), BF), V((z.pairs, z.rl), BF),
        V((h, z.pairs, cc), BF), V((h, z.pairs, cc), BF),
        V((z.r1, z.rl), BF), V((z.r1, z.rl), BF),
        V((h, z.r1, cc), BF), V((h, z.r1, cc), BF),
        V((2, z.width), F32), V((2, z.width), F32),
        V((z.n_ep, z.rw, chd), F32), V((z.n_ep // 2, z.rw, chd), F32),
        V((z.rw, chd), F32), V((z.rw, chd), F32),
    ]
    D = pltpu.SemaphoreType.DMA
    sems = [
        D((nc + 2, z.groups)), D((nc + 2, z.groups)), D((nc + 1, z.gs)), D((nc + 1, z.gs)),
        D((nc, z.gs)), D((nc, z.gs)), D((h,)), D((h,)),
        D((h + 1, z.gs)), D((h + 1, z.gs)), D((h + 1, z.groups)), D((h + 1, z.groups)),
        D((3,)), D((3,)), D((z.n_ep // 2,)), D((z.n_ep // 2,)),
    ]
    spec = pl.BlockSpec(memory_space=pltpu.VMEM)
    return pl.pallas_call(
        functools.partial(kernel, z),
        out_shape=[jax.ShapeDtypeStruct(s, d) for s, d in outs],
        in_specs=[spec] * 8,
        out_specs=[spec] * len(outs),
        scratch_shapes=scratch + sems,
        compiler_params=pltpu.CompilerParams(
            collective_id=0, has_side_effects=True, vmem_limit_bytes=44 * 2**20
        ),
    )(tokens, cotangent, routes.T, router_expert.T, router_group.T, gate_proj[0], up_proj[0], down_proj[0])


def body(axes, tokens, cotangent, routes, router_group, router_expert, gate_proj, up_proj, down_proj):
    z = sizes_of(axes, tokens, routes, router_group, router_expert, gate_proj)
    rout_shape = (z.rw, z.ch) if z.reduce_here else (min(z.rw, z.rl), z.width)
    outs = [
        ((z.rows, z.cw), BF), ((z.width, z.ff), BF), ((z.width, z.ff), BF), ((z.ff, z.width), BF),
        ((1, z.width), F32), ((1, z.width), F32), ((1, z.ff), F32), (rout_shape, F32),
    ]
    spec = pl.BlockSpec(memory_space=pltpu.VMEM)
    D = pltpu.SemaphoreType.DMA
    run = run_sourced if by_source(z) else run_wide
    tg, gate, up, down, gsq, usq, dsq, rout = run(
        z, outs, tokens, cotangent, routes, router_group, router_expert, gate_proj, up_proj, down_proj
    )
    if z.reduce_here:
        half = z.ch // 2
        shapes = [gate, up, down, tg, gsq, usq, dsq]
        anywhere = pl.BlockSpec(memory_space=pl.ANY)
        gate, up, down, tg, gsq, usq, dsq, reg, rgg, rrows = pl.pallas_call(
            functools.partial(finish, z),
            out_shape=[jax.ShapeDtypeStruct(a.shape, a.dtype) for a in shapes]
            + [jax.ShapeDtypeStruct((n, half), F32) for n in (z.experts, z.groups, 1)],
            in_specs=[spec] * 8,
            out_specs=[anywhere] * 10,
            scratch_shapes=[pltpu.VMEM((n, half), F32) for n in (z.experts, z.groups, 1)] + [D((10,))],
            compiler_params=pltpu.CompilerParams(vmem_limit_bytes=16 * 2**20),
        )(*shapes, rout)
        reg, rgg, rrows = reg.T, rgg.T, rrows[0]
    else:
        mine = lax.psum_scatter(rout.T, ("ep", "tp"), scatter_dimension=0, tiled=True)
        reg = mine[:, : z.experts]
        rgg = mine[:, z.experts : z.experts + z.groups]
        rrows = jnp.sum(reg * reg, axis=1) + jnp.sum(rgg * rgg, axis=1)
    return (tg, gate[None], up[None], down[None], gsq, usq, dsq, reg, rgg, rrows)


def solution(mesh):
    return jax.shard_map(
        functools.partial(body, dict(mesh.shape)),
        mesh=mesh,
        in_specs=(
            P("ep", None), P("ep", None), P("ep", None), P(), P(),
            P("ep", None, "tp"), P("ep", None, "tp"), P("ep", "tp", None),
        ),
        out_specs=(
            P("ep", "tp"), P("ep", None, "tp"), P("ep", None, "tp"), P("ep", "tp", None),
            P("ep", None), P("ep", None), P("ep", "tp"),
            P(("ep", "tp"), None), P(("ep", "tp"), None), P(("ep", "tp")),
        ),
        check_vma=False,
    )
```

```python
import functools

import jax
import jax.numpy as jnp
from jax import lax
from jax.experimental import pallas as pl
from jax.experimental.pallas import tpu as pltpu
from jax.sharding import PartitionSpec as P

MESH = pl.DeviceIdType.MESH
BF = jnp.bfloat16
F32 = jnp.float32


def mm(a, b, da=1, db=0):
    return lax.dot_general(a, b, (((da,), (db,)), ((), ())), preferred_element_type=F32)


def lanes_of(shape, dim=1):
    return lax.broadcasted_iota(jnp.int32, shape, dim)


class Sizes:
    pass


def sizes_of(mesh, tokens, routes, router_group, router_expert, gate_proj):
    z = Sizes()
    z.n_ep, z.n_tp = mesh["ep"], mesh["tp"]
    z.rows, z.width = tokens.shape
    z.top = routes.shape[1]
    z.groups, z.experts = router_group.shape[1], router_expert.shape[1]
    z.gs = z.experts // z.groups
    z.cap = z.rows // z.gs
    z.gr = z.gs * z.cap // z.top
    z.r1 = z.groups * z.gr
    z.sl = z.groups * z.cap
    z.pairs = z.gs * z.sl
    z.ff = gate_proj.shape[2]
    z.cw = z.width // z.n_tp
    z.half_chunks = 4
    z.nc = 2 * z.half_chunks
    z.cc = z.cw // z.half_chunks
    z.rl = -(-(z.experts + z.groups) // 128) * 128
    z.rw = -(-(z.experts + z.groups) // 8) * 8
    z.ch = z.width // z.n_ep
    z.reduce_here = z.ch % 128 == 0 and z.n_ep % 2 == 0
    assert z.experts == z.n_ep and z.n_tp == 2 and z.top == 2
    assert z.sl & (z.sl - 1) == 0 and z.gr & (z.gr - 1) == 0
    return z


def kernel(
    z, tok_ref, cot_ref, routes_ref, rexp_ref, rgrp_ref, gate_ref, up_ref, down_ref,
    tg_out, gate_out, up_out, down_out, gsq_out, usq_out, dsq_out, rout_out,
    rc_ref, s1w, r1w,
    s_mat, t_mat, s1m, r1m, s1, r1, s2m, x2m, s2, x2, y2m, y2,
    gacc, uacc, pacc, dcat, hid, wcol, wp, wpr, pts, ptr, pto,
    s3m, r3m, s3, r3, s4m, r4m, s4, r4, sq, sqr, term, trec, tsum, tsumr,
    z1s, z1r, p2s, p2r, fs, fr, ptsm, ptrm, r3s, r3r, r4s, r4r, ms, mr, ts, tr,
):
    e, t = lax.axis_index("ep"), lax.axis_index("tp")
    g, p = e // z.gs, e % z.gs
    other = 1 - t

    def rcopy(src, dst, ss, rs, ep, tp):
        return pltpu.make_async_remote_copy(
            src_ref=src, dst_ref=dst, send_sem=ss, recv_sem=rs,
            device_id=(ep, tp), device_id_type=MESH,
        )

    barrier = pltpu.get_barrier_semaphore()
    for d in range(1, z.n_ep):
        pl.semaphore_signal(
            barrier, inc=1, device_id=((e + d) % z.n_ep, t), device_id_type=MESH
        )
    pl.semaphore_signal(barrier, inc=1, device_id=(e, other), device_id_type=MESH)

    sends = []

    def grows(h):
        return pl.ds(pl.multiple_of(h * z.gr, z.gr), z.gr)

    def prows(q):
        return pl.ds(pl.multiple_of(q * z.sl, z.sl), z.sl)

    def group_send(src, dst, ss, rs, c):
        for d in range(1, z.groups):
            h = (g + d) % z.groups
            cp = rcopy(src.at[grows(h)], dst.at[grows(g)], ss.at[c, d], rs.at[c, d], h * z.gs + p, t)
            cp.start()
            sends.append(cp)
        dst[grows(g), :] = src[grows(g), :]

    def group_wait(src, dst, ss, rs, c):
        for d in range(1, z.groups):
            h = (g + z.groups - d) % z.groups
            rcopy(src.at[grows(h)], dst.at[grows(h)], ss.at[c, d], rs.at[c, d], h * z.gs + p, t).wait_recv()

    def plane_send(src, dst, ss, rs, c):
        for d in range(1, z.gs):
            q = (p + d) % z.gs
            cp = rcopy(src.at[prows(q)], dst.at[prows(p)], ss.at[c, d], rs.at[c, d], g * z.gs + q, t)
            cp.start()
            sends.append(cp)
        dst[prows(p), :] = src[prows(p), :]

    def plane_wait_one(src, dst, ss, rs, c, d):
        q = (p + z.gs - d) % z.gs
        rcopy(src.at[prows(q)], dst.at[prows(q)], ss.at[c, d], rs.at[c, d], g * z.gs + q, t).wait_recv()

    def plane_wait(src, dst, ss, rs, c):
        for d in range(1, z.gs):
            plane_wait_one(src, dst, ss, rs, c, d)

    def pair_send(src, dst, ss, rs):
        cp = rcopy(src, dst, ss, rs, e, other)
        cp.start()
        sends.append(cp)
        return cp

    lane = lanes_of((z.rows, z.rl))
    eye = lanes_of((z.rows, z.rows), 0) == lanes_of((z.rows, z.rows), 1)

    def column(row):
        return jnp.sum(jnp.where(eye, row.astype(F32), 0.0), axis=1, keepdims=True).astype(jnp.int32)

    r0, r1_ = column(routes_ref[0:1, :]), column(routes_ref[1:2, :])
    chosen = (lane == r0) | (lane == r1_)
    low = (lane - z.experts) * z.gs
    is_group = (lane >= z.experts) & (lane < z.experts + z.groups)
    in_group = is_group & (r0 >= low) & (r0 < low + z.gs)

    def before(n):
        return (lanes_of((n, n), 1) < lanes_of((n, n), 0)).astype(F32).astype(BF)

    ghot = in_group.astype(F32)
    grank = mm(before(z.rows), ghot.astype(BF))
    grank = jnp.where(in_group, grank, -1.0).astype(BF)
    er, el = lanes_of((z.rl, z.r1), 0) - z.experts, lanes_of((z.rl, z.r1), 1)
    expand = ((el >= er * z.gr) & (el < (er + 1) * z.gr)).astype(F32).astype(BF)
    place = (lanes_of((z.rows, z.r1)) & (z.gr - 1)).astype(F32)
    s_mat[...] = (mm(grank, expand) == place).astype(F32).astype(BF)

    s1m[...] = mm(s_mat[...], chosen.astype(F32).astype(BF), 0, 0).astype(BF)
    pl.semaphore_wait(barrier, z.n_ep)
    group_send(s1m, r1m, z1s, z1r, z.nc)

    def cols_at(half, k):
        return pl.ds(pl.multiple_of(half * z.cw + k * z.cc, z.cc), z.cc)

    for c in range(z.nc):
        src = tok_ref if c < z.half_chunks else cot_ref
        s1[c] = mm(s_mat[...], src[:, cols_at(t, c % z.half_chunks)], 0, 0).astype(BF)
        group_send(s1.at[c], r1.at[c], z1s, z1r, c)

    rc_ref[...] = jnp.zeros_like(rc_ref)
    rc_ref[0 : z.experts, :] = rexp_ref[...]
    rc_ref[z.experts : z.experts + z.groups, :] = rgrp_ref[...]
    expd = jnp.exp(mm(tok_ref[...], rc_ref[...], 1, 1))
    gexp = jnp.where(is_group, expd, 0.0)
    gprob = gexp / jnp.sum(gexp, axis=1, keepdims=True)
    picked = jnp.sum(jnp.where(in_group, gprob, 0.0), axis=1, keepdims=True)
    pexp = jnp.where(chosen, expd, 0.0)
    paired = pexp / jnp.sum(pexp, axis=1, keepdims=True)
    s1w[...] = mm(s_mat[...], (picked * paired).astype(BF), 0, 0).astype(BF)
    group_send(s1w, r1w, z1s, z1r, z.nc + 1)

    group_wait(s1m, r1m, z1s, z1r, z.nc)
    vals = r1m[...]
    lane1 = lanes_of((z.r1, z.rl))
    member = (vals.astype(F32) > 0.0) & (lane1 < z.experts)
    rank = mm(before(z.r1), member.astype(F32).astype(BF))
    rank = jnp.where(member, rank, -1.0).astype(BF)
    er, el = lanes_of((z.rl, z.pairs), 0) - g * z.gs, lanes_of((z.rl, z.pairs), 1)
    expand = ((el >= er * z.sl) & (el < (er + 1) * z.sl)).astype(F32).astype(BF)
    place = (lanes_of((z.r1, z.pairs)) & (z.sl - 1)).astype(F32)
    t_mat[...] = (mm(rank, expand) == place).astype(F32).astype(BF)

    def pack_two(c):
        group_wait(s1.at[c], r1.at[c], z1s, z1r, c)
        s2[c] = mm(t_mat[...], r1[c], 0, 0).astype(BF)
        plane_send(s2.at[c], x2.at[c], p2s, p2r, c)
        pair_send(x2.at[c, prows(p)], y2.at[c, prows(p)], fs.at[c, 0], fr.at[c, 0])

    def accumulate(x, half, c):
        if c < z.half_chunks:
            at = cols_at(half, c)
            gate_add, up_add = mm(x, gate_ref[at, :]), mm(x, up_ref[at, :])
            gacc[...] += gate_add
            uacc[...] += up_add
        else:
            pacc[...] += mm(x, down_ref[:, cols_at(half, c - z.half_chunks)], 1, 1)

    def land(c):
        for d in range(1, z.gs):
            plane_wait_one(s2.at[c], x2.at[c], p2s, p2r, c, d)
            q = (p + z.gs - d) % z.gs
            pair_send(x2.at[c, prows(q)], y2.at[c, prows(q)], fs.at[c, d], fr.at[c, d])
        accumulate(x2[c], t, c)

    def land_other(c):
        for d in range(z.gs):
            q = (p + z.gs - d) % z.gs
            rcopy(x2.at[c, prows(q)], y2.at[c, prows(q)], fs.at[c, d], fr.at[c, d], e, other).wait_recv()
        accumulate(y2[c], other, c)

    gacc[...] = jnp.zeros_like(gacc)
    uacc[...] = jnp.zeros_like(uacc)
    pacc[...] = jnp.zeros_like(pacc)
    for c in range(z.nc + 3):
        if c < z.nc:
            pack_two(c)
        if c == z.nc - 1:
            group_wait(s1w, r1w, z1s, z1r, z.nc + 1)
            s2m[...] = mm(t_mat[...], r1w[...], 0, 0).astype(BF)
            plane_send(s2m, x2m, p2s, p2r, z.nc)
        if 2 <= c < z.nc + 2:
            land(c - 2)
        if c >= 3:
            land_other(c - 3)
    plane_wait(s2m, x2m, p2s, p2r, z.nc)

    lane2 = lanes_of((z.pairs, z.rl))
    scale = jnp.sum(jnp.where(lane2 == e, x2m[...].astype(F32), 0.0), axis=1, keepdims=True)
    wcol[...] = jnp.broadcast_to(scale, wcol.shape)
    gate_pre, up_pre, pulled = gacc[...], uacc[...], pacc[...]
    sig = 1.0 / (1.0 + jnp.exp(-gate_pre))
    silu = gate_pre * sig
    hidden = (silu * up_pre).astype(BF)
    hid[...] = hidden
    wp[...] = jnp.broadcast_to(
        jnp.sum(pulled * hidden.astype(F32), axis=1, keepdims=True), wp.shape
    )
    w_copy = pair_send(wp, wpr, ms.at[0], mr.at[0])
    dh = scale * pulled
    dcat[:, : z.ff] = (dh * up_pre * sig * (1.0 + gate_pre * (1.0 - sig))).astype(BF)
    dcat[:, z.ff :] = (dh * silu).astype(BF)

    def token_term(half, k):
        at = cols_at(half, k)
        return (
            mm(dcat[:, : z.ff], gate_ref[at, :], 1, 1) + mm(dcat[:, z.ff :], up_ref[at, :], 1, 1)
        ).astype(BF)

    pt = []
    for k in range(z.half_chunks):
        pts[k] = token_term(other, k)
        pt.append(pair_send(pts.at[k], ptr.at[k], ptsm.at[k], ptrm.at[k]))
    w_copy.wait_recv()
    wsum = wp[:, 0:1] + wpr[:, 0:1]
    s3m[...] = jnp.where(lane2 == e, wsum, 0.0).astype(BF)
    plane_send(s3m, r3m, r3s, r3r, z.half_chunks)
    for k in range(z.half_chunks):
        pto[k] = token_term(t, k)
        pt[k].wait_recv()
        s3[k] = (pto[k].astype(F32) + ptr[k].astype(F32)).astype(BF)
        plane_send(s3.at[k], r3.at[k], r3s, r3r, k)

    ones_ff = jnp.ones((16, z.ff), BF)

    def gate_up_grads(xs, half, k):
        at = cols_at(half, k)
        total = mm(xs[k], dcat[...], 0, 0)
        gate_out[at, :] = total[:, : z.ff].astype(BF)
        up_out[at, :] = total[:, z.ff :].astype(BF)
        square = (total * total).astype(BF)
        sq[0:1, at] = mm(ones_ff, square[:, : z.ff], 1, 1)[0:1]
        sq[1:2, at] = mm(ones_ff, square[:, z.ff :], 1, 1)[0:1]

    def down_grads(xs, half, k):
        scaled = (wcol[:, 0:1] * xs[z.half_chunks + k].astype(F32)).astype(BF)
        total = mm(hid[...], scaled, 0, 0)
        down_out[:, cols_at(half, k)] = total.astype(BF)
        return mm(jnp.ones((16, z.cc), BF), (total * total).astype(BF), 1, 1)[0:1]

    def back_two(k):
        plane_wait(s3.at[k], r3.at[k], r3s, r3r, k)
        s4[k] = mm(t_mat[...], r3[k]).astype(BF)
        group_send(s4.at[k], r4.at[k], r4s, r4r, k)

    gate_up_grads(x2, t, 0)
    plane_wait(s3m, r3m, r3s, r3r, z.half_chunks)
    s4m[...] = mm(t_mat[...], r3m[...]).astype(BF)
    group_send(s4m, r4m, r4s, r4r, z.half_chunks)
    gate_up_grads(x2, t, 1)
    for k in range(z.half_chunks - 1):
        back_two(k)
        if k + 2 < z.half_chunks:
            gate_up_grads(x2, t, k + 2)
        else:
            gate_up_grads(y2, other, 0)

    group_wait(s4m, r4m, r4s, r4r, z.half_chunks)
    dw = mm(s_mat[...], r4m[...])
    dpicked = jnp.sum(dw * paired, axis=1, keepdims=True)
    q = picked * dw
    dchosen = paired * (q - jnp.sum(paired * q, axis=1, keepdims=True))
    dgroup = jnp.where(is_group, (dpicked * picked) * (ghot - gprob), 0.0)
    dall = (dchosen + dgroup).astype(BF)
    dterm = dall[:, : z.rw] if z.rw < z.rl else dall
    tcopies = []
    if z.reduce_here:
        full = mm(dterm, tok_ref[...], 0, 0)
        for i in range(z.n_ep):
            term[i] = full[:, i * z.ch : (i + 1) * z.ch]

        def term_copy(m):
            to = (e + 2 * m + t) % z.n_ep
            return rcopy(term.at[to], trec.at[m], ts.at[m], tr.at[m], to, t)

        @pl.when(t == 0)
        def _():
            trec[0] = term[e]

        @pl.when(t == 1)
        def _():
            term_copy(0).start()

        for m in range(1, z.n_ep // 2):
            term_copy(m).start()
    else:
        row = lanes_of((z.rows, z.rl), 0)[:, : dterm.shape[1]]
        mine = (row >= t * (z.rows // 2)) & (row < (t + 1) * (z.rows // 2))
        dterm = jnp.where(mine, dterm.astype(F32), 0.0).astype(BF)
        rout_out[...] = mm(dterm, tok_ref[...], 0, 0)

    back_two(z.half_chunks - 1)
    for k in range(1, z.half_chunks):
        gate_up_grads(y2, other, k)
    sq_copy = pair_send(sq, sqr, ms.at[1], mr.at[1])
    dsq = jnp.zeros((1, z.ff), F32)
    for k in range(z.half_chunks):
        dsq += down_grads(x2, t, k)

    if z.reduce_here:

        @pl.when(t == 1)
        def _():
            term_copy(0).wait_recv()

        for m in range(1, z.n_ep // 2):
            term_copy(m).wait_recv()
        acc = trec[0]
        for m in range(1, z.n_ep // 2):
            acc = acc + trec[m]
        tsum[...] = acc
        t_pair = pair_send(tsum, tsumr, ms.at[2], mr.at[2])
    for k in range(z.half_chunks):
        dsq += down_grads(y2, other, k)
    dsq_out[...] = dsq

    for k in range(z.half_chunks):
        group_wait(s4.at[k], r4.at[k], r4s, r4r, k)
        tg_out[:, k * z.cc : (k + 1) * z.cc] = (
            mm(s_mat[...], r4[k]) + mm(dall, rc_ref[:, cols_at(t, k)])
        ).astype(BF)
    sq_copy.wait_recv()
    gsq_out[...] = sq[0:1, :] + sqr[0:1, :]
    usq_out[...] = sq[1:2, :] + sqr[1:2, :]
    if z.reduce_here:
        t_pair.wait_recv()
        rout_out[...] = tsum[...] + tsumr[...]

        @pl.when(t == 1)
        def _():
            term_copy(0).wait_send()

        for m in range(1, z.n_ep // 2):
            term_copy(m).wait_send()
    for cp in sends:
        cp.wait_send()


def sourced(
    z, tok_h, cot_h, routes_h, rexp_h, rgrp_h, gate_h, up_h, down_h,
    tg_out, gate_out, up_out, down_out, gsq_out, usq_out, dsq_out, rout_out,
    tok_ref, cot_ref, routes_ref, rexp_ref, rgrp_ref, gate_ref, up_ref, down_ref,
    rc_ref, s_mat, s_tr, t_mat, t_tr, s1w, r1w, s1, r1, s2m, x2m, s2, x2, y2,
    gacc, uacc, pacc, gate_tr, up_tr, down_tr,
    dcat, hid, hid_tr, wp, wpr, pts, ptr, s3m, r3m, s3, r3, s4, r4, dall_ref,
    sq, sqr, term, tra, tsa, trb,
    ins, z1s, z1r, p2s, p2r, fs, fr, ws, wr, ptsm, ptrm, r3s, r3r, r4s, r4r, ms, mr, tas, tar, tbs, tbr,
):
    e, t = lax.axis_index("ep"), lax.axis_index("tp")
    g, p = e // z.gs, e % z.gs
    other = 1 - t
    hk = [g, g + 1 - 2 * (g % 2), 3 - g, (g + 2) % 4]
    qd = [p, p + 1 - 2 * (p % 2), (p + 2) % 4, 3 - p]
    inner = (g + 1) // 2 == 1
    nj, cc, gr, cap, blk, per = z.nj, z.cc, z.gr, z.cap, z.blk, z.per
    ng = 2 * nj
    far = (1, 2, 3)

    def rcopy(src, dst, ss, rs, ep, tp):
        return pltpu.make_async_remote_copy(
            src_ref=src, dst_ref=dst, send_sem=ss, recv_sem=rs,
            device_id=(ep, tp), device_id_type=MESH,
        )

    barrier = pltpu.get_barrier_semaphore()
    for k in far:
        pl.semaphore_signal(barrier, inc=1, device_id=(hk[k] * z.gs + p, t), device_id_type=MESH)
        pl.semaphore_signal(barrier, inc=1, device_id=(hk[k] * z.gs + p, other), device_id_type=MESH)
        pl.semaphore_signal(barrier, inc=1, device_id=(g * z.gs + qd[k], t), device_id_type=MESH)
    pl.semaphore_signal(barrier, inc=1, device_id=(e, other), device_id_type=MESH)

    loads = [
        pltpu.make_async_copy(a, b, ins.at[i])
        for i, (a, b) in enumerate((
            (routes_h, routes_ref), (tok_h, tok_ref), (rexp_h, rexp_ref), (rgrp_h, rgrp_ref),
            (cot_h, cot_ref), (gate_h, gate_ref), (up_h, up_ref), (down_h, down_ref),
        ))
    ]
    for cp in loads:
        cp.start()

    def kr(k, n=1):
        return pl.ds(k * gr, n * gr)

    def kb(k, n=1):
        return pl.ds(k * blk, n * blk)

    def in_block(k, q):
        return pl.ds(pl.multiple_of(k * blk + q * cap, cap), cap)

    def three(k):
        return pl.ds(k * blk, 3 * cap)

    def cols(half, j):
        return pl.ds(pl.multiple_of(half * z.cw + j * cc, cc), cc)

    def z_copy(src, dst, c, k):
        return rcopy(src.at[kr(k)], dst.at[kr(k)], z1s.at[c // ng], z1r.at[c, k - 1], hk[k] * z.gs + p, t)

    def spread(src, dst, ss, rs, k):
        for d in (3, 1, 2):
            rcopy(src.at[in_block(k, qd[d])], dst.at[in_block(k, p)], ss, rs, g * z.gs + qd[d], t).start()
        dst[in_block(k, p), :] = src[in_block(k, p), :]

    def gathered(src, dst, ss, rs, k):
        rcopy(src.at[three(k)], dst.at[three(k)], ss, rs, g * z.gs + qd[3], t).wait_recv()

    def line_out(src, dst, ss, rs, k, line):
        mine = pl.ds(pl.multiple_of((k * z.gs + p) * 16, 16), 16)
        src[k * 16 : (k + 1) * 16, :] = line.astype(BF)
        for d in (3, 1, 2):
            rcopy(src.at[pl.ds(k * 16, 16)], dst.at[mine], ss, rs, g * z.gs + qd[d], t).start()
        dst[mine, :] = src[k * 16 : (k + 1) * 16, :]

    def line_wait(dst, ss, rs, k):
        part = dst.at[pl.ds(k * z.gs * 16, 48)]
        rcopy(part, part, ss, rs, g * z.gs + qd[3], t).wait_recv()

    def line_column(dst, k):
        tiles = []
        for q in range(z.gs):
            at = (k * z.gs + q) * 16
            tiles += [dst[at : at + 16, :]] * (cap // 16)
        rows = jnp.concatenate(tiles, axis=0).astype(F32)
        r, c = lanes_of((blk, blk), 0), lanes_of((blk, blk), 1)
        return jnp.sum(jnp.where(c == p * cap + r % cap, rows, 0.0), axis=1, keepdims=True)

    def pair(src, dst, ss, rs):
        return rcopy(src, dst, ss, rs, e, other)

    lane = lanes_of((z.rows, z.rl))
    ll, lb = lane % per, lane // per
    eye = lanes_of((z.rows, z.rows), 0) == lanes_of((z.rows, z.rows), 1)

    def column(row):
        return jnp.sum(jnp.where(eye, row.astype(F32), 0.0), axis=1, keepdims=True).astype(jnp.int32)

    def before(n):
        r, c = lanes_of((n, n), 0), lanes_of((n, n), 1)
        return ((c < r) & (r // gr == c // gr)).astype(F32).astype(BF)

    def make_t(k, n):
        m = n * gr
        vals = r1w[kr(k, n), :]
        member = (vals.astype(F32) > 0.0) & (lanes_of((m, z.rl)) < z.experts)
        rank = mm(before(m), member.astype(F32).astype(BF))
        rank = jnp.where(member, rank, -1.0).astype(BF)
        sr, sc = lanes_of((z.rl, blk), 0) - g * z.gs, lanes_of((z.rl, blk), 1)
        expand = (sr == sc // cap).astype(F32).astype(BF)
        spot = (lanes_of((m, blk)) % cap).astype(F32)
        tf = (mm(rank, expand) == spot).astype(F32)
        t_mat[kr(k, n), :] = tf.astype(BF)
        t_tr[:, kr(k, n)] = tf.T.astype(BF)

    def t_rows(k):
        return t_mat[k * gr : (k + 1) * gr, :]

    def t_cols(k):
        return t_tr[:, k * gr : (k + 1) * gr]

    loads[0].wait()
    r0, r1_ = column(routes_ref[0:1, :]), column(routes_ref[1:2, :])
    chosen = (ll == r0) | (ll == r1_)
    low = (ll - z.experts) * z.gs
    is_group = (ll >= z.experts) & (ll < z.experts + z.groups)
    in_group = is_group & (r0 >= low) & (r0 < low + z.gs)
    tri = lanes_of((z.rows, z.rows), 1) < lanes_of((z.rows, z.rows), 0)
    grank = mm(tri.astype(F32).astype(BF), in_group.astype(F32).astype(BF))
    grank = jnp.where(in_group, grank, -1.0).astype(BF)
    er, el = lanes_of((z.rl, z.r1), 0) - z.experts, lanes_of((z.rl, z.r1), 1)
    kk = el // gr
    want = jnp.where(kk == 0, hk[0], jnp.where(kk == 1, hk[1], jnp.where(kk == 2, hk[2], hk[3])))
    expand = (er == want).astype(F32).astype(BF)
    place = (lanes_of((z.rows, z.r1)) % gr).astype(F32)
    s_f = (mm(grank, expand) == place).astype(F32)
    s_mat[...] = s_f.astype(BF)
    s_tr[...] = s_f.T.astype(BF)
    pick_mask = jnp.where(chosen & (lb == 0), 1.0, 0.0)
    r1w[kr(0), :] = mm(s_tr[kr(0), :], pick_mask.astype(BF)).astype(BF)

    def fill(c):
        j = c % nj
        src = tok_ref if c < nj else cot_ref
        s1[c] = mm(s_tr[...], src[:, cols(t, j)]).astype(BF)
        r1[c, kr(0), :] = s1[c, kr(0), :]

    def near_out(c):
        z_copy(s1.at[c], r1.at[c], c, 1).start()

        @pl.when(inner)
        def _():
            z_copy(s1.at[c], r1.at[c], c, 2).start()

    def op_a(k, c):
        if k:
            z_copy(s1.at[c], r1.at[c], c, k).wait_recv()
        s2[c, kb(k), :] = mm(t_cols(k), r1[c, kr(k), :]).astype(BF)
        spread(s2.at[c], x2.at[c], p2s.at[0], p2r.at[c, k], k)

    def op_am(k):
        er, ec = lanes_of((z.rl, blk), 0), lanes_of((z.rl, blk), 1)
        pick = (er == per + g * z.gs + ec // cap).astype(F32).astype(BF)
        weight = mm(r1w[kr(k), :], pick) * t_rows(k).astype(F32)
        line_out(s2m, x2m, p2s.at[1], p2r.at[ng, k], k, mm(jnp.ones((16, gr), BF), weight.astype(BF)))

    make_t(0, 1)
    loads[1].wait()
    fill(0)
    pl.semaphore_wait(barrier, 10)
    near_out(0)
    op_a(0, 0)
    for c in range(1, nj):
        fill(c)
        near_out(c)
        op_a(0, c)

    rc_ref[...] = jnp.zeros_like(rc_ref)
    loads[2].wait()
    loads[3].wait()
    for b in range(z.rl // per):
        rc_ref[b * per : b * per + z.experts, :] = rexp_ref[...]
        rc_ref[b * per + z.experts : b * per + z.experts + z.groups, :] = rgrp_ref[...]
    expd = jnp.exp(mm(tok_ref[...], rc_ref[...], 1, 1))
    gexp = jnp.where(is_group, expd, 0.0)
    gprob = gexp / jnp.sum(jnp.where(lb == 0, gexp, 0.0), axis=1, keepdims=True)
    picked = jnp.sum(jnp.where(in_group & (lb == 0), gprob, 0.0), axis=1, keepdims=True)
    pexp = jnp.where(chosen, expd, 0.0)
    paired = pexp / jnp.sum(jnp.where(lb == 0, pexp, 0.0), axis=1, keepdims=True)
    both = paired + gprob
    upper = both.astype(BF).astype(F32)
    meta = jnp.where(lb == 1, picked * paired, jnp.where(lb == 2, upper, jnp.where(lb == 3, both - upper, pick_mask)))
    s1w[...] = mm(s_tr[...], meta.astype(BF)).astype(BF)
    r1w[kr(0), :] = s1w[kr(0), :]
    for k in far:
        z_copy(s1w, r1w, ng, k).start()
    loads[4].wait()
    for c in range(nj, ng):
        fill(c)
        near_out(c)
        op_a(0, c)

    def op_s(k):
        for c in range(ng):
            z_copy(s1.at[c], r1.at[c], c, k).start()

    @pl.when(inner)
    def _():
        op_s(3)

    op_am(0)

    def op_t(k):
        z_copy(s1w, r1w, ng, k).wait_recv()
        make_t(k, 1)

    def relay(k, c):
        return pair(x2.at[c, kb(k)], y2.at[c, kb(k)], fs.at[0], fr.at[max(0, c - nj + 1), k])

    def op_b(k, c):
        gathered(s2.at[c], x2.at[c], p2s.at[0], p2r.at[c, k], k)
        relay(k, c).start()

    def op_c1(k, n):
        ga = ua = None
        for half, xs in ((t, x2), (other, y2)):
            for j in range(nj):
                if xs is y2 and j == 0:
                    for i in range(n):
                        both_in = pl.ds(0, nj), kb(k + i)
                        pair(x2.at[both_in], y2.at[both_in], fs.at[0], fr.at[0, k + i]).wait_recv()
                x, at = xs[j, kb(k, n), :], cols(half, j)
                a, b = mm(x, gate_ref[at, :]), mm(x, up_ref[at, :])
                ga, ua = (a, b) if ga is None else (ga + a, ua + b)
        gacc[kb(k, n), :] = ga
        uacc[kb(k, n), :] = ua

    def token_term(k, n, half, j):
        at = cols(half, j)
        return (
            mm(dcat[kb(k, n), : z.ff], gate_tr[:, at]) + mm(dcat[kb(k, n), z.ff :], up_tr[:, at])
        ).astype(BF)

    def w_pair(k, n):
        return pair(wp.at[kb(k, n)], wpr.at[kb(k, n)], ws.at[0], wr.at[k])

    def pt_pair(j, k, n):
        return pair(pts.at[j, kb(k, n)], ptr.at[j, kb(k, n)], ptsm.at[0], ptrm.at[j, k])

    def pull(k, n, js, pulled):
        for half, xs in ((t, x2), (other, y2)):
            for j in js:
                if xs is y2:
                    for i in range(n):
                        relay(k + i, nj + j).wait_recv()
                a = mm(xs[nj + j, kb(k, n), :], down_tr[cols(half, j), :])
                pulled = a if pulled is None else pulled + a
        return pulled

    def op_p(k, n):
        pacc[kb(k, n), :] = pull(k, n, range(nj - 1), None)

    def op_c2(k, n):
        pulled = pull(k, n, (nj - 1,), pacc[kb(k, n), :])
        for i in range(n):
            line_wait(x2m, p2s.at[1], p2r.at[ng, k + i], k + i)
        m = n * blk
        scale = jnp.concatenate([line_column(x2m, k + i) for i in range(n)], axis=0)
        gate_pre, up_pre = gacc[kb(k, n), :], uacc[kb(k, n), :]
        sig = 1.0 / (1.0 + jnp.exp(-gate_pre))
        silu = gate_pre * sig
        product = silu * up_pre
        hidden = product.astype(BF)
        hid[kb(k, n), :] = (scale * product).astype(BF)
        wp[kb(k, n), :] = jnp.broadcast_to(
            jnp.sum(pulled * hidden.astype(F32), axis=1, keepdims=True), (m, z.rl)
        )
        w_pair(k, n).start()
        dh = scale * pulled
        dcat[kb(k, n), : z.ff] = (dh * up_pre * sig * (1.0 + gate_pre * (1.0 - sig))).astype(BF)
        dcat[kb(k, n), z.ff :] = (dh * silu).astype(BF)
        for j in range(nj):
            pts[j, kb(k, n), :] = token_term(k, n, other, j)
            pt_pair(j, k, n).start()

    def op_d(k, n, out=False):
        mine = token_term(k, n, t, 0)
        w_pair(k, n).wait_recv()
        wsum = wp[kb(k, n), :] + wpr[kb(k, n), :]
        same = lanes_of((blk, blk), 0) == lanes_of((blk, blk), 1)
        for i in range(n):
            diag = jnp.where(same, wsum[i * blk : (i + 1) * blk, :blk], 0.0).astype(BF)
            line_out(s3m, r3m, r3s.at[1], r3r.at[nj, k + i], k + i, mm(jnp.ones((16, blk), BF), diag))
        for j in range(nj):
            if j:
                mine = token_term(k, n, t, j)
            pt_pair(j, k, n).wait_recv()
            s3[j, kb(k, n), :] = (mine.astype(F32) + ptr[j, kb(k, n), :].astype(F32)).astype(BF)
            if out:
                spread(s3.at[j], r3.at[j], r3s.at[0], r3r.at[j, k], k)

    def op_dr(k, n):
        op_d(k, n, True)

    def op_r(k):
        for j in range(nj):
            spread(s3.at[j], r3.at[j], r3s.at[0], r3r.at[j, k], k)

    def home_copy(j, k):
        return rcopy(s4.at[j, kr(k)], r4.at[j, kr(k)], r4s.at[0], r4r.at[j], hk[k] * z.gs + p, t)

    lane3 = lanes_of((gr, z.rl))
    i1, i2 = lanes_of((z.rl, z.rl), 0), lanes_of((z.rl, z.rl), 1)
    fold = ((i2 < per) & ((i1 == 2 * per + i2) | (i1 == 3 * per + i2))).astype(F32).astype(BF)

    def op_e(k):
        vals = mm(r1w[kr(k), :], fold)
        g_lane = (lane3 >= z.experts) & (lane3 < z.experts + z.groups)
        pr = jnp.where(lane3 < z.experts, vals, 0.0)
        here = lane3 == z.experts + g
        pk = jnp.sum(jnp.where(here, vals, 0.0), axis=1, keepdims=True)
        line_wait(r3m, r3s.at[1], r3r.at[nj, k], k)
        lr, lc = lanes_of((blk, z.rl), 0), lanes_of((blk, z.rl), 1)
        dw = mm(t_rows(k), jnp.where(lc == g * z.gs + lr // cap, line_column(r3m, k), 0.0).astype(BF))
        dpicked = jnp.sum(dw * pr, axis=1, keepdims=True)
        q = pk * dw
        dchosen = pr * (q - jnp.sum(pr * q, axis=1, keepdims=True))
        dgroup = jnp.where(g_lane, (dpicked * pk) * (here.astype(F32) - vals), 0.0)
        dall_ref[kr(k), :] = (dchosen + dgroup).astype(BF)

    def op_f(k):
        dall = dall_ref[kr(k), :]
        for j in range(nj):
            gathered(s3.at[j], r3.at[j], r3s.at[0], r3r.at[j, k], k)
            row = (mm(t_rows(k), r3[j, kb(k), :]) + mm(dall, rc_ref[:, cols(t, j)])).astype(BF)
            if k:
                s4[j, kr(k), :] = row
                home_copy(j, k).start()
            else:
                r4[j, kr(k), :] = row

    sub = min(cc, 256)
    ns = cc // sub
    ones_ff = jnp.ones((16, z.ff), BF)
    ones_sub = jnp.ones((16, sub), BF)
    n_piece = z.cw // sub

    def gate_up_grads(i):
        half, xs = (t, x2) if i < n_piece else (other, y2)
        i = i % n_piece
        j, o = i // ns, (i % ns) * sub
        at = pl.ds(pl.multiple_of(half * z.cw + i * sub, sub), sub)
        total = mm(xs[j, :, o : o + sub], dcat[...], 0, 0)
        gate_out[at, :] = total[:, : z.ff].astype(BF)
        up_out[at, :] = total[:, z.ff :].astype(BF)
        square = (total * total).astype(BF)
        sq[0:1, at] = mm(ones_ff, square[:, : z.ff], 1, 1)[0:1]
        sq[1:2, at] = mm(ones_ff, square[:, z.ff :], 1, 1)[0:1]

    def down_grads(i):
        half, xs = (t, x2) if i < n_piece else (other, y2)
        i = i % n_piece
        j, o = i // ns, (i % ns) * sub
        at = pl.ds(pl.multiple_of(half * z.cw + i * sub, sub), sub)
        total = mm(hid_tr[...], xs[nj + j, :, o : o + sub])
        down_out[:, at] = total.astype(BF)
        return mm(ones_sub, (total * total).astype(BF), 1, 1)[0:1]

    loads[5].wait()
    gate_tr[...] = gate_ref[...].T
    loads[6].wait()
    up_tr[...] = up_ref[...].T
    loads[7].wait()
    down_tr[...] = down_ref[...].T

    per_core = z.cw // z.ch // z.gs
    home_core = g // per_core
    all_a = rcopy(term.at[pl.ds(0, 3)], tra, tas.at[0], tar.at[0], g * z.gs + qd[3], t)

    def term_b(k, core):
        return rcopy(tsa.at[hk[k] % per_core], trb.at[k], tbs.at[0], tbr.at[0], hk[k] * z.gs + p, core)

    t_pair = pair(tsa.at[g % per_core], trb.at[0], ms.at[1], mr.at[1])

    def op_x():
        dterm = dall_ref[:, : z.rw]
        for j in range(nj):
            full = mm(dterm, r1[j], 0, 0)
            for i in range(cc // z.ch):
                n = j * (cc // z.ch) + i
                term[n % z.gs, n // z.gs] = full[:, i * z.ch : (i + 1) * z.ch]
        for d in far:
            rcopy(term.at[qd[d]], tra.at[d - 1], tas.at[0], tar.at[0], g * z.gs + qd[d], t).start()

    def op_y():
        all_a.wait_recv()
        tsa[...] = term[p] + tra[0] + tra[1] + tra[2]
        for k in far:

            @pl.when(hk[k] // per_core == t)
            def _():
                for core in range(z.n_tp):
                    term_b(k, core).start()

        @pl.when(home_core == t)
        def _():
            t_pair.start()

    sq_copy = pair(sq, sqr, ms.at[0], mr.at[0])

    def op_h():
        hid_tr[...] = hid[...].T

    def op_q():
        sq_copy.start()

    def op_w(i):
        part = down_grads(i)
        dsq_out[...] = dsq_out[...] + part if i else part

    ops = {
        "t": op_t, "a": op_a, "m": op_am, "b": op_b, "c": op_c1, "p": op_p, "C": op_c2, "d": op_d, "D": op_dr, "r": op_r,
        "e": op_e, "f": op_f, "x": op_x, "y": op_y, "g": gate_up_grads, "h": op_h, "q": op_q, "w": op_w, "s": op_s,
    }

    def play(text):
        for word in " ".join(text).split():
            ops[word[0]](*(int(x) for x in word[1:]))

    @pl.when((g + 1) // 2 != 1)
    def _():
        play(z.order_end)

    @pl.when(inner)
    def _():
        play(z.order_mid)

    def home(j):
        rcopy(s4.at[j, kr(1, 3)], r4.at[j, kr(1, 3)], r4s.at[0], r4r.at[j], e, other).wait_recv()
        tg_out[:, j * cc : (j + 1) * cc] = mm(s_mat[...], r4[j]).astype(BF)

    for j in range(nj):
        home(j)
    sq_copy.wait_recv()
    gsq_out[...] = sq[0:1, :] + sqr[0:1, :]
    usq_out[...] = sq[1:2, :] + sqr[1:2, :]
    got = trb.at[pl.ds(1, 3)]
    rcopy(got, got, tbs.at[0], tbr.at[0], e, other).wait_recv()

    @pl.when(home_core == t)
    def _():
        rout_out[...] = tsa[g % per_core] + trb[1] + trb[2] + trb[3]

    @pl.when(home_core != t)
    def _():
        t_pair.wait_recv()
        rout_out[...] = trb[0] + trb[1] + trb[2] + trb[3]

    @pl.when(home_core == t)
    def _():
        t_pair.wait_send()
        rcopy(trb.at[pl.ds(0, 2)], trb.at[pl.ds(0, 2)], tbs.at[0], tbr.at[0], e, other).wait_send()

    @pl.when(home_core != t)
    def _():
        rcopy(trb, trb, tbs.at[0], tbr.at[0], e, other).wait_send()

    most, some = pl.ds(0, 3 * blk), pl.ds(0, 16 * 12)

    def left(src, dst, ss, rs):
        rcopy(src, dst, ss, rs, e, other).wait_send()

    left(s1.at[:, kr(1, 3)], r1.at[:, kr(1, 3)], z1s.at[0], z1r.at[0, 0])
    left(s1w.at[kr(1, 3)], r1w.at[kr(1, 3)], z1s.at[1], z1r.at[ng, 0])
    left(s2.at[:, most], x2.at[:, most], p2s.at[0], p2r.at[0, 0])
    left(x2m.at[some], x2m.at[some], p2s.at[1], p2r.at[ng, 0])
    left(x2, y2, fs.at[0], fr.at[0, 0])
    left(wp, wpr, ws.at[0], wr.at[0])
    left(pts, ptr, ptsm.at[0], ptrm.at[0, 0])
    left(s3.at[:, most], r3.at[:, most], r3s.at[0], r3r.at[0, 0])
    left(r3m.at[some], r3m.at[some], r3s.at[1], r3r.at[nj, 0])
    left(s4.at[:, kr(1, 3)], r4.at[:, kr(1, 3)], r4s.at[0], r4r.at[0])
    all_a.wait_send()
    sq_copy.wait_send()


def finish(
    z, gate_in, up_in, down_in, tg_in, gsq_in, usq_in, dsq_in, rout_in,
    gate_out, up_out, down_out, tg_out, gsq_out, usq_out, dsq_out, reg_out, rgg_out, rows_out,
    reg_ref, rgg_ref, rows_ref, sem,
):
    pairs = [
        (gate_in, gate_out), (up_in, up_out), (down_in, down_out), (tg_in, tg_out),
        (gsq_in, gsq_out), (usq_in, usq_out), (dsq_in, dsq_out),
        (reg_ref, reg_out), (rgg_ref, rgg_out), (rows_ref, rows_out),
    ]
    copies = [pltpu.make_async_copy(src, dst, sem.at[i]) for i, (src, dst) in enumerate(pairs)]
    for cp in copies[:7]:
        cp.start()
    half = z.ch // 2
    both = rout_in[...]
    mine = jnp.where(lax.axis_index("tp") == 0, both[:, :half], both[:, half:])
    reg = mine[: z.experts]
    rgg = mine[z.experts : z.experts + z.groups]
    reg_ref[...] = reg
    rgg_ref[...] = rgg
    rows_ref[...] = jnp.sum(reg * reg, axis=0, keepdims=True) + jnp.sum(rgg * rgg, axis=0, keepdims=True)
    for cp in copies[7:]:
        cp.start()
    for cp in copies:
        cp.wait()


def by_source(z):
    return (
        z.reduce_here and z.groups == 4 and z.gs == 4 and z.cap % 16 == 0 and z.gr % 16 == 0
        and z.experts + z.groups <= z.rl // 4 and z.cw % 512 == 0 and (z.cw // z.ch) % z.gs == 0
    )


def run_sourced(z, outs, tokens, cotangent, routes, router_group, router_expert, gate_proj, up_proj, down_proj):
    z.nj = 2
    z.cc = z.cw // z.nj
    z.blk = z.gs * z.cap
    z.per = z.rl // 4
    z.order_end = (
        "t1 a10 b00 a11", "b01 a12 b02 a13", "b03 m1 b10 t3", "a30 b11 a31 b12", "a32 s2 s3 b13",
        "a33 m3 c02 p02", "C02 d02 t2 a20", "b30 b31 a21 c31", "a22 b32 p31 b33", "a23 m2 C31 b20",
        "b21 D31 r1 c21", "b22 p21 b23 C21", "D21 e3 f3 e1", "e0 g0 e2 x", "r0 f2 f1 g1", "g2 y g3 g4",
        "g5 g6 g7 q", "h w0 w1 f0", "w2 w3 w4 w5", "w6 w7",
    )
    z.order_mid = (
        "t1 a10 b00 a11", "b01 a12 b02 a13", "b03 m1 t2 a20", "a21 a22 a23 m2", "b10 b11 c02 b12",
        "p02 b13 C02 d02", "r1 b20 b21 c21", "b22 p21 b23 t3", "a30 a31 C21 a32", "a33 m3 D21 e0",
        "e1 f1 b30 b31", "c31 b32 p31 b33", "C31 e2 f2 D31", "g0 g1 g2 g3", "e3 x r0 f3", "g4 g5 g6 g7",
        "q h y w0", "w1 w2 f0 w3", "w4 w5 w6 w7",
    )
    nj, ng, cc = z.nj, 2 * z.nj, z.cc
    V = pltpu.VMEM
    args = (tokens, cotangent, routes.T, router_expert.T, router_group.T, gate_proj[0], up_proj[0], down_proj[0])
    hb = z.cw // z.ch // z.gs
    scratch = [V(a.shape, a.dtype) for a in args] + [
        V((z.rl, z.width), BF), V((z.rows, z.r1), BF), V((z.r1, z.rows), BF),
        V((z.r1, z.blk), BF), V((z.blk, z.r1), BF),
        V((z.r1, z.rl), BF), V((z.r1, z.rl), BF),
        V((ng, z.r1, cc), BF), V((ng, z.r1, cc), BF),
        V((16 * 4, z.blk), BF), V((16 * 4 * z.gs, z.blk), BF),
        V((ng, z.pairs, cc), BF), V((ng, z.pairs, cc), BF), V((ng, z.pairs, cc), BF),
        V((z.pairs, z.ff), F32), V((z.pairs, z.ff), F32), V((z.pairs, z.ff), F32),
        V((z.ff, z.width), BF), V((z.ff, z.width), BF), V((z.width, z.ff), BF),
        V((z.pairs, 2 * z.ff), BF), V((z.pairs, z.ff), BF), V((z.ff, z.pairs), BF),
        V((z.pairs, z.rl), F32), V((z.pairs, z.rl), F32),
        V((nj, z.pairs, cc), BF), V((nj, z.pairs, cc), BF),
        V((16 * 4, z.blk), BF), V((16 * 4 * z.gs, z.blk), BF),
        V((nj, z.pairs, cc), BF), V((nj, z.pairs, cc), BF),
        V((nj, z.r1, cc), BF), V((nj, z.r1, cc), BF), V((z.r1, z.rl), BF),
        V((2, z.width), F32), V((2, z.width), F32),
        V((z.gs, hb, z.rw, z.ch), F32), V((z.gs - 1, hb, z.rw, z.ch), F32), V((hb, z.rw, z.ch), F32),
        V((z.groups, z.rw, z.ch), F32),
    ]
    D = pltpu.SemaphoreType.DMA
    sems = [D((len(args),))] + [
        D(s) for s in (
            (2,), (ng + 1, 3), (2,), (ng + 1, 4), (1,), (nj + 1, 4), (1,), (4,), (1,), (nj, 4),
            (2,), (nj + 1, 4), (1,), (nj,), (2,), (2,), (1,), (1,), (1,), (1,),
        )
    ]
    spec = pl.BlockSpec(memory_space=pltpu.VMEM)
    return pl.pallas_call(
        functools.partial(sourced, z),
        out_shape=[pltpu.VMEM(s, d) for s, d in outs],
        in_specs=[pl.BlockSpec(memory_space=pltpu.HBM)] * len(args),
        out_specs=[spec] * len(outs),
        scratch_shapes=scratch + sems,
        compiler_params=pltpu.CompilerParams(
            collective_id=0, has_side_effects=True, vmem_limit_bytes=44 * 2**20
        ),
    )(*[pltpu.with_memory_space_constraint(a, pltpu.HBM) for a in args])


def run_wide(z, outs, tokens, cotangent, routes, router_group, router_expert, gate_proj, up_proj, down_proj):
    h, nc, cc = z.half_chunks, z.nc, z.cc
    V = pltpu.VMEM
    chd = z.ch if z.reduce_here else 128
    scratch = [
        V((z.rl, z.width), BF), V((z.r1, z.rl), BF), V((z.r1, z.rl), BF),
        V((z.rows, z.r1), BF), V((z.r1, z.pairs), BF),
        V((z.r1, z.rl), BF), V((z.r1, z.rl), BF),
        V((nc, z.r1, cc), BF), V((nc, z.r1, cc), BF),
        V((z.pairs, z.rl), BF), V((z.pairs, z.rl), BF),
        V((nc, z.pairs, cc), BF), V((nc, z.pairs, cc), BF),
        V((8, 128), BF), V((nc, z.pairs, cc), BF),
        V((z.pairs, z.ff), F32), V((z.pairs, z.ff), F32), V((z.pairs, z.ff), F32),
        V((z.pairs, 2 * z.ff), BF), V((z.pairs, z.ff), BF), V((z.pairs, 128), F32),
        V((z.pairs, 128), F32), V((z.pairs, 128), F32),
        V((h, z.pairs, cc), BF), V((h, z.pairs, cc), BF), V((h, z.pairs, cc), BF),
        V((z.pairs, z.rl), BF), V((z.pairs, z.rl), BF),
        V((h, z.pairs, cc), BF), V((h, z.pairs, cc), BF),
        V((z.r1, z.rl), BF), V((z.r1, z.rl), BF),
        V((h, z.r1, cc), BF), V((h, z.r1, cc), BF),
        V((2, z.width), F32), V((2, z.width), F32),
        V((z.n_ep, z.rw, chd), F32), V((z.n_ep // 2, z.rw, chd), F32),
        V((z.rw, chd), F32), V((z.rw, chd), F32),
    ]
    D = pltpu.SemaphoreType.DMA
    sems = [
        D((nc + 2, z.groups)), D((nc + 2, z.groups)), D((nc + 1, z.gs)), D((nc + 1, z.gs)),
        D((nc, z.gs)), D((nc, z.gs)), D((h,)), D((h,)),
        D((h + 1, z.gs)), D((h + 1, z.gs)), D((h + 1, z.groups)), D((h + 1, z.groups)),
        D((3,)), D((3,)), D((z.n_ep // 2,)), D((z.n_ep // 2,)),
    ]
    spec = pl.BlockSpec(memory_space=pltpu.VMEM)
    return pl.pallas_call(
        functools.partial(kernel, z),
        out_shape=[jax.ShapeDtypeStruct(s, d) for s, d in outs],
        in_specs=[spec] * 8,
        out_specs=[spec] * len(outs),
        scratch_shapes=scratch + sems,
        compiler_params=pltpu.CompilerParams(
            collective_id=0, has_side_effects=True, vmem_limit_bytes=44 * 2**20
        ),
    )(tokens, cotangent, routes.T, router_expert.T, router_group.T, gate_proj[0], up_proj[0], down_proj[0])


def body(axes, tokens, cotangent, routes, router_group, router_expert, gate_proj, up_proj, down_proj):
    z = sizes_of(axes, tokens, routes, router_group, router_expert, gate_proj)
    rout_shape = (z.rw, z.ch) if z.reduce_here else (min(z.rw, z.rl), z.width)
    outs = [
        ((z.rows, z.cw), BF), ((z.width, z.ff), BF), ((z.width, z.ff), BF), ((z.ff, z.width), BF),
        ((1, z.width), F32), ((1, z.width), F32), ((1, z.ff), F32), (rout_shape, F32),
    ]
    spec = pl.BlockSpec(memory_space=pltpu.VMEM)
    D = pltpu.SemaphoreType.DMA
    run = run_sourced if by_source(z) else run_wide
    tg, gate, up, down, gsq, usq, dsq, rout = run(
        z, outs, tokens, cotangent, routes, router_group, router_expert, gate_proj, up_proj, down_proj
    )
    if z.reduce_here:
        half = z.ch // 2
        shapes = [gate, up, down, tg, gsq, usq, dsq]
        anywhere = pl.BlockSpec(memory_space=pl.ANY)
        gate, up, down, tg, gsq, usq, dsq, reg, rgg, rrows = pl.pallas_call(
            functools.partial(finish, z),
            out_shape=[jax.ShapeDtypeStruct(a.shape, a.dtype) for a in shapes]
            + [jax.ShapeDtypeStruct((n, half), F32) for n in (z.experts, z.groups, 1)],
            in_specs=[spec] * 8,
            out_specs=[anywhere] * 10,
            scratch_shapes=[pltpu.VMEM((n, half), F32) for n in (z.experts, z.groups, 1)] + [D((10,))],
            compiler_params=pltpu.CompilerParams(vmem_limit_bytes=16 * 2**20),
        )(*shapes, rout)
        reg, rgg, rrows = reg.T, rgg.T, rrows[0]
    else:
        mine = lax.psum_scatter(rout.T, ("ep", "tp"), scatter_dimension=0, tiled=True)
        reg = mine[:, : z.experts]
        rgg = mine[:, z.experts : z.experts + z.groups]
        rrows = jnp.sum(reg * reg, axis=1) + jnp.sum(rgg * rgg, axis=1)
    return (tg, gate[None], up[None], down[None], gsq, usq, dsq, reg, rgg, rrows)


def solution(mesh):
    return jax.shard_map(
        functools.partial(body, dict(mesh.shape)),
        mesh=mesh,
        in_specs=(
            P("ep", None), P("ep", None), P("ep", None), P(), P(),
            P("ep", None, "tp"), P("ep", None, "tp"), P("ep", "tp", None),
        ),
        out_specs=(
            P("ep", "tp"), P("ep", None, "tp"), P("ep", None, "tp"), P("ep", "tp", None),
            P("ep", None), P("ep", None), P("ep", "tp"),
            P(("ep", "tp"), None), P(("ep", "tp"), None), P(("ep", "tp")),
        ),
        check_vma=False,
    )
```

```python
import functools

import jax
import jax.numpy as jnp
from jax import lax
from jax.experimental import pallas as pl
from jax.experimental.pallas import tpu as pltpu
from jax.sharding import PartitionSpec as P

MESH = pl.DeviceIdType.MESH
BF = jnp.bfloat16
F32 = jnp.float32


def mm(a, b, da=1, db=0):
    return lax.dot_general(a, b, (((da,), (db,)), ((), ())), preferred_element_type=F32)


def lanes_of(shape, dim=1):
    return lax.broadcasted_iota(jnp.int32, shape, dim)


class Sizes:
    pass


def sizes_of(mesh, tokens, routes, router_group, router_expert, gate_proj):
    z = Sizes()
    z.n_ep, z.n_tp = mesh["ep"], mesh["tp"]
    z.rows, z.width = tokens.shape
    z.top = routes.shape[1]
    z.groups, z.experts = router_group.shape[1], router_expert.shape[1]
    z.gs = z.experts // z.groups
    z.cap = z.rows // z.gs
    z.gr = z.gs * z.cap // z.top
    z.r1 = z.groups * z.gr
    z.sl = z.groups * z.cap
    z.pairs = z.gs * z.sl
    z.ff = gate_proj.shape[2]
    z.cw = z.width // z.n_tp
    z.half_chunks = 4
    z.nc = 2 * z.half_chunks
    z.cc = z.cw // z.half_chunks
    z.rl = -(-(z.experts + z.groups) // 128) * 128
    z.rw = -(-(z.experts + z.groups) // 8) * 8
    z.ch = z.width // z.n_ep
    z.reduce_here = z.ch % 128 == 0 and z.n_ep % 2 == 0
    assert z.experts == z.n_ep and z.n_tp == 2 and z.top == 2
    assert z.sl & (z.sl - 1) == 0 and z.gr & (z.gr - 1) == 0
    return z


def kernel(
    z, tok_ref, cot_ref, routes_ref, rexp_ref, rgrp_ref, gate_ref, up_ref, down_ref,
    tg_out, gate_out, up_out, down_out, gsq_out, usq_out, dsq_out, rout_out,
    rc_ref, s1w, r1w,
    s_mat, t_mat, s1m, r1m, s1, r1, s2m, x2m, s2, x2, y2m, y2,
    gacc, uacc, pacc, dcat, hid, wcol, wp, wpr, pts, ptr, pto,
    s3m, r3m, s3, r3, s4m, r4m, s4, r4, sq, sqr, term, trec, tsum, tsumr,
    z1s, z1r, p2s, p2r, fs, fr, ptsm, ptrm, r3s, r3r, r4s, r4r, ms, mr, ts, tr,
):
    e, t = lax.axis_index("ep"), lax.axis_index("tp")
    g, p = e // z.gs, e % z.gs
    other = 1 - t

    def rcopy(src, dst, ss, rs, ep, tp):
        return pltpu.make_async_remote_copy(
            src_ref=src, dst_ref=dst, send_sem=ss, recv_sem=rs,
            device_id=(ep, tp), device_id_type=MESH,
        )

    barrier = pltpu.get_barrier_semaphore()
    for d in range(1, z.n_ep):
        pl.semaphore_signal(
            barrier, inc=1, device_id=((e + d) % z.n_ep, t), device_id_type=MESH
        )
    pl.semaphore_signal(barrier, inc=1, device_id=(e, other), device_id_type=MESH)

    sends = []

    def grows(h):
        return pl.ds(pl.multiple_of(h * z.gr, z.gr), z.gr)

    def prows(q):
        return pl.ds(pl.multiple_of(q * z.sl, z.sl), z.sl)

    def group_send(src, dst, ss, rs, c):
        for d in range(1, z.groups):
            h = (g + d) % z.groups
            cp = rcopy(src.at[grows(h)], dst.at[grows(g)], ss.at[c, d], rs.at[c, d], h * z.gs + p, t)
            cp.start()
            sends.append(cp)
        dst[grows(g), :] = src[grows(g), :]

    def group_wait(src, dst, ss, rs, c):
        for d in range(1, z.groups):
            h = (g + z.groups - d) % z.groups
            rcopy(src.at[grows(h)], dst.at[grows(h)], ss.at[c, d], rs.at[c, d], h * z.gs + p, t).wait_recv()

    def plane_send(src, dst, ss, rs, c):
        for d in range(1, z.gs):
            q = (p + d) % z.gs
            cp = rcopy(src.at[prows(q)], dst.at[prows(p)], ss.at[c, d], rs.at[c, d], g * z.gs + q, t)
            cp.start()
            sends.append(cp)
        dst[prows(p), :] = src[prows(p), :]

    def plane_wait_one(src, dst, ss, rs, c, d):
        q = (p + z.gs - d) % z.gs
        rcopy(src.at[prows(q)], dst.at[prows(q)], ss.at[c, d], rs.at[c, d], g * z.gs + q, t).wait_recv()

    def plane_wait(src, dst, ss, rs, c):
        for d in range(1, z.gs):
            plane_wait_one(src, dst, ss, rs, c, d)

    def pair_send(src, dst, ss, rs):
        cp = rcopy(src, dst, ss, rs, e, other)
        cp.start()
        sends.append(cp)
        return cp

    lane = lanes_of((z.rows, z.rl))
    eye = lanes_of((z.rows, z.rows), 0) == lanes_of((z.rows, z.rows), 1)

    def column(row):
        return jnp.sum(jnp.where(eye, row.astype(F32), 0.0), axis=1, keepdims=True).astype(jnp.int32)

    r0, r1_ = column(routes_ref[0:1, :]), column(routes_ref[1:2, :])
    chosen = (lane == r0) | (lane == r1_)
    low = (lane - z.experts) * z.gs
    is_group = (lane >= z.experts) & (lane < z.experts + z.groups)
    in_group = is_group & (r0 >= low) & (r0 < low + z.gs)

    def before(n):
        return (lanes_of((n, n), 1) < lanes_of((n, n), 0)).astype(F32).astype(BF)

    ghot = in_group.astype(F32)
    grank = mm(before(z.rows), ghot.astype(BF))
    grank = jnp.where(in_group, grank, -1.0).astype(BF)
    er, el = lanes_of((z.rl, z.r1), 0) - z.experts, lanes_of((z.rl, z.r1), 1)
    expand = ((el >= er * z.gr) & (el < (er + 1) * z.gr)).astype(F32).astype(BF)
    place = (lanes_of((z.rows, z.r1)) & (z.gr - 1)).astype(F32)
    s_mat[...] = (mm(grank, expand) == place).astype(F32).astype(BF)

    s1m[...] = mm(s_mat[...], chosen.astype(F32).astype(BF), 0, 0).astype(BF)
    pl.semaphore_wait(barrier, z.n_ep)
    group_send(s1m, r1m, z1s, z1r, z.nc)

    def cols_at(half, k):
        return pl.ds(pl.multiple_of(half * z.cw + k * z.cc, z.cc), z.cc)

    for c in range(z.nc):
        src = tok_ref if c < z.half_chunks else cot_ref
        s1[c] = mm(s_mat[...], src[:, cols_at(t, c % z.half_chunks)], 0, 0).astype(BF)
        group_send(s1.at[c], r1.at[c], z1s, z1r, c)

    rc_ref[...] = jnp.zeros_like(rc_ref)
    rc_ref[0 : z.experts, :] = rexp_ref[...]
    rc_ref[z.experts : z.experts + z.groups, :] = rgrp_ref[...]
    expd = jnp.exp(mm(tok_ref[...], rc_ref[...], 1, 1))
    gexp = jnp.where(is_group, expd, 0.0)
    gprob = gexp / jnp.sum(gexp, axis=1, keepdims=True)
    picked = jnp.sum(jnp.where(in_group, gprob, 0.0), axis=1, keepdims=True)
    pexp = jnp.where(chosen, expd, 0.0)
    paired = pexp / jnp.sum(pexp, axis=1, keepdims=True)
    s1w[...] = mm(s_mat[...], (picked * paired).astype(BF), 0, 0).astype(BF)
    group_send(s1w, r1w, z1s, z1r, z.nc + 1)

    group_wait(s1m, r1m, z1s, z1r, z.nc)
    vals = r1m[...]
    lane1 = lanes_of((z.r1, z.rl))
    member = (vals.astype(F32) > 0.0) & (lane1 < z.experts)
    rank = mm(before(z.r1), member.astype(F32).astype(BF))
    rank = jnp.where(member, rank, -1.0).astype(BF)
    er, el = lanes_of((z.rl, z.pairs), 0) - g * z.gs, lanes_of((z.rl, z.pairs), 1)
    expand = ((el >= er * z.sl) & (el < (er + 1) * z.sl)).astype(F32).astype(BF)
    place = (lanes_of((z.r1, z.pairs)) & (z.sl - 1)).astype(F32)
    t_mat[...] = (mm(rank, expand) == place).astype(F32).astype(BF)

    def pack_two(c):
        group_wait(s1.at[c], r1.at[c], z1s, z1r, c)
        s2[c] = mm(t_mat[...], r1[c], 0, 0).astype(BF)
        plane_send(s2.at[c], x2.at[c], p2s, p2r, c)
        pair_send(x2.at[c, prows(p)], y2.at[c, prows(p)], fs.at[c, 0], fr.at[c, 0])

    def accumulate(x, half, c):
        if c < z.half_chunks:
            at = cols_at(half, c)
            gate_add, up_add = mm(x, gate_ref[at, :]), mm(x, up_ref[at, :])
            gacc[...] += gate_add
            uacc[...] += up_add
        else:
            pacc[...] += mm(x, down_ref[:, cols_at(half, c - z.half_chunks)], 1, 1)

    def land(c):
        for d in range(1, z.gs):
            plane_wait_one(s2.at[c], x2.at[c], p2s, p2r, c, d)
            q = (p + z.gs - d) % z.gs
            pair_send(x2.at[c, prows(q)], y2.at[c, prows(q)], fs.at[c, d], fr.at[c, d])
        accumulate(x2[c], t, c)

    def land_other(c):
        for d in range(z.gs):
            q = (p + z.gs - d) % z.gs
            rcopy(x2.at[c, prows(q)], y2.at[c, prows(q)], fs.at[c, d], fr.at[c, d], e, other).wait_recv()
        accumulate(y2[c], other, c)

    gacc[...] = jnp.zeros_like(gacc)
    uacc[...] = jnp.zeros_like(uacc)
    pacc[...] = jnp.zeros_like(pacc)
    for c in range(z.nc + 3):
        if c < z.nc:
            pack_two(c)
        if c == z.nc - 1:
            group_wait(s1w, r1w, z1s, z1r, z.nc + 1)
            s2m[...] = mm(t_mat[...], r1w[...], 0, 0).astype(BF)
            plane_send(s2m, x2m, p2s, p2r, z.nc)
        if 2 <= c < z.nc + 2:
            land(c - 2)
        if c >= 3:
            land_other(c - 3)
    plane_wait(s2m, x2m, p2s, p2r, z.nc)

    lane2 = lanes_of((z.pairs, z.rl))
    scale = jnp.sum(jnp.where(lane2 == e, x2m[...].astype(F32), 0.0), axis=1, keepdims=True)
    wcol[...] = jnp.broadcast_to(scale, wcol.shape)
    gate_pre, up_pre, pulled = gacc[...], uacc[...], pacc[...]
    sig = 1.0 / (1.0 + jnp.exp(-gate_pre))
    silu = gate_pre * sig
    hidden = (silu * up_pre).astype(BF)
    hid[...] = hidden
    wp[...] = jnp.broadcast_to(
        jnp.sum(pulled * hidden.astype(F32), axis=1, keepdims=True), wp.shape
    )
    w_copy = pair_send(wp, wpr, ms.at[0], mr.at[0])
    dh = scale * pulled
    dcat[:, : z.ff] = (dh * up_pre * sig * (1.0 + gate_pre * (1.0 - sig))).astype(BF)
    dcat[:, z.ff :] = (dh * silu).astype(BF)

    def token_term(half, k):
        at = cols_at(half, k)
        return (
            mm(dcat[:, : z.ff], gate_ref[at, :], 1, 1) + mm(dcat[:, z.ff :], up_ref[at, :], 1, 1)
        ).astype(BF)

    pt = []
    for k in range(z.half_chunks):
        pts[k] = token_term(other, k)
        pt.append(pair_send(pts.at[k], ptr.at[k], ptsm.at[k], ptrm.at[k]))
    w_copy.wait_recv()
    wsum = wp[:, 0:1] + wpr[:, 0:1]
    s3m[...] = jnp.where(lane2 == e, wsum, 0.0).astype(BF)
    plane_send(s3m, r3m, r3s, r3r, z.half_chunks)
    for k in range(z.half_chunks):
        pto[k] = token_term(t, k)
        pt[k].wait_recv()
        s3[k] = (pto[k].astype(F32) + ptr[k].astype(F32)).astype(BF)
        plane_send(s3.at[k], r3.at[k], r3s, r3r, k)

    ones_ff = jnp.ones((16, z.ff), BF)

    def gate_up_grads(xs, half, k):
        at = cols_at(half, k)
        total = mm(xs[k], dcat[...], 0, 0)
        gate_out[at, :] = total[:, : z.ff].astype(BF)
        up_out[at, :] = total[:, z.ff :].astype(BF)
        square = (total * total).astype(BF)
        sq[0:1, at] = mm(ones_ff, square[:, : z.ff], 1, 1)[0:1]
        sq[1:2, at] = mm(ones_ff, square[:, z.ff :], 1, 1)[0:1]

    def down_grads(xs, half, k):
        scaled = (wcol[:, 0:1] * xs[z.half_chunks + k].astype(F32)).astype(BF)
        total = mm(hid[...], scaled, 0, 0)
        down_out[:, cols_at(half, k)] = total.astype(BF)
        return mm(jnp.ones((16, z.cc), BF), (total * total).astype(BF), 1, 1)[0:1]

    def back_two(k):
        plane_wait(s3.at[k], r3.at[k], r3s, r3r, k)
        s4[k] = mm(t_mat[...], r3[k]).astype(BF)
        group_send(s4.at[k], r4.at[k], r4s, r4r, k)

    gate_up_grads(x2, t, 0)
    plane_wait(s3m, r3m, r3s, r3r, z.half_chunks)
    s4m[...] = mm(t_mat[...], r3m[...]).astype(BF)
    group_send(s4m, r4m, r4s, r4r, z.half_chunks)
    gate_up_grads(x2, t, 1)
    for k in range(z.half_chunks - 1):
        back_two(k)
        if k + 2 < z.half_chunks:
            gate_up_grads(x2, t, k + 2)
        else:
            gate_up_grads(y2, other, 0)

    group_wait(s4m, r4m, r4s, r4r, z.half_chunks)
    dw = mm(s_mat[...], r4m[...])
    dpicked = jnp.sum(dw * paired, axis=1, keepdims=True)
    q = picked * dw
    dchosen = paired * (q - jnp.sum(paired * q, axis=1, keepdims=True))
    dgroup = jnp.where(is_group, (dpicked * picked) * (ghot - gprob), 0.0)
    dall = (dchosen + dgroup).astype(BF)
    dterm = dall[:, : z.rw] if z.rw < z.rl else dall
    tcopies = []
    if z.reduce_here:
        full = mm(dterm, tok_ref[...], 0, 0)
        for i in range(z.n_ep):
            term[i] = full[:, i * z.ch : (i + 1) * z.ch]

        def term_copy(m):
            to = (e + 2 * m + t) % z.n_ep
            return rcopy(term.at[to], trec.at[m], ts.at[m], tr.at[m], to, t)

        @pl.when(t == 0)
        def _():
            trec[0] = term[e]

        @pl.when(t == 1)
        def _():
            term_copy(0).start()

        for m in range(1, z.n_ep // 2):
            term_copy(m).start()
    else:
        row = lanes_of((z.rows, z.rl), 0)[:, : dterm.shape[1]]
        mine = (row >= t * (z.rows // 2)) & (row < (t + 1) * (z.rows // 2))
        dterm = jnp.where(mine, dterm.astype(F32), 0.0).astype(BF)
        rout_out[...] = mm(dterm, tok_ref[...], 0, 0)

    back_two(z.half_chunks - 1)
    for k in range(1, z.half_chunks):
        gate_up_grads(y2, other, k)
    sq_copy = pair_send(sq, sqr, ms.at[1], mr.at[1])
    dsq = jnp.zeros((1, z.ff), F32)
    for k in range(z.half_chunks):
        dsq += down_grads(x2, t, k)

    if z.reduce_here:

        @pl.when(t == 1)
        def _():
            term_copy(0).wait_recv()

        for m in range(1, z.n_ep // 2):
            term_copy(m).wait_recv()
        acc = trec[0]
        for m in range(1, z.n_ep // 2):
            acc = acc + trec[m]
        tsum[...] = acc
        t_pair = pair_send(tsum, tsumr, ms.at[2], mr.at[2])
    for k in range(z.half_chunks):
        dsq += down_grads(y2, other, k)
    dsq_out[...] = dsq

    for k in range(z.half_chunks):
        group_wait(s4.at[k], r4.at[k], r4s, r4r, k)
        tg_out[:, k * z.cc : (k + 1) * z.cc] = (
            mm(s_mat[...], r4[k]) + mm(dall, rc_ref[:, cols_at(t, k)])
        ).astype(BF)
    sq_copy.wait_recv()
    gsq_out[...] = sq[0:1, :] + sqr[0:1, :]
    usq_out[...] = sq[1:2, :] + sqr[1:2, :]
    if z.reduce_here:
        t_pair.wait_recv()
        rout_out[...] = tsum[...] + tsumr[...]

        @pl.when(t == 1)
        def _():
            term_copy(0).wait_send()

        for m in range(1, z.n_ep // 2):
            term_copy(m).wait_send()
    for cp in sends:
        cp.wait_send()


def sourced(
    z, tok_h, cot_h, routes_h, rexp_h, rgrp_h, gate_h, up_h, down_h,
    tg_out, gate_out, up_out, down_out, gsq_out, usq_out, dsq_out, rout_out,
    tok_ref, cot_ref, routes_ref, rexp_ref, rgrp_ref, gate_ref, up_ref, down_ref,
    rc_ref, s_mat, s_tr, t_mat, t_tr, s1w, r1w, s1, r1, s2m, x2m, s2, x2, y2,
    gacc, uacc, pacc, gate_tr, up_tr, down_tr,
    dcat, hid, hid_tr, wp, wpr, pts, ptr, s3m, r3m, s3, r3, s4, r4, dall_ref,
    sq, sqr, term, tra, tsa, trb,
    ins, z1s, z1r, p2s, p2r, fs, fr, ws, wr, ptsm, ptrm, r3s, r3r, r4s, r4r, ms, mr, tas, tar, tbs, tbr,
):
    e, t = lax.axis_index("ep"), lax.axis_index("tp")
    g, p = e // z.gs, e % z.gs
    other = 1 - t
    hk = [g, g + 1 - 2 * (g % 2), 3 - g, (g + 2) % 4]
    qd = [p, p + 1 - 2 * (p % 2), (p + 2) % 4, 3 - p]
    inner = (g + 1) // 2 == 1
    nj, cc, gr, cap, blk, per = z.nj, z.cc, z.gr, z.cap, z.blk, z.per
    ng = 2 * nj
    far = (1, 2, 3)

    def rcopy(src, dst, ss, rs, ep, tp):
        return pltpu.make_async_remote_copy(
            src_ref=src, dst_ref=dst, send_sem=ss, recv_sem=rs,
            device_id=(ep, tp), device_id_type=MESH,
        )

    barrier = pltpu.get_barrier_semaphore()
    for k in far:
        pl.semaphore_signal(barrier, inc=1, device_id=(hk[k] * z.gs + p, t), device_id_type=MESH)
        pl.semaphore_signal(barrier, inc=1, device_id=(hk[k] * z.gs + p, other), device_id_type=MESH)
        pl.semaphore_signal(barrier, inc=1, device_id=(g * z.gs + qd[k], t), device_id_type=MESH)
    pl.semaphore_signal(barrier, inc=1, device_id=(e, other), device_id_type=MESH)

    loads = [
        pltpu.make_async_copy(a, b, ins.at[i])
        for i, (a, b) in enumerate((
            (routes_h, routes_ref), (tok_h, tok_ref), (rexp_h, rexp_ref), (rgrp_h, rgrp_ref),
            (cot_h, cot_ref), (gate_h, gate_ref), (up_h, up_ref), (down_h, down_ref),
        ))
    ]
    for cp in loads:
        cp.start()

    def kr(k, n=1):
        return pl.ds(k * gr, n * gr)

    def kb(k, n=1):
        return pl.ds(k * blk, n * blk)

    def in_block(k, q):
        return pl.ds(pl.multiple_of(k * blk + q * cap, cap), cap)

    def three(k):
        return pl.ds(k * blk, 3 * cap)

    def cols(half, j):
        return pl.ds(pl.multiple_of(half * z.cw + j * cc, cc), cc)

    def z_copy(src, dst, c, k):
        return rcopy(src.at[kr(k)], dst.at[kr(k)], z1s.at[c // ng], z1r.at[c, k - 1], hk[k] * z.gs + p, t)

    def spread(src, dst, ss, rs, k):
        for d in (3, 1, 2):
            rcopy(src.at[in_block(k, qd[d])], dst.at[in_block(k, p)], ss, rs, g * z.gs + qd[d], t).start()
        dst[in_block(k, p), :] = src[in_block(k, p), :]

    def gathered(src, dst, ss, rs, k):
        rcopy(src.at[three(k)], dst.at[three(k)], ss, rs, g * z.gs + qd[3], t).wait_recv()

    def line_out(src, dst, ss, rs, k, line):
        mine = pl.ds(pl.multiple_of((k * z.gs + p) * 16, 16), 16)
        src[k * 16 : (k + 1) * 16, :] = line.astype(BF)
        for d in (3, 1, 2):
            rcopy(src.at[pl.ds(k * 16, 16)], dst.at[mine], ss, rs, g * z.gs + qd[d], t).start()
        dst[mine, :] = src[k * 16 : (k + 1) * 16, :]

    def line_wait(dst, ss, rs, k):
        part = dst.at[pl.ds(k * z.gs * 16, 48)]
        rcopy(part, part, ss, rs, g * z.gs + qd[3], t).wait_recv()

    def line_column(dst, k):
        tiles = []
        for q in range(z.gs):
            at = (k * z.gs + q) * 16
            tiles += [dst[at : at + 16, :]] * (cap // 16)
        rows = jnp.concatenate(tiles, axis=0).astype(F32)
        r, c = lanes_of((blk, blk), 0), lanes_of((blk, blk), 1)
        return jnp.sum(jnp.where(c == p * cap + r % cap, rows, 0.0), axis=1, keepdims=True)

    def pair(src, dst, ss, rs):
        return rcopy(src, dst, ss, rs, e, other)

    lane = lanes_of((z.rows, z.rl))
    ll, lb = lane % per, lane // per
    eye = lanes_of((z.rows, z.rows), 0) == lanes_of((z.rows, z.rows), 1)

    def column(row):
        return jnp.sum(jnp.where(eye, row.astype(F32), 0.0), axis=1, keepdims=True).astype(jnp.int32)

    def before(n):
        r, c = lanes_of((n, n), 0), lanes_of((n, n), 1)
        return ((c < r) & (r // gr == c // gr)).astype(F32).astype(BF)

    def make_t(k, n):
        m = n * gr
        vals = r1w[kr(k, n), :]
        member = (vals.astype(F32) > 0.0) & (lanes_of((m, z.rl)) < z.experts)
        rank = mm(before(m), member.astype(F32).astype(BF))
        rank = jnp.where(member, rank, -1.0).astype(BF)
        sr, sc = lanes_of((z.rl, blk), 0) - g * z.gs, lanes_of((z.rl, blk), 1)
        expand = (sr == sc // cap).astype(F32).astype(BF)
        spot = (lanes_of((m, blk)) % cap).astype(F32)
        tf = (mm(rank, expand) == spot).astype(F32)
        t_mat[kr(k, n), :] = tf.astype(BF)
        t_tr[:, kr(k, n)] = tf.T.astype(BF)

    def t_rows(k):
        return t_mat[k * gr : (k + 1) * gr, :]

    def t_cols(k):
        return t_tr[:, k * gr : (k + 1) * gr]

    loads[0].wait()
    r0, r1_ = column(routes_ref[0:1, :]), column(routes_ref[1:2, :])
    chosen = (ll == r0) | (ll == r1_)
    low = (ll - z.experts) * z.gs
    is_group = (ll >= z.experts) & (ll < z.experts + z.groups)
    in_group = is_group & (r0 >= low) & (r0 < low + z.gs)
    tri = lanes_of((z.rows, z.rows), 1) < lanes_of((z.rows, z.rows), 0)
    grank = mm(tri.astype(F32).astype(BF), in_group.astype(F32).astype(BF))
    grank = jnp.where(in_group, grank, -1.0).astype(BF)
    er, el = lanes_of((z.rl, z.r1), 0) - z.experts, lanes_of((z.rl, z.r1), 1)
    kk = el // gr
    want = jnp.where(kk == 0, hk[0], jnp.where(kk == 1, hk[1], jnp.where(kk == 2, hk[2], hk[3])))
    expand = (er == want).astype(F32).astype(BF)
    place = (lanes_of((z.rows, z.r1)) % gr).astype(F32)
    s_f = (mm(grank, expand) == place).astype(F32)
    s_mat[...] = s_f.astype(BF)
    s_tr[...] = s_f.T.astype(BF)
    pick_mask = jnp.where(chosen & (lb == 0), 1.0, 0.0)
    r1w[kr(0), :] = mm(s_tr[kr(0), :], pick_mask.astype(BF)).astype(BF)

    def fill(c):
        j = c % nj
        src = tok_ref if c < nj else cot_ref
        s1[c] = mm(s_tr[...], src[:, cols(t, j)]).astype(BF)
        r1[c, kr(0), :] = s1[c, kr(0), :]

    def near_out(c):
        z_copy(s1.at[c], r1.at[c], c, 1).start()

        @pl.when(inner)
        def _():
            z_copy(s1.at[c], r1.at[c], c, 2).start()

    def op_a(k, c):
        if k:
            z_copy(s1.at[c], r1.at[c], c, k).wait_recv()
        s2[c, kb(k), :] = mm(t_cols(k), r1[c, kr(k), :]).astype(BF)
        spread(s2.at[c], x2.at[c], p2s.at[0], p2r.at[c, k], k)

    def op_am(k):
        er, ec = lanes_of((z.rl, blk), 0), lanes_of((z.rl, blk), 1)
        pick = (er == per + g * z.gs + ec // cap).astype(F32).astype(BF)
        weight = mm(r1w[kr(k), :], pick) * t_rows(k).astype(F32)
        line_out(s2m, x2m, p2s.at[1], p2r.at[ng, k], k, mm(jnp.ones((16, gr), BF), weight.astype(BF)))

    make_t(0, 1)
    loads[1].wait()
    fill(0)
    pl.semaphore_wait(barrier, 10)
    near_out(0)
    op_a(0, 0)
    for c in range(1, nj):
        fill(c)
        near_out(c)
        op_a(0, c)

    rc_ref[...] = jnp.zeros_like(rc_ref)
    loads[2].wait()
    loads[3].wait()
    for b in range(z.rl // per):
        rc_ref[b * per : b * per + z.experts, :] = rexp_ref[...]
        rc_ref[b * per + z.experts : b * per + z.experts + z.groups, :] = rgrp_ref[...]
    expd = jnp.exp(mm(tok_ref[...], rc_ref[...], 1, 1))
    gexp = jnp.where(is_group, expd, 0.0)
    gprob = gexp / jnp.sum(jnp.where(lb == 0, gexp, 0.0), axis=1, keepdims=True)
    picked = jnp.sum(jnp.where(in_group & (lb == 0), gprob, 0.0), axis=1, keepdims=True)
    pexp = jnp.where(chosen, expd, 0.0)
    paired = pexp / jnp.sum(jnp.where(lb == 0, pexp, 0.0), axis=1, keepdims=True)
    both = paired + gprob
    upper = both.astype(BF).astype(F32)
    meta = jnp.where(lb == 1, picked * paired, jnp.where(lb == 2, upper, jnp.where(lb == 3, both - upper, pick_mask)))
    s1w[...] = mm(s_tr[...], meta.astype(BF)).astype(BF)
    r1w[kr(0), :] = s1w[kr(0), :]
    for k in far:
        z_copy(s1w, r1w, ng, k).start()
    loads[4].wait()
    for c in range(nj, ng):
        fill(c)
        near_out(c)
        op_a(0, c)

    def op_s(k):
        for c in range(ng):
            z_copy(s1.at[c], r1.at[c], c, k).start()

    @pl.when(inner)
    def _():
        op_s(3)

    op_am(0)

    def op_t(k):
        z_copy(s1w, r1w, ng, k).wait_recv()
        make_t(k, 1)

    def relay(k, c):
        return pair(x2.at[c, kb(k)], y2.at[c, kb(k)], fs.at[0], fr.at[max(0, c - nj + 1), k])

    def op_b(k, c):
        gathered(s2.at[c], x2.at[c], p2s.at[0], p2r.at[c, k], k)
        relay(k, c).start()

    def op_c1(k, n):
        ga = ua = None
        for half, xs in ((t, x2), (other, y2)):
            for j in range(nj):
                if xs is y2 and j == 0:
                    for i in range(n):
                        both_in = pl.ds(0, nj), kb(k + i)
                        pair(x2.at[both_in], y2.at[both_in], fs.at[0], fr.at[0, k + i]).wait_recv()
                x, at = xs[j, kb(k, n), :], cols(half, j)
                a, b = mm(x, gate_ref[at, :]), mm(x, up_ref[at, :])
                ga, ua = (a, b) if ga is None else (ga + a, ua + b)
        gacc[kb(k, n), :] = ga
        uacc[kb(k, n), :] = ua

    def token_term(k, n, half, j):
        at = cols(half, j)
        return (
            mm(dcat[kb(k, n), : z.ff], gate_tr[:, at]) + mm(dcat[kb(k, n), z.ff :], up_tr[:, at])
        ).astype(BF)

    def w_pair(k, n):
        return pair(wp.at[kb(k, n)], wpr.at[kb(k, n)], ws.at[0], wr.at[k])

    def pt_pair(j, k, n):
        return pair(pts.at[j, kb(k, n)], ptr.at[j, kb(k, n)], ptsm.at[0], ptrm.at[j, k])

    def pull(k, n, js, pulled):
        for half, xs in ((t, x2), (other, y2)):
            for j in js:
                if xs is y2:
                    for i in range(n):
                        relay(k + i, nj + j).wait_recv()
                a = mm(xs[nj + j, kb(k, n), :], down_tr[cols(half, j), :])
                pulled = a if pulled is None else pulled + a
        return pulled

    def op_p(k, n):
        pacc[kb(k, n), :] = pull(k, n, range(nj - 1), None)

    def op_c2(k, n):
        pulled = pull(k, n, (nj - 1,), pacc[kb(k, n), :])
        for i in range(n):
            line_wait(x2m, p2s.at[1], p2r.at[ng, k + i], k + i)
        m = n * blk
        scale = jnp.concatenate([line_column(x2m, k + i) for i in range(n)], axis=0)
        gate_pre, up_pre = gacc[kb(k, n), :], uacc[kb(k, n), :]
        sig = 1.0 / (1.0 + jnp.exp(-gate_pre))
        silu = gate_pre * sig
        product = silu * up_pre
        hidden = product.astype(BF)
        hid[kb(k, n), :] = (scale * product).astype(BF)
        wp[kb(k, n), :] = jnp.broadcast_to(
            jnp.sum(pulled * hidden.astype(F32), axis=1, keepdims=True), (m, z.rl)
        )
        w_pair(k, n).start()
        dh = scale * pulled
        dcat[kb(k, n), : z.ff] = (dh * up_pre * sig * (1.0 + gate_pre * (1.0 - sig))).astype(BF)
        dcat[kb(k, n), z.ff :] = (dh * silu).astype(BF)
        for j in range(nj):
            pts[j, kb(k, n), :] = token_term(k, n, other, j)
            pt_pair(j, k, n).start()

    def op_d(k, n, out=False):
        mine = token_term(k, n, t, 0)
        w_pair(k, n).wait_recv()
        wsum = wp[kb(k, n), :] + wpr[kb(k, n), :]
        same = lanes_of((blk, blk), 0) == lanes_of((blk, blk), 1)
        for i in range(n):
            diag = jnp.where(same, wsum[i * blk : (i + 1) * blk, :blk], 0.0).astype(BF)
            line_out(s3m, r3m, r3s.at[1], r3r.at[nj, k + i], k + i, mm(jnp.ones((16, blk), BF), diag))
        for j in range(nj):
            if j:
                mine = token_term(k, n, t, j)
            pt_pair(j, k, n).wait_recv()
            s3[j, kb(k, n), :] = (mine.astype(F32) + ptr[j, kb(k, n), :].astype(F32)).astype(BF)
            if out:
                spread(s3.at[j], r3.at[j], r3s.at[0], r3r.at[j, k], k)

    def op_dr(k, n):
        op_d(k, n, True)

    def op_r(k):
        for j in range(nj):
            spread(s3.at[j], r3.at[j], r3s.at[0], r3r.at[j, k], k)

    def home_copy(j, k):
        return rcopy(s4.at[j, kr(k)], r4.at[j, kr(k)], r4s.at[0], r4r.at[j], hk[k] * z.gs + p, t)

    lane3 = lanes_of((gr, z.rl))
    i1, i2 = lanes_of((z.rl, z.rl), 0), lanes_of((z.rl, z.rl), 1)
    fold = ((i2 < per) & ((i1 == 2 * per + i2) | (i1 == 3 * per + i2))).astype(F32).astype(BF)

    def op_e(k):
        vals = mm(r1w[kr(k), :], fold)
        g_lane = (lane3 >= z.experts) & (lane3 < z.experts + z.groups)
        pr = jnp.where(lane3 < z.experts, vals, 0.0)
        here = lane3 == z.experts + g
        pk = jnp.sum(jnp.where(here, vals, 0.0), axis=1, keepdims=True)
        line_wait(r3m, r3s.at[1], r3r.at[nj, k], k)
        lr, lc = lanes_of((blk, z.rl), 0), lanes_of((blk, z.rl), 1)
        dw = mm(t_rows(k), jnp.where(lc == g * z.gs + lr // cap, line_column(r3m, k), 0.0).astype(BF))
        dpicked = jnp.sum(dw * pr, axis=1, keepdims=True)
        q = pk * dw
        dchosen = pr * (q - jnp.sum(pr * q, axis=1, keepdims=True))
        dgroup = jnp.where(g_lane, (dpicked * pk) * (here.astype(F32) - vals), 0.0)
        dall_ref[kr(k), :] = (dchosen + dgroup).astype(BF)

    def op_f(k):
        dall = dall_ref[kr(k), :]
        for j in range(nj):
            gathered(s3.at[j], r3.at[j], r3s.at[0], r3r.at[j, k], k)
            row = (mm(t_rows(k), r3[j, kb(k), :]) + mm(dall, rc_ref[:, cols(t, j)])).astype(BF)
            if k:
                s4[j, kr(k), :] = row
                home_copy(j, k).start()
            else:
                r4[j, kr(k), :] = row

    sub = min(cc, 256)
    ns = cc // sub
    ones_ff = jnp.ones((16, z.ff), BF)
    ones_sub = jnp.ones((16, sub), BF)
    n_piece = z.cw // sub

    def gate_up_grads(i):
        half, xs = (t, x2) if i < n_piece else (other, y2)
        i = i % n_piece
        j, o = i // ns, (i % ns) * sub
        at = pl.ds(pl.multiple_of(half * z.cw + i * sub, sub), sub)
        total = mm(xs[j, :, o : o + sub], dcat[...], 0, 0)
        gate_out[at, :] = total[:, : z.ff].astype(BF)
        up_out[at, :] = total[:, z.ff :].astype(BF)
        square = (total * total).astype(BF)
        sq[0:1, at] = mm(ones_ff, square[:, : z.ff], 1, 1)[0:1]
        sq[1:2, at] = mm(ones_ff, square[:, z.ff :], 1, 1)[0:1]

    def down_grads(i):
        half, xs = (t, x2) if i < n_piece else (other, y2)
        i = i % n_piece
        j, o = i // ns, (i % ns) * sub
        at = pl.ds(pl.multiple_of(half * z.cw + i * sub, sub), sub)
        total = mm(hid_tr[...], xs[nj + j, :, o : o + sub])
        down_out[:, at] = total.astype(BF)
        return mm(ones_sub, (total * total).astype(BF), 1, 1)[0:1]

    loads[5].wait()
    gate_tr[...] = gate_ref[...].T
    loads[6].wait()
    up_tr[...] = up_ref[...].T
    loads[7].wait()
    down_tr[...] = down_ref[...].T

    per_core = z.cw // z.ch // z.gs
    home_core = g // per_core
    all_a = rcopy(term.at[pl.ds(0, 3)], tra, tas.at[0], tar.at[0], g * z.gs + qd[3], t)

    def term_b(k, core):
        return rcopy(tsa.at[hk[k] % per_core], trb.at[k], tbs.at[0], tbr.at[0], hk[k] * z.gs + p, core)

    t_pair = pair(tsa.at[g % per_core], trb.at[0], ms.at[1], mr.at[1])

    def op_x():
        dterm = dall_ref[:, : z.rw]
        for j in range(nj):
            full = mm(dterm, r1[j], 0, 0)
            for i in range(cc // z.ch):
                n = j * (cc // z.ch) + i
                term[n % z.gs, n // z.gs] = full[:, i * z.ch : (i + 1) * z.ch]
        for d in far:
            rcopy(term.at[qd[d]], tra.at[d - 1], tas.at[0], tar.at[0], g * z.gs + qd[d], t).start()

    def op_y():
        all_a.wait_recv()
        tsa[...] = term[p] + tra[0] + tra[1] + tra[2]
        for k in far:

            @pl.when(hk[k] // per_core == t)
            def _():
                for core in range(z.n_tp):
                    term_b(k, core).start()

        @pl.when(home_core == t)
        def _():
            t_pair.start()

    sq_copy = pair(sq, sqr, ms.at[0], mr.at[0])

    def op_h():
        hid_tr[...] = hid[...].T

    def op_q():
        sq_copy.start()

    def op_w(i):
        part = down_grads(i)
        dsq_out[...] = dsq_out[...] + part if i else part

    ops = {
        "t": op_t, "a": op_a, "m": op_am, "b": op_b, "c": op_c1, "p": op_p, "C": op_c2, "d": op_d, "D": op_dr, "r": op_r,
        "e": op_e, "f": op_f, "x": op_x, "y": op_y, "g": gate_up_grads, "h": op_h, "q": op_q, "w": op_w, "s": op_s,
    }

    def play(text):
        for word in " ".join(text).split():
            ops[word[0]](*(int(x) for x in word[1:]))

    @pl.when((g + 1) // 2 != 1)
    def _():
        play(z.order_end)

    @pl.when(inner)
    def _():
        play(z.order_mid)

    def home(j):
        rcopy(s4.at[j, kr(1, 3)], r4.at[j, kr(1, 3)], r4s.at[0], r4r.at[j], e, other).wait_recv()
        tg_out[:, j * cc : (j + 1) * cc] = mm(s_mat[...], r4[j]).astype(BF)

    for j in range(nj):
        home(j)
    sq_copy.wait_recv()
    gsq_out[...] = sq[0:1, :] + sqr[0:1, :]
    usq_out[...] = sq[1:2, :] + sqr[1:2, :]
    got = trb.at[pl.ds(1, 3)]
    rcopy(got, got, tbs.at[0], tbr.at[0], e, other).wait_recv()

    @pl.when(home_core == t)
    def _():
        rout_out[...] = tsa[g % per_core] + trb[1] + trb[2] + trb[3]

    @pl.when(home_core != t)
    def _():
        t_pair.wait_recv()
        rout_out[...] = trb[0] + trb[1] + trb[2] + trb[3]

    @pl.when(home_core == t)
    def _():
        t_pair.wait_send()
        rcopy(trb.at[pl.ds(0, 2)], trb.at[pl.ds(0, 2)], tbs.at[0], tbr.at[0], e, other).wait_send()

    @pl.when(home_core != t)
    def _():
        rcopy(trb, trb, tbs.at[0], tbr.at[0], e, other).wait_send()

    most, some = pl.ds(0, 3 * blk), pl.ds(0, 16 * 12)

    def left(src, dst, ss, rs):
        rcopy(src, dst, ss, rs, e, other).wait_send()

    left(s1.at[:, kr(1, 3)], r1.at[:, kr(1, 3)], z1s.at[0], z1r.at[0, 0])
    left(s1w.at[kr(1, 3)], r1w.at[kr(1, 3)], z1s.at[1], z1r.at[ng, 0])
    left(s2.at[:, most], x2.at[:, most], p2s.at[0], p2r.at[0, 0])
    left(x2m.at[some], x2m.at[some], p2s.at[1], p2r.at[ng, 0])
    left(x2, y2, fs.at[0], fr.at[0, 0])
    left(wp, wpr, ws.at[0], wr.at[0])
    left(pts, ptr, ptsm.at[0], ptrm.at[0, 0])
    left(s3.at[:, most], r3.at[:, most], r3s.at[0], r3r.at[0, 0])
    left(r3m.at[some], r3m.at[some], r3s.at[1], r3r.at[nj, 0])
    left(s4.at[:, kr(1, 3)], r4.at[:, kr(1, 3)], r4s.at[0], r4r.at[0])
    all_a.wait_send()
    sq_copy.wait_send()


def finish(
    z, gate_in, up_in, down_in, tg_in, gsq_in, usq_in, dsq_in, rout_in,
    gate_out, up_out, down_out, tg_out, gsq_out, usq_out, dsq_out, reg_out, rgg_out, rows_out,
    reg_ref, rgg_ref, rows_ref, sem,
):
    pairs = [
        (gate_in, gate_out), (up_in, up_out), (down_in, down_out), (tg_in, tg_out),
        (gsq_in, gsq_out), (usq_in, usq_out), (dsq_in, dsq_out),
        (reg_ref, reg_out), (rgg_ref, rgg_out), (rows_ref, rows_out),
    ]
    copies = [pltpu.make_async_copy(src, dst, sem.at[i]) for i, (src, dst) in enumerate(pairs)]
    for cp in copies[:7]:
        cp.start()
    half = z.ch // 2
    both = rout_in[...]
    mine = jnp.where(lax.axis_index("tp") == 0, both[:, :half], both[:, half:])
    reg = mine[: z.experts]
    rgg = mine[z.experts : z.experts + z.groups]
    reg_ref[...] = reg
    rgg_ref[...] = rgg
    rows_ref[...] = jnp.sum(reg * reg, axis=0, keepdims=True) + jnp.sum(rgg * rgg, axis=0, keepdims=True)
    for cp in copies[7:]:
        cp.start()
    for cp in copies:
        cp.wait()


def by_source(z):
    return (
        z.reduce_here and z.groups == 4 and z.gs == 4 and z.cap % 16 == 0 and z.gr % 16 == 0
        and z.experts + z.groups <= z.rl // 4 and z.cw % 512 == 0 and (z.cw // z.ch) % z.gs == 0
    )


def run_sourced(z, outs, tokens, cotangent, routes, router_group, router_expert, gate_proj, up_proj, down_proj):
    z.nj = 2
    z.cc = z.cw // z.nj
    z.blk = z.gs * z.cap
    z.per = z.rl // 4
    z.order_end = (
        "t1 a10 b00 a11", "b01 a12 b02 a13", "b03 m1 b10 t3", "a30 b11 a31 b12", "a32 s2 s3 b13",
        "a33 m3 c02 p02", "C02 d02 t2 a20", "b30 b31 a21 b32", "c31 b33 a22 p31", "C31 a23 m2 b20",
        "D31 b21 r1 c21", "b22 b23 p21 e3", "C21 D21 f3 e1", "e0 g0 e2 x", "r0 f2 f1 g1", "g2 y g3 g4",
        "g5 g6 g7 q", "h w0 w1 f0", "w2 w3 w4 w5", "w6 w7",
    )
    z.order_mid = (
        "t1 a10 b00 a11", "b01 a12 b02 a13", "b03 m1 t2 a20", "a21 a22 a23 m2", "b10 b11 c02 b12",
        "b13 p02 C02 d02", "r1 b20 b21 c21", "b22 b23 p21 t3", "a30 a31 C21 a32", "a33 m3 D21 e0",
        "e1 f1 b30 b31", "c31 b32 b33 p31", "C31 e2 f2 D31", "g0 g1 g2 e3", "x r0 f3 g3", "g4 g5 g6 g7",
        "q h y w0", "w1 w2 f0 w3", "w4 w5 w6 w7",
    )
    nj, ng, cc = z.nj, 2 * z.nj, z.cc
    V = pltpu.VMEM
    args = (tokens, cotangent, routes.T, router_expert.T, router_group.T, gate_proj[0], up_proj[0], down_proj[0])
    hb = z.cw // z.ch // z.gs
    scratch = [V(a.shape, a.dtype) for a in args] + [
        V((z.rl, z.width), BF), V((z.rows, z.r1), BF), V((z.r1, z.rows), BF),
        V((z.r1, z.blk), BF), V((z.blk, z.r1), BF),
        V((z.r1, z.rl), BF), V((z.r1, z.rl), BF),
        V((ng, z.r1, cc), BF), V((ng, z.r1, cc), BF),
        V((16 * 4, z.blk), BF), V((16 * 4 * z.gs, z.blk), BF),
        V((ng, z.pairs, cc), BF), V((ng, z.pairs, cc), BF), V((ng, z.pairs, cc), BF),
        V((z.pairs, z.ff), F32), V((z.pairs, z.ff), F32), V((z.pairs, z.ff), F32),
        V((z.ff, z.width), BF), V((z.ff, z.width), BF), V((z.width, z.ff), BF),
        V((z.pairs, 2 * z.ff), BF), V((z.pairs, z.ff), BF), V((z.ff, z.pairs), BF),
        V((z.pairs, z.rl), F32), V((z.pairs, z.rl), F32),
        V((nj, z.pairs, cc), BF), V((nj, z.pairs, cc), BF),
        V((16 * 4, z.blk), BF), V((16 * 4 * z.gs, z.blk), BF),
        V((nj, z.pairs, cc), BF), V((nj, z.pairs, cc), BF),
        V((nj, z.r1, cc), BF), V((nj, z.r1, cc), BF), V((z.r1, z.rl), BF),
        V((2, z.width), F32), V((2, z.width), F32),
        V((z.gs, hb, z.rw, z.ch), F32), V((z.gs - 1, hb, z.rw, z.ch), F32), V((hb, z.rw, z.ch), F32),
        V((z.groups, z.rw, z.ch), F32),
    ]
    D = pltpu.SemaphoreType.DMA
    sems = [D((len(args),))] + [
        D(s) for s in (
            (2,), (ng + 1, 3), (2,), (ng + 1, 4), (1,), (nj + 1, 4), (1,), (4,), (1,), (nj, 4),
            (2,), (nj + 1, 4), (1,), (nj,), (2,), (2,), (1,), (1,), (1,), (1,),
        )
    ]
    spec = pl.BlockSpec(memory_space=pltpu.VMEM)
    return pl.pallas_call(
        functools.partial(sourced, z),
        out_shape=[pltpu.VMEM(s, d) for s, d in outs],
        in_specs=[pl.BlockSpec(memory_space=pltpu.HBM)] * len(args),
        out_specs=[spec] * len(outs),
        scratch_shapes=scratch + sems,
        compiler_params=pltpu.CompilerParams(
            collective_id=0, has_side_effects=True, vmem_limit_bytes=44 * 2**20
        ),
    )(*[pltpu.with_memory_space_constraint(a, pltpu.HBM) for a in args])


def run_wide(z, outs, tokens, cotangent, routes, router_group, router_expert, gate_proj, up_proj, down_proj):
    h, nc, cc = z.half_chunks, z.nc, z.cc
    V = pltpu.VMEM
    chd = z.ch if z.reduce_here else 128
    scratch = [
        V((z.rl, z.width), BF), V((z.r1, z.rl), BF), V((z.r1, z.rl), BF),
        V((z.rows, z.r1), BF), V((z.r1, z.pairs), BF),
        V((z.r1, z.rl), BF), V((z.r1, z.rl), BF),
        V((nc, z.r1, cc), BF), V((nc, z.r1, cc), BF),
        V((z.pairs, z.rl), BF), V((z.pairs, z.rl), BF),
        V((nc, z.pairs, cc), BF), V((nc, z.pairs, cc), BF),
        V((8, 128), BF), V((nc, z.pairs, cc), BF),
        V((z.pairs, z.ff), F32), V((z.pairs, z.ff), F32), V((z.pairs, z.ff), F32),
        V((z.pairs, 2 * z.ff), BF), V((z.pairs, z.ff), BF), V((z.pairs, 128), F32),
        V((z.pairs, 128), F32), V((z.pairs, 128), F32),
        V((h, z.pairs, cc), BF), V((h, z.pairs, cc), BF), V((h, z.pairs, cc), BF),
        V((z.pairs, z.rl), BF), V((z.pairs, z.rl), BF),
        V((h, z.pairs, cc), BF), V((h, z.pairs, cc), BF),
        V((z.r1, z.rl), BF), V((z.r1, z.rl), BF),
        V((h, z.r1, cc), BF), V((h, z.r1, cc), BF),
        V((2, z.width), F32), V((2, z.width), F32),
        V((z.n_ep, z.rw, chd), F32), V((z.n_ep // 2, z.rw, chd), F32),
        V((z.rw, chd), F32), V((z.rw, chd), F32),
    ]
    D = pltpu.SemaphoreType.DMA
    sems = [
        D((nc + 2, z.groups)), D((nc + 2, z.groups)), D((nc + 1, z.gs)), D((nc + 1, z.gs)),
        D((nc, z.gs)), D((nc, z.gs)), D((h,)), D((h,)),
        D((h + 1, z.gs)), D((h + 1, z.gs)), D((h + 1, z.groups)), D((h + 1, z.groups)),
        D((3,)), D((3,)), D((z.n_ep // 2,)), D((z.n_ep // 2,)),
    ]
    spec = pl.BlockSpec(memory_space=pltpu.VMEM)
    return pl.pallas_call(
        functools.partial(kernel, z),
        out_shape=[jax.ShapeDtypeStruct(s, d) for s, d in outs],
        in_specs=[spec] * 8,
        out_specs=[spec] * len(outs),
        scratch_shapes=scratch + sems,
        compiler_params=pltpu.CompilerParams(
            collective_id=0, has_side_effects=True, vmem_limit_bytes=44 * 2**20
        ),
    )(tokens, cotangent, routes.T, router_expert.T, router_group.T, gate_proj[0], up_proj[0], down_proj[0])


def body(axes, tokens, cotangent, routes, router_group, router_expert, gate_proj, up_proj, down_proj):
    z = sizes_of(axes, tokens, routes, router_group, router_expert, gate_proj)
    rout_shape = (z.rw, z.ch) if z.reduce_here else (min(z.rw, z.rl), z.width)
    outs = [
        ((z.rows, z.cw), BF), ((z.width, z.ff), BF), ((z.width, z.ff), BF), ((z.ff, z.width), BF),
        ((1, z.width), F32), ((1, z.width), F32), ((1, z.ff), F32), (rout_shape, F32),
    ]
    spec = pl.BlockSpec(memory_space=pltpu.VMEM)
    D = pltpu.SemaphoreType.DMA
    run = run_sourced if by_source(z) else run_wide
    tg, gate, up, down, gsq, usq, dsq, rout = run(
        z, outs, tokens, cotangent, routes, router_group, router_expert, gate_proj, up_proj, down_proj
    )
    if z.reduce_here:
        half = z.ch // 2
        shapes = [gate, up, down, tg, gsq, usq, dsq]
        anywhere = pl.BlockSpec(memory_space=pl.ANY)
        gate, up, down, tg, gsq, usq, dsq, reg, rgg, rrows = pl.pallas_call(
            functools.partial(finish, z),
            out_shape=[jax.ShapeDtypeStruct(a.shape, a.dtype) for a in shapes]
            + [jax.ShapeDtypeStruct((n, half), F32) for n in (z.experts, z.groups, 1)],
            in_specs=[spec] * 8,
            out_specs=[anywhere] * 10,
            scratch_shapes=[pltpu.VMEM((n, half), F32) for n in (z.experts, z.groups, 1)] + [D((10,))],
            compiler_params=pltpu.CompilerParams(vmem_limit_bytes=16 * 2**20),
        )(*shapes, rout)
        reg, rgg, rrows = reg.T, rgg.T, rrows[0]
    else:
        mine = lax.psum_scatter(rout.T, ("ep", "tp"), scatter_dimension=0, tiled=True)
        reg = mine[:, : z.experts]
        rgg = mine[:, z.experts : z.experts + z.groups]
        rrows = jnp.sum(reg * reg, axis=1) + jnp.sum(rgg * rgg, axis=1)
    return (tg, gate[None], up[None], down[None], gsq, usq, dsq, reg, rgg, rrows)


def solution(mesh):
    return jax.shard_map(
        functools.partial(body, dict(mesh.shape)),
        mesh=mesh,
        in_specs=(
            P("ep", None), P("ep", None), P("ep", None), P(), P(),
            P("ep", None, "tp"), P("ep", None, "tp"), P("ep", "tp", None),
        ),
        out_specs=(
            P("ep", "tp"), P("ep", None, "tp"), P("ep", None, "tp"), P("ep", "tp", None),
            P("ep", None), P("ep", None), P("ep", "tp"),
            P(("ep", "tp"), None), P(("ep", "tp"), None), P(("ep", "tp")),
        ),
        check_vma=False,
    )
```
